32 devices in a mesh: kv: 16 (over z, y, core), tp: 2 (over x).
Axes of the slice: x: 2, y: 2, z: 4, core: 2. Of those that a mesh axis runs over, the one named last changes fastest.
Arguments:
- layer_input: bfloat16 [3072, 2048], P('kv', 'tp'), may hold values from -0.15625 to 0.15625
- queries: bfloat16 [3072, 1024], P('kv', 'tp'), may hold values from -6 to 6
- keys: bfloat16 [3072, 256], P('kv', 'tp'), may hold values from -6 to 6
- values: bfloat16 [3072, 256], P('kv', 'tp'), may hold values from -6 to 6
- attn_out: bfloat16 [3072, 1024], P('kv', 'tp'), may hold values from -1.25 to 1.25
- grad_out: bfloat16 [3072, 1024], P('kv', 'tp'), may hold values from -128 to 128
- log_sum: float32 [3072, 16], P('kv', 'tp'), may hold values from 6 to 7.5
- chosen: int32 [48, 8], replicated, may hold values from -1 to 47, as said below
Outputs:
- grad_queries: bfloat16 [3072, 1024], P('kv', 'tp')
- grad_keys: bfloat16 [3072, 256], P('kv', 'tp')
- grad_values: bfloat16 [3072, 256], P('kv', 'tp')
- grad_weight: float32 [2048, 1024], P('kv', 'tp')
The draws below stay inside these ranges and needn't reach their ends.
Inputs may be any that keep to these rules, and one draw needn't show every extreme that they name: Write R = 3 and call positions [s * 192, (s + 1) * 192) segment s. For query block b in segment c = b // R and level l < 4, the entries chosen[b, 2 l + i] for i < 2 name 2 different key blocks of segment c - g_l, with g = 1, 2, 4, 8; all of them are -1 where c - g_l is negative.
All inputs are finite; a program needn't handle non-finite values.
Results may differ from the reference program's by a relative error of at most 0.0053.
Values may be sent and summed in bfloat16 or wider, within the bound.
A program may use at most 64 MiB of HBM per device.

```python
import jax
import jax.numpy as jnp
from jax import lax

D = 2048
HEADS = 16
KVH = 4
DH = 64
BLOCK = 64
PER = 2
LEVELS = 4
TOK_DEV = 192
TOKENS = 3072
TOPK = 8
HOP = 2


def draw_chosen(key, part):
    per_segment = TOK_DEV // BLOCK
    total_blocks = TOKENS // BLOCK
    distances = jnp.array([1, HOP, 2 * HOP, 4 * HOP], jnp.int32)
    block_ids = jnp.arange(total_blocks, dtype=jnp.int32)
    segment = block_ids // per_segment
    ranks = jax.random.randint(jax.random.fold_in(key, 17), (total_blocks, LEVELS, per_segment), 0, 1 << 20)
    ranks = ranks * per_segment + jnp.arange(per_segment, dtype=jnp.int32)
    unused, order = lax.top_k(ranks, PER)
    source = segment[:, None] - distances[None, :]
    picked = source[:, :, None] * per_segment + order.astype(jnp.int32)
    picked = jnp.where(source[:, :, None] >= 0, picked, -1)
    return picked.reshape(total_blocks, LEVELS * PER).astype(jnp.int32)


def spiked(values, own_key, source, target, parts, factor):
    def block_of(position):
        return (jnp.arange(values.shape[position]) // (values.shape[position] // parts)).reshape((-1,) + (1,) * (values.ndim - 1 - position))

    one_side = jax.random.permutation(own_key, parts)[block_of(target)]
    far = (block_of(target) + parts // 2) % parts
    return jnp.where((block_of(source) == one_side) | (block_of(source) == far), factor * values, values)


def level_of(own_key, extent, cuts, least, largest):
    gain, own = 1.0, jax.random.fold_in(own_key, 6)
    for axis_at, blocks in cuts:
        draws = jnp.exp(jax.random.uniform(jax.random.fold_in(own, axis_at), (blocks,), jnp.float32, least / len(cuts), largest / len(cuts)))
        gain = gain * jnp.repeat(draws, extent[axis_at] // blocks).reshape([-1 if axis == axis_at else 1 for axis in range(len(extent))])
    return gain


def centred(stream_key, dims, deviation, limit, cuts=(), held_as=jnp.bfloat16):
    result = deviation * jax.random.normal(stream_key, dims, jnp.float32)
    if cuts:
        result = result * level_of(stream_key, dims, cuts, -0.22, 0.18)
    return jnp.clip(result, -limit, limit).astype(held_as)


def heavy_noise(key, shape, spread, most, cuts, heavy, kind=jnp.bfloat16):
    entries = spread * jax.random.normal(key, shape, jnp.float32)
    if cuts:
        entries = entries * level_of(key, shape, cuts, -0.22, 0.18)
    return jnp.clip(spiked(entries, jax.random.fold_in(key, 3), *heavy), -most, most).astype(kind)


def setup_inputs(seed: int = 0) -> dict:
    streams_of = jax.random.split(jax.random.key(seed), 9)
    layer_input = heavy_noise(streams_of[0], (TOKENS, D), (TOKENS ** -0.5), 0.15625, ((0, 16), (1, 2)), (0, 1, 16, 2.0))
    queries = centred(streams_of[1], (TOKENS, HEADS * DH), 1.0, 6.0, ((0, 16), (1, 2)))
    keys = centred(streams_of[2], (TOKENS, KVH * DH), 1.0, 6.0, ((0, 16), (1, 2)))
    values = centred(streams_of[3], (TOKENS, KVH * DH), 1.0, 6.0, ((0, 16), (1, 2)))
    attn_out = centred(streams_of[4], (TOKENS, HEADS * DH), 0.2, 1.25, ((0, 16), (1, 2)))
    grad_out = centred(streams_of[5], (TOKENS, HEADS * DH), 24.0, 128.0, ((0, 16), (1, 2)))
    log_sum = jnp.clip(6.0 + 1.5 * jax.random.uniform(streams_of[6], (TOKENS, HEADS), jnp.float32) ** level_of(streams_of[6], (TOKENS, HEADS), ((0, 16), (1, 2)), -0.2, 0.2), 6.0, 7.5)
    chosen = draw_chosen(jax.random.fold_in(streams_of[8], 71), 0)
    return {"layer_input": layer_input, "queries": queries, "keys": keys, "values": values, "attn_out": attn_out, "grad_out": grad_out, "log_sum": log_sum, "chosen": chosen}


def pair_terms(query_blk, grad_blk, lse_blk, delta_blk, key_blk, value_blk, keep_mask, scale_value):
    query_f = query_blk.astype(jnp.float32)
    grad_f = grad_blk.astype(jnp.float32)
    key_f = key_blk.astype(jnp.float32)
    value_f = value_blk.astype(jnp.float32)
    scores = jnp.einsum('pbkge,pcke->pkgbc', query_f, key_f) * scale_value
    lse_cols = jnp.transpose(lse_blk, (0, 2, 3, 1))[..., None]
    delta_cols = jnp.transpose(delta_blk, (0, 2, 3, 1))[..., None]
    weights = jnp.where(keep_mask[:, None, None], jnp.exp(scores - lse_cols), jnp.float32(0.0))
    weights_low = lax.optimization_barrier(weights.astype(jnp.bfloat16)).astype(jnp.float32)
    dweights = jnp.einsum('pbkge,pcke->pkgbc', grad_f, value_f)
    dscores = lax.optimization_barrier((weights * (dweights - delta_cols)).astype(jnp.bfloat16)).astype(jnp.float32)
    grad_query = jnp.einsum('pkgbc,pcke->pbkge', dscores, key_f) * scale_value
    grad_key = jnp.einsum('pkgbc,pbkge->pcke', dscores, query_f) * scale_value
    grad_value = jnp.einsum('pkgbc,pbkge->pcke', weights_low, grad_f)
    return grad_query, grad_key, grad_value


def reference(layer_input, queries, keys, values, attn_out, grad_out, log_sum, chosen):
    total_rows = queries.shape[0]
    nblocks = total_rows // BLOCK
    group_size = HEADS // KVH
    scale_value = DH ** -0.5
    query_all = queries.reshape(nblocks, BLOCK, KVH, group_size, DH)
    grad_all = grad_out.reshape(nblocks, BLOCK, KVH, group_size, DH)
    delta_all = jnp.sum(grad_out.astype(jnp.float32).reshape(nblocks, BLOCK, KVH, group_size, DH)
                        * attn_out.astype(jnp.float32).reshape(nblocks, BLOCK, KVH, group_size, DH), axis=-1)
    lse_all = log_sum.reshape(nblocks, BLOCK, KVH, group_size)
    key_all = keys.reshape(nblocks, BLOCK, KVH, DH)
    value_all = values.reshape(nblocks, BLOCK, KVH, DH)
    causal = lax.broadcasted_iota(jnp.int32, (BLOCK, BLOCK), 0) >= lax.broadcasted_iota(jnp.int32, (BLOCK, BLOCK), 1)
    slot_ids = jnp.arange(TOPK + 1, dtype=jnp.int32)

    def one_block(carry, block_num):
        key_acc, value_acc = carry
        listed = chosen[block_num].astype(jnp.int32)
        targets = jnp.concatenate([block_num[None], listed]).astype(jnp.int32)
        is_live = targets >= 0
        safe_ids = jnp.where(is_live, targets, 0).astype(jnp.int32)
        keep_mask = jnp.where((slot_ids == 0)[:, None, None], causal[None], True) & is_live[:, None, None]
        count_pairs = TOPK + 1
        query_rep = jnp.broadcast_to(query_all[block_num][None], (count_pairs, BLOCK, KVH, group_size, DH))
        grad_rep = jnp.broadcast_to(grad_all[block_num][None], (count_pairs, BLOCK, KVH, group_size, DH))
        lse_rep = jnp.broadcast_to(lse_all[block_num][None], (count_pairs, BLOCK, KVH, group_size))
        delta_rep = jnp.broadcast_to(delta_all[block_num][None], (count_pairs, BLOCK, KVH, group_size))
        grad_query, grad_key, grad_value = pair_terms(query_rep, grad_rep, lse_rep, delta_rep,
                                                      key_all[safe_ids], value_all[safe_ids], keep_mask, scale_value)
        key_acc = key_acc.at[safe_ids].add(grad_key)
        value_acc = value_acc.at[safe_ids].add(grad_value)
        return (key_acc, value_acc), jnp.sum(grad_query, axis=0)

    zeros_acc = jnp.zeros((nblocks, BLOCK, KVH, DH), jnp.float32)
    (key_acc, value_acc), grad_blocks = lax.scan(one_block, (zeros_acc, zeros_acc),
                                                 jnp.arange(nblocks, dtype=jnp.int32))
    grad_queries = grad_blocks.reshape(total_rows, HEADS * DH).astype(jnp.bfloat16)
    grad_keys = key_acc.reshape(total_rows, KVH * DH).astype(jnp.bfloat16)
    grad_values = value_acc.reshape(total_rows, KVH * DH).astype(jnp.bfloat16)
    grad_weight = jnp.dot(layer_input.T, grad_queries, preferred_element_type=jnp.float32)
    return grad_queries, grad_keys, grad_values, grad_weight
```

```python
import functools
import math

import jax
import jax.numpy as jnp
from jax import lax
from jax.experimental import pallas as pl
from jax.experimental.pallas import tpu as pltpu
from jax.sharding import PartitionSpec as P

DH = 64
BLOCK = 64
PER = 2
LEVELS = 4
LOG2E = 1.4426950408889634
NEG = -1e30
NT = (((1,), (1,)), ((), ()))
TN = (((0,), (0,)), ((), ()))
NN = (((1,), (0,)), ((), ()))
BF = jnp.bfloat16
F32 = jnp.float32


def dot(a, b, dims):
    return lax.dot_general(a, b, dims, preferred_element_type=F32)


def kernel(cfg, *refs):
    n, tp, with_dw = cfg
    count_in = 7 if with_dw else 6
    hbm, refs = refs[:count_in], refs[count_in:]
    ch_hbm, refs = refs[0], refs[1:]
    count_out = 4 if with_dw else 3
    outs, refs = refs[:count_out], refs[count_out:]
    held, refs = refs[:count_in], refs[count_in:]
    ch_ref, refs = refs[0], refs[1:]
    (in_s, qs, gs, lrow, drow, dqt, acc, kvbuf, gsend, grecv,
     kv_s, kv_r, g_s, g_r) = refs[:14]
    dq_out, dk_out, dv_out = outs[:3]
    k_ref, v_ref, q_ref, g_ref, o_ref, lse_ref = held[:3] + held[-3:]
    if with_dw:
        x_ref = held[3]
        dw_out = outs[3]
        (xbuf, xt, dqall, part, precv, x_s, x_r, a_s, a_r, f_s, f_r, w_s, w_r) = refs[14:]
    loads = [pltpu.make_async_copy(hbm[i], held[i], in_s.at[i]) for i in range(count_in)]
    loads.append(pltpu.make_async_copy(ch_hbm, ch_ref, in_s.at[count_in]))
    for load in loads:
        load.start()
    me = lax.axis_index("kv")
    mt = lax.axis_index("tp")
    tok = q_ref.shape[0]
    kvh = k_ref.shape[1] // DH
    qh = q_ref.shape[1] // DH
    grp = qh // kvh
    nb = tok // BLOCK
    cols = grp * tok
    scale = DH ** -0.5
    dist = [1, n // 8, n // 4, n // 2]
    if with_dw:
        wn = math.isqrt(n)
        zn = n // wn
        zper = zn // tp
        rows = dw_out.shape[0]
        z = me // wn
        w = lax.rem(me, wn)
        pair = w + 1 - 2 * lax.rem(w, 2)
        across = lax.rem(w + 2, wn)
        across_pair = lax.rem(pair + 2, wn)
        near = z + 1 - 2 * lax.rem(z, 2)
        far = lax.rem(z + 2, zn)
        plane = [(pair, mt), (across, mt), (across_pair, mt), (w, 1 - mt), (pair, 1 - mt)]

    barrier = pltpu.get_barrier_semaphore()
    count = jnp.int32(0)
    for d in dist:
        @pl.when(me + d < n)
        def _():
            pl.semaphore_signal(barrier, inc=1, device_id={"kv": me + d}, device_id_type=pl.DeviceIdType.MESH)

        @pl.when(me >= d)
        def _():
            pl.semaphore_signal(barrier, inc=1, device_id={"kv": me - d}, device_id_type=pl.DeviceIdType.MESH)

        count = count + jnp.where(me + d < n, 1, 0) + jnp.where(me >= d, 1, 0)
    if with_dw:
        for wt, tt in plane:
            pl.semaphore_signal(barrier, inc=1, device_id={"kv": z * wn + wt, "tp": tt}, device_id_type=pl.DeviceIdType.MESH)
        for zt in (near, far):
            pl.semaphore_signal(barrier, inc=1, device_id={"kv": zt * wn + w}, device_id_type=pl.DeviceIdType.MESH)
        count = count + len(plane) + 2
    pl.semaphore_wait(barrier, count)

    def kv_copy(level, i):
        return pltpu.make_async_remote_copy(
            src_ref=(k_ref, v_ref)[i], dst_ref=kvbuf.at[level, i],
            send_sem=kv_s.at[level, i], recv_sem=kv_r.at[level, i],
            device_id={"kv": me + dist[level]}, device_id_type=pl.DeviceIdType.MESH)

    def g_copy(level):
        return pltpu.make_async_remote_copy(
            src_ref=gsend.at[level], dst_ref=grecv.at[level],
            send_sem=g_s.at[level], recv_sem=g_r.at[level],
            device_id={"kv": me - dist[level]}, device_id_type=pl.DeviceIdType.MESH)

    loads[0].wait()
    loads[1].wait()
    turns = [0, 1, 3, 2]
    for level in turns:
        @pl.when(me + dist[level] < n)
        def _():
            kv_copy(level, 0).start()
            kv_copy(level, 1).start()

    if with_dw:
        def x_copy(idx, zz):
            wt, tt = plane[idx]
            off = pl.multiple_of((zz * wn + wt) * rows, rows)
            return pltpu.make_async_remote_copy(
                src_ref=x_ref.at[:, pl.ds(off, rows)],
                dst_ref=xbuf.at[mt * zper + zz, pl.ds(pl.multiple_of(w * tok, tok), tok)],
                send_sem=x_s.at[idx, zz], recv_sem=x_r.at[idx, zz],
                device_id={"kv": z * wn + wt, "tp": tt}, device_id_type=pl.DeviceIdType.MESH)

        def x_forward(idx, zz):
            slot = xbuf.at[mt * zper + zz, pl.ds(pl.multiple_of(plane[idx][0] * tok, tok), tok)]
            return pltpu.make_async_remote_copy(
                src_ref=slot, dst_ref=slot,
                send_sem=x_s.at[idx + 4, zz], recv_sem=x_r.at[idx + 4, zz],
                device_id={"kv": me, "tp": 1 - mt}, device_id_type=pl.DeviceIdType.MESH)

        loads[3].wait()
        for zz in range(zper):
            for idx in (1, 2, 3, 4, 0):
                x_copy(idx, zz).start()
        for zz in range(zper):
            off = pl.multiple_of((zz * wn + w) * rows, rows)
            xbuf[mt * zper + zz, pl.ds(pl.multiple_of(w * tok, tok), tok), :] = x_ref[:, pl.ds(off, rows)]

    for i in range(count_in + 1):
        if i not in (0, 1, 3) or (i == 3 and not with_dw):
            loads[i].wait()
    lse_t = lse_ref[...] * (-LOG2E)
    prod = g_ref[...].astype(F32) * o_ref[...].astype(F32)
    hi = prod.astype(BF)
    lo = (prod - hi.astype(F32)).astype(BF)
    pick = (lax.broadcasted_iota(jnp.int32, (16, qh * DH), 1) // DH
            == lax.broadcasted_iota(jnp.int32, (16, qh * DH), 0)).astype(F32).astype(BF)
    delta_t = dot(pick, hi, NT) + dot(pick, lo, NT)
    for h in range(kvh):
        for g in range(grp):
            i = h * grp + g
            lrow[h, 0:1, g * tok:(g + 1) * tok] = lse_t[i:i + 1, 0:tok]
            drow[h, 0:1, g * tok:(g + 1) * tok] = delta_t[i:i + 1, :]
            qs[h, g * tok:(g + 1) * tok, :] = q_ref[:, i * DH:(i + 1) * DH]
            gs[h, g * tok:(g + 1) * tok, :] = g_ref[:, i * DH:(i + 1) * DH]

    q_block = lax.rem(lax.broadcasted_iota(jnp.int32, (1, cols), 1), tok) // BLOCK

    def run_pass(h, k, v, bias):
        lse = lrow[h, 0:1, :]
        st = dot(k, qs[h], NT) * (scale * LOG2E)
        if bias is None:
            kp = lax.broadcasted_iota(jnp.int32, (tok, cols), 0)
            qp = lax.rem(lax.broadcasted_iota(jnp.int32, (tok, cols), 1), tok)
            keep = (qp >= kp) & ((qp // BLOCK) == (kp // BLOCK))
            p = jnp.exp2(jnp.where(keep, st + lse, NEG))
        else:
            p = jnp.concatenate(
                [jnp.exp2(st[b * BLOCK:(b + 1) * BLOCK] + (lse + bias[b])) for b in range(nb)], axis=0)
        dp = dot(v, gs[h], NT)
        ds = (p * (dp - drow[h, 0:1, :])).astype(BF)
        dv = dot(p.astype(BF), gs[h], NN)
        dk = dot(ds, qs[h], NN) * scale
        dq = dot(k, ds, TN)
        return dq, dk, dv

    for h in range(kvh):
        lanes = slice(h * DH, (h + 1) * DH)
        dq, dk, dv = run_pass(h, k_ref[:, lanes], v_ref[:, lanes], None)
        dqt[h] = dq
        acc[0, :, lanes] = dk
        acc[1, :, lanes] = dv

    def level_bias(level):
        bias = []
        for kb in range(nb):
            row = jnp.full((1, cols), NEG, F32)
            target = (me - dist[level]) * nb + kb
            for qb in range(nb):
                hit = jnp.float32(NEG)
                for i in range(PER):
                    hit = jnp.where(ch_ref[PER * level + i, me * nb + qb] == target, jnp.float32(0.0), hit)
                row = jnp.where(q_block == qb, hit, row)
            bias.append(row)
        return bias

    def far_pass(level, h, bias):
        lanes = slice(h * DH, (h + 1) * DH)
        dq, dk, dv = run_pass(h, kvbuf[level, 0, :, lanes], kvbuf[level, 1, :, lanes], bias)
        dqt[h] = dqt[h] + dq
        gsend[level, 0, :, lanes] = dk.astype(BF)
        gsend[level, 1, :, lanes] = dv.astype(BF)

    for level in turns[:-1]:
        @pl.when(me >= dist[level])
        def _():
            kv_copy(level, 0).wait_recv()
            kv_copy(level, 1).wait_recv()
            bias = level_bias(level)
            for h in range(kvh):
                far_pass(level, h, bias)
            g_copy(level).start()

    if with_dw:
        mine = pl.ds(pl.multiple_of(w * tok, tok), tok)
        hops = list(range(2, wn, 2))

        def a_copy(h, s):
            to = pair if s == 0 else lax.rem(w + s, wn)
            return pltpu.make_async_remote_copy(
                src_ref=dqall.at[h, mine], dst_ref=dqall.at[h, mine],
                send_sem=a_s.at[h, s // 2], recv_sem=a_r.at[h, s // 2],
                device_id={"kv": z * wn + to}, device_id_type=pl.DeviceIdType.MESH)

        def f_copy(h, s):
            slot = pl.ds(pl.multiple_of(lax.rem(w + wn - s, wn) * tok, tok), tok)
            return pltpu.make_async_remote_copy(
                src_ref=dqall.at[h, slot], dst_ref=dqall.at[h, slot],
                send_sem=f_s.at[h, s // 2 - 1], recv_sem=f_r.at[h, s // 2 - 1],
                device_id={"kv": z * wn + pair}, device_id_type=pl.DeviceIdType.MESH)

    if with_dw:
        for zz in range(zper):
            for idx in (1, 2):
                x_copy(idx, zz).wait_recv()
                x_forward(idx, zz).start()

    last = turns[-1]
    for h in range(kvh):
        @pl.when(me >= dist[last])
        def _():
            if h == 0:
                kv_copy(last, 0).wait_recv()
                kv_copy(last, 1).wait_recv()
            far_pass(last, h, level_bias(last))
        whole = dqt[h] * scale
        for g in range(grp):
            low = whole[:, g * tok:(g + 1) * tok].T.astype(BF)
            i = h * grp + g
            dq_out[:, i * DH:(i + 1) * DH] = low
            if with_dw:
                dqall[h, mine, g * DH:(g + 1) * DH] = low
        if with_dw:
            for s in hops:
                a_copy(h, s).start()
            a_copy(h, 0).start()

    @pl.when(me >= dist[last])
    def _():
        g_copy(last).start()

    if with_dw:
        for zz in range(zper):
            for idx in range(len(plane)):
                if idx in (1, 2):
                    x_copy(idx, zz).wait_send()
                    x_forward(idx, zz).wait()
                else:
                    x_copy(idx, zz).wait()
        for zz in range(zn):
            xt[zz] = xbuf[zz].T

        def w_copy(h, i):
            return pltpu.make_async_remote_copy(
                src_ref=part.at[h, i], dst_ref=precv.at[h, i],
                send_sem=w_s.at[h, i], recv_sem=w_r.at[h, i],
                device_id={"kv": (far if i == 2 else near) * wn + w}, device_id_type=pl.DeviceIdType.MESH)

        def send_near(h):
            part[h, 1] = dot(xt[near], dqall[h], NN).astype(BF)
            w_copy(h, 1).start()

        for h in range(kvh):
            for s in hops:
                a_copy(h, s).wait_recv()
                f_copy(h, s).start()
            a_copy(h, 0).wait_recv()
            for s in hops:
                f_copy(h, s).wait_recv()
            part[h, 0] = dot(xt[lax.rem(near + 2, zn)], dqall[h], NN).astype(BF)
            w_copy(h, 0).start()
        send_near(0)
        for h in range(kvh):
            ours = dot(xt[far], dqall[h], NN)
            w_copy(h, 0).wait_recv()
            part[h, 2] = (ours + precv[h, 0].astype(F32)).astype(BF)
            w_copy(h, 2).start()
        for h in range(1, kvh):
            send_near(h)
        width = grp * DH
        for h in range(kvh):
            dw_out[:, h * width:(h + 1) * width] = dot(xt[z], dqall[h], NN)
        for h in range(kvh):
            for s in [0] + hops:
                a_copy(h, s).wait_send()
            for s in hops:
                f_copy(h, s).wait_send()

    for level, d in enumerate(dist):
        @pl.when(me + d < n)
        def _():
            kv_copy(level, 0).wait_send()
            kv_copy(level, 1).wait_send()
            g_copy(level).wait_recv()
            acc[...] = acc[...] + grecv[level].astype(F32)

        @pl.when(me >= d)
        def _():
            g_copy(level).wait_send()

    dk_out[...] = acc[0].astype(BF)
    dv_out[...] = acc[1].astype(BF)
    if with_dw:
        for h in range(kvh):
            lanes = slice(h * width, (h + 1) * width)
            w_copy(h, 0).wait_send()
            w_copy(h, 1).wait()
            w_copy(h, 2).wait()
            dw_out[:, lanes] = dw_out[:, lanes] + precv[h, 1].astype(F32) + precv[h, 2].astype(F32)


def writer(*refs):
    count = (len(refs) - 1) // 2
    sem = refs[-1]
    copies = [pltpu.make_async_copy(refs[i], refs[count + i], sem.at[i]) for i in range(count)]
    for copy in copies:
        copy.start()
    for copy in copies:
        copy.wait()


def shards(layer_input, queries, keys, values, attn_out, grad_out, log_sum, chosen):
    n = lax.axis_size("kv")
    tp = lax.axis_size("tp")
    tok, qw = queries.shape
    kw = keys.shape[1]
    kvh, qh = kw // DH, qw // DH
    cols = qh // kvh * tok
    depth = layer_input.shape[1] * tp
    rows = depth // n
    wn = math.isqrt(n)
    zn = n // wn
    with_dw = wn * wn == n and zn == 4 and tp == 2 and rows % 128 == 0
    vm = pl.BlockSpec(memory_space=pltpu.VMEM)
    out_shape = [
        jax.ShapeDtypeStruct((tok, qw), BF),
        jax.ShapeDtypeStruct((tok, kw), BF),
        jax.ShapeDtypeStruct((tok, kw), BF),
    ]
    args = [keys, values, queries, grad_out, attn_out, log_sum.T]
    if with_dw:
        args.insert(3, layer_input)
    scratch = [pltpu.VMEM(a.shape, a.dtype) for a in args] + [
        pltpu.SMEM(chosen.T.shape, chosen.dtype),
        pltpu.SemaphoreType.DMA((len(args) + 1,)),
        pltpu.VMEM((kvh, cols, DH), BF),
        pltpu.VMEM((kvh, cols, DH), BF),
        pltpu.VMEM((kvh, 1, cols), F32),
        pltpu.VMEM((kvh, 1, cols), F32),
        pltpu.VMEM((kvh, DH, cols), F32),
        pltpu.VMEM((2, tok, kw), F32),
        pltpu.VMEM((LEVELS, 2, tok, kw), BF),
        pltpu.VMEM((LEVELS, 2, tok, kw), BF),
        pltpu.VMEM((LEVELS, 2, tok, kw), BF),
        pltpu.SemaphoreType.DMA((LEVELS, 2)),
        pltpu.SemaphoreType.DMA((LEVELS, 2)),
        pltpu.SemaphoreType.DMA((LEVELS,)),
        pltpu.SemaphoreType.DMA((LEVELS,)),
    ]
    hbm = pl.BlockSpec(memory_space=pltpu.HBM)
    specs = [hbm] * (len(args) + 1)
    if with_dw:
        out_shape.append(jax.ShapeDtypeStruct((rows, qw), F32))
        peers = 7
        zper = zn // tp
        scratch += [
            pltpu.VMEM((zn, wn * tok, rows), BF),
            pltpu.VMEM((zn, rows, wn * tok), BF),
            pltpu.VMEM((kvh, wn * tok, qw // kvh), BF),
            pltpu.VMEM((kvh, zn - 1, rows, qw // kvh), BF),
            pltpu.VMEM((kvh, zn - 1, rows, qw // kvh), BF),
            pltpu.SemaphoreType.DMA((peers, zper)),
            pltpu.SemaphoreType.DMA((peers, zper)),
            pltpu.SemaphoreType.DMA((kvh, wn // 2)),
            pltpu.SemaphoreType.DMA((kvh, wn // 2)),
            pltpu.SemaphoreType.DMA((kvh, max(wn // 2 - 1, 1))),
            pltpu.SemaphoreType.DMA((kvh, max(wn // 2 - 1, 1))),
            pltpu.SemaphoreType.DMA((kvh, zn - 1)),
            pltpu.SemaphoreType.DMA((kvh, zn - 1)),
        ]
    outs = pl.pallas_call(
        functools.partial(kernel, (n, tp, with_dw)),
        out_shape=[pltpu.VMEM(a.shape, a.dtype) for a in out_shape],
        in_specs=specs,
        out_specs=[vm] * len(out_shape),
        scratch_shapes=scratch,
        compiler_params=pltpu.CompilerParams(
            collective_id=0, has_side_effects=True, vmem_limit_bytes=66100000),
    )(*args, chosen.T)
    outs = pl.pallas_call(
        writer,
        out_shape=out_shape,
        in_specs=[vm] * len(out_shape),
        out_specs=[hbm] * len(out_shape),
        scratch_shapes=[pltpu.SemaphoreType.DMA((len(out_shape),))],
        compiler_params=pltpu.CompilerParams(vmem_limit_bytes=1024 * 1024),
    )(*outs)
    if with_dw:
        return tuple(outs)
    whole_input = lax.all_gather(layer_input, "tp", axis=1, tiled=True)
    grad_weight = lax.psum_scatter(
        jnp.einsum("td,tc->dc", whole_input, outs[0], preferred_element_type=F32),
        "kv", scatter_dimension=0, tiled=True)
    return tuple(outs) + (grad_weight,)


def solution(mesh):
    spec = P("kv", "tp")
    return jax.shard_map(
        shards,
        mesh=mesh,
        in_specs=(spec,) * 7 + (P(),),
        out_specs=(spec,) * 4,
        check_vma=False,
    )
```

```python
import functools
import math

import jax
import jax.numpy as jnp
from jax import lax
from jax.experimental import pallas as pl
from jax.experimental.pallas import tpu as pltpu
from jax.sharding import PartitionSpec as P

DH = 64
BLOCK = 64
PER = 2
LEVELS = 4
LOG2E = 1.4426950408889634
NEG = -1e30
NT = (((1,), (1,)), ((), ()))
TN = (((0,), (0,)), ((), ()))
NN = (((1,), (0,)), ((), ()))
BF = jnp.bfloat16
F32 = jnp.float32


def dot(a, b, dims):
    return lax.dot_general(a, b, dims, preferred_element_type=F32)


def kernel(cfg, *refs):
    n, tp, with_dw = cfg
    count_in = 7 if with_dw else 6
    hbm, refs = refs[:count_in], refs[count_in:]
    ch_hbm, refs = refs[0], refs[1:]
    count_out = 4 if with_dw else 3
    outs, refs = refs[:count_out], refs[count_out:]
    held, refs = refs[:count_in], refs[count_in:]
    ch_ref, refs = refs[0], refs[1:]
    (in_s, qs, gs, lrow, drow, dqt, acc, kvbuf, gsend, grecv,
     kv_s, kv_r, g_s, g_r) = refs[:14]
    dq_out, dk_out, dv_out = outs[:3]
    k_ref, v_ref, q_ref, g_ref, o_ref, lse_ref = held[:3] + held[-3:]
    if with_dw:
        x_ref = held[3]
        dw_out = outs[3]
        (xbuf, xt, dqall, part, precv, x_s, x_r, a_s, a_r, f_s, f_r, w_s, w_r) = refs[14:]
    loads = [pltpu.make_async_copy(hbm[i], held[i], in_s.at[i]) for i in range(count_in)]
    loads.append(pltpu.make_async_copy(ch_hbm, ch_ref, in_s.at[count_in]))
    for load in loads:
        load.start()
    me = lax.axis_index("kv")
    mt = lax.axis_index("tp")
    tok = q_ref.shape[0]
    kvh = k_ref.shape[1] // DH
    qh = q_ref.shape[1] // DH
    grp = qh // kvh
    nb = tok // BLOCK
    cols = grp * tok
    scale = DH ** -0.5
    dist = [1, n // 8, n // 4, n // 2]

    def span(level):
        if isinstance(level, int):
            return dist[level]
        return jnp.where(level == 0, dist[0], jnp.where(level == 1, dist[1], jnp.where(level == 2, dist[2], dist[3])))

    if with_dw:
        wn = math.isqrt(n)
        zn = n // wn
        zper = zn // tp
        rows = dw_out.shape[0]
        z = me // wn
        w = lax.rem(me, wn)
        pair = w + 1 - 2 * lax.rem(w, 2)
        across = lax.rem(w + 2, wn)
        across_pair = lax.rem(pair + 2, wn)
        near = z + 1 - 2 * lax.rem(z, 2)
        far = lax.rem(z + 2, zn)
        partner = me + 1 - 2 * lax.rem(me, 2)
        first = lax.rem(me, 2) == 0
        second = lax.rem(me, 2) == 1
        order = [1 - lax.rem(z, 2), lax.rem(z, 2)]
        plane = [(pair, mt), (across, mt), (across_pair, mt), (w, 1 - mt), (pair, 1 - mt)]

    barrier = pltpu.get_barrier_semaphore()
    count = jnp.int32(0)
    for d in dist[1:] if with_dw else dist:
        @pl.when(me + d < n)
        def _():
            pl.semaphore_signal(barrier, inc=1, device_id={"kv": me + d}, device_id_type=pl.DeviceIdType.MESH)

        @pl.when(me >= d)
        def _():
            pl.semaphore_signal(barrier, inc=1, device_id={"kv": me - d}, device_id_type=pl.DeviceIdType.MESH)

        count = count + jnp.where(me + d < n, 1, 0) + jnp.where(me >= d, 1, 0)
    if with_dw:
        for wt, tt in plane:
            pl.semaphore_signal(barrier, inc=1, device_id={"kv": z * wn + wt, "tp": tt}, device_id_type=pl.DeviceIdType.MESH)
        for zt in (near, far):
            pl.semaphore_signal(barrier, inc=1, device_id={"kv": zt * wn + w}, device_id_type=pl.DeviceIdType.MESH)
        count = count + len(plane) + 2
    pl.semaphore_wait(barrier, count)

    def kv_copy(level, i):
        return pltpu.make_async_remote_copy(
            src_ref=(k_ref, v_ref)[i], dst_ref=kvbuf.at[level, i],
            send_sem=kv_s.at[level, i], recv_sem=kv_r.at[level, i],
            device_id={"kv": me + span(level)}, device_id_type=pl.DeviceIdType.MESH)

    def kv_pass_on(level, i, held_kv):
        to, src = (0, held_kv) if level == 0 else (3, kvbuf.at[2, i])
        return pltpu.make_async_remote_copy(
            src_ref=src, dst_ref=kvbuf.at[to, i],
            send_sem=kv_s.at[to, i], recv_sem=kv_r.at[to, i],
            device_id={"kv": partner if level == 0 else me + dist[2]}, device_id_type=pl.DeviceIdType.MESH)

    def g_copy(level):
        to = jnp.where(level == 0, partner, me - span(level)) if with_dw else me - dist[level]
        return pltpu.make_async_remote_copy(
            src_ref=gsend.at[level], dst_ref=grecv.at[level],
            send_sem=g_s.at[level], recv_sem=g_r.at[level],
            device_id={"kv": to}, device_id_type=pl.DeviceIdType.MESH)

    loads[0].wait()
    loads[1].wait()
    turns = [0, 1, 3, 2]
    if with_dw:
        late = w == 0
        turns = [jnp.where(second, 0, 2), jnp.where(second, 2, jnp.where(late, 0, 1)),
                 jnp.where(second, 1, jnp.where(late, 3, 0)), jnp.where(late, 1, 3)]
    for level in (2, 1) if with_dw else turns:
        @pl.when(me + dist[level] < n)
        def _():
            kv_copy(level, 0).start()
            kv_copy(level, 1).start()

    if with_dw:
        @pl.when(first)
        def _():
            kv_pass_on(0, 0, k_ref).start()
            kv_pass_on(0, 1, v_ref).start()

        def x_copy(idx, k):
            wt, tt = plane[idx]
            zz = order[k]
            off = pl.multiple_of((zz * wn + wt) * rows, rows)
            return pltpu.make_async_remote_copy(
                src_ref=x_ref.at[:, pl.ds(off, rows)],
                dst_ref=xbuf.at[mt * zper + zz, pl.ds(pl.multiple_of(w * tok, tok), tok)],
                send_sem=x_s.at[idx, k], recv_sem=x_r.at[idx, k],
                device_id={"kv": z * wn + wt, "tp": tt}, device_id_type=pl.DeviceIdType.MESH)

        def x_forward(idx, k):
            slot = xbuf.at[mt * zper + order[k], pl.ds(pl.multiple_of(plane[idx][0] * tok, tok), tok)]
            return pltpu.make_async_remote_copy(
                src_ref=slot, dst_ref=slot,
                send_sem=x_s.at[idx + 4, k], recv_sem=x_r.at[idx + 4, k],
                device_id={"kv": me, "tp": 1 - mt}, device_id_type=pl.DeviceIdType.MESH)

        loads[3].wait()
        for k in range(zper):
            for idx in (1, 2, 3, 4, 0):
                x_copy(idx, k).start()
        for zz in range(zper):
            off = pl.multiple_of((zz * wn + w) * rows, rows)
            xbuf[mt * zper + zz, pl.ds(pl.multiple_of(w * tok, tok), tok), :] = x_ref[:, pl.ds(off, rows)]

    for i in range(count_in + 1):
        if i not in (0, 1, 3) or (i == 3 and not with_dw):
            loads[i].wait()
    lse_t = lse_ref[...] * (-LOG2E)
    prod = g_ref[...].astype(F32) * o_ref[...].astype(F32)
    hi = prod.astype(BF)
    lo = (prod - hi.astype(F32)).astype(BF)
    pick = (lax.broadcasted_iota(jnp.int32, (16, qh * DH), 1) // DH
            == lax.broadcasted_iota(jnp.int32, (16, qh * DH), 0)).astype(F32).astype(BF)
    delta_t = dot(pick, hi, NT) + dot(pick, lo, NT)
    for h in range(kvh):
        for g in range(grp):
            i = h * grp + g
            lrow[h, 0:1, g * tok:(g + 1) * tok] = lse_t[i:i + 1, 0:tok]
            drow[h, 0:1, g * tok:(g + 1) * tok] = delta_t[i:i + 1, :]
            qs[h, g * tok:(g + 1) * tok, :] = q_ref[:, i * DH:(i + 1) * DH]
            gs[h, g * tok:(g + 1) * tok, :] = g_ref[:, i * DH:(i + 1) * DH]

    q_block = lax.rem(lax.broadcasted_iota(jnp.int32, (1, cols), 1), tok) // BLOCK

    def run_pass(h, k, v, bias):
        lse = lrow[h, 0:1, :]
        st = dot(k, qs[h], NT) * (scale * LOG2E)
        if bias is None:
            kp = lax.broadcasted_iota(jnp.int32, (tok, cols), 0)
            qp = lax.rem(lax.broadcasted_iota(jnp.int32, (tok, cols), 1), tok)
            keep = (qp >= kp) & ((qp // BLOCK) == (kp // BLOCK))
            p = jnp.exp2(jnp.where(keep, st + lse, NEG))
        else:
            p = jnp.concatenate(
                [jnp.exp2(st[b * BLOCK:(b + 1) * BLOCK] + (lse + bias[b])) for b in range(nb)], axis=0)
        dp = dot(v, gs[h], NT)
        ds = (p * (dp - drow[h, 0:1, :])).astype(BF)
        dv = dot(p.astype(BF), gs[h], NN)
        dk = dot(ds, qs[h], NN) * scale
        dq = dot(k, ds, TN)
        return dq, dk, dv

    for h in range(kvh):
        lanes = slice(h * DH, (h + 1) * DH)
        dq, dk, dv = run_pass(h, k_ref[:, lanes], v_ref[:, lanes], None)
        dqt[h] = dq
        acc[0, :, lanes] = dk
        acc[1, :, lanes] = dv

    def level_bias(level):
        bias = []
        for kb in range(nb):
            row = jnp.full((1, cols), NEG, F32)
            target = (me - span(level)) * nb + kb
            for qb in range(nb):
                hit = jnp.float32(NEG)
                for i in range(PER):
                    hit = jnp.where(ch_ref[PER * level + i, me * nb + qb] == target, jnp.float32(0.0), hit)
                row = jnp.where(q_block == qb, hit, row)
            bias.append(row)
        return bias

    def far_pass(level, h, bias):
        lanes = slice(h * DH, (h + 1) * DH)
        dq, dk, dv = run_pass(h, kvbuf[level, 0, :, lanes], kvbuf[level, 1, :, lanes], bias)
        dqt[h] = dqt[h] + dq
        gsend[level, 0, :, lanes] = dk.astype(BF)
        gsend[level, 1, :, lanes] = dv.astype(BF)

    def wait_kv(level):
        kv_copy(level, 0).wait_recv()
        kv_copy(level, 1).wait_recv()

    def far_level(level):
        bias = level_bias(level)
        for h in range(kvh):
            far_pass(level, h, bias)

    def arrive(level):
        wait_kv(level)
        if with_dw:
            @pl.when((level == 2) & (me + dist[2] < n))
            def _():
                kv_pass_on(3, 0, None).start()
                kv_pass_on(3, 1, None).start()

            @pl.when((level == 1) & second)
            def _():
                kv_pass_on(0, 0, kvbuf.at[1, 0]).start()
                kv_pass_on(0, 1, kvbuf.at[1, 1]).start()

    def return_level(level):
        if with_dw:
            @pl.when(level != 1)
            def _():
                g_copy(level).start()
        else:
            g_copy(level).start()

    def pass_x_on(k):
        for idx in (1, 2):
            x_copy(idx, k).wait_recv()
            x_forward(idx, k).start()

    for turn, level in enumerate(turns[:-1]):
        if with_dw and turn == 2:
            @pl.when((z >= 1) & first)
            def _():
                pass_x_on(0)

        @pl.when(me >= span(level))
        def _():
            arrive(level)
            far_level(level)
            return_level(level)

    if with_dw:
        mine = pl.ds(pl.multiple_of(w * tok, tok), tok)
        hops = list(range(2, wn, 2))

        def a_copy(h, s):
            to = pair if s == 0 else lax.rem(w + s, wn)
            return pltpu.make_async_remote_copy(
                src_ref=dqall.at[h, mine], dst_ref=dqall.at[h, mine],
                send_sem=a_s.at[h, s // 2], recv_sem=a_r.at[h, s // 2],
                device_id={"kv": z * wn + to}, device_id_type=pl.DeviceIdType.MESH)

        def f_copy(h, s):
            slot = pl.ds(pl.multiple_of(lax.rem(w + wn - s, wn) * tok, tok), tok)
            return pltpu.make_async_remote_copy(
                src_ref=dqall.at[h, slot], dst_ref=dqall.at[h, slot],
                send_sem=f_s.at[h, s // 2 - 1], recv_sem=f_r.at[h, s // 2 - 1],
                device_id={"kv": z * wn + pair}, device_id_type=pl.DeviceIdType.MESH)

    if with_dw:
        @pl.when((z >= 2) & second)
        def _():
            pass_x_on(0)

    last = turns[-1]
    for h in range(kvh):
        @pl.when(me >= span(last))
        def _():
            if h == 0:
                arrive(last)
            far_pass(last, h, level_bias(last))
        whole = dqt[h] * scale
        for g in range(grp):
            low = whole[:, g * tok:(g + 1) * tok].T.astype(BF)
            i = h * grp + g
            dq_out[:, i * DH:(i + 1) * DH] = low
            if with_dw:
                dqall[h, mine, g * DH:(g + 1) * DH] = low
        if with_dw:
            for s in hops:
                a_copy(h, s).start()
            a_copy(h, 0).start()

    @pl.when(me >= span(last))
    def _():
        return_level(last)

    def early_sum():
        @pl.when(second)
        def _():
            g_copy(0).wait_recv()
            gsend[1] = (gsend[1].astype(F32) + grecv[0].astype(F32)).astype(BF)

        g_copy(1).start()

    if with_dw:
        @pl.when((z < 1) | ((z < 2) & second))
        def _():
            pass_x_on(0)

        pass_x_on(1)

        @pl.when((me >= dist[1]) & (w < 2))
        def _():
            early_sum()

        def x_arrive(k):
            for idx in (0, 3, 4):
                x_copy(idx, k).wait_recv()
            for idx in (1, 2):
                x_forward(idx, k).wait_recv()

        def w_copy(h, i):
            return pltpu.make_async_remote_copy(
                src_ref=part.at[h, i], dst_ref=precv.at[h, i],
                send_sem=w_s.at[h, i], recv_sem=w_r.at[h, i],
                device_id={"kv": (far if i == 2 else near) * wn + w}, device_id_type=pl.DeviceIdType.MESH)

        for h in range(kvh):
            for s in hops:
                a_copy(h, s).wait_recv()
                f_copy(h, s).start()
            if h == 0:
                x_arrive(0)
                for zz in (lax.rem(near + 2, zn), near):
                    xt[zz] = xbuf[zz].T
            a_copy(h, 0).wait_recv()
            for s in hops:
                f_copy(h, s).wait_recv()
            part[h, 0] = dot(xt[lax.rem(near + 2, zn)], dqall[h], NN).astype(BF)
            w_copy(h, 0).start()
            part[h, 1] = dot(xt[near], dqall[h], NN).astype(BF)
            w_copy(h, 1).start()
        @pl.when(w >= 2)
        def _():
            early_sum()

        x_arrive(1)
        for zz in (far, z):
            xt[zz] = xbuf[zz].T
        for h in range(kvh):
            ours = dot(xt[far], dqall[h], NN)
            w_copy(h, 0).wait_recv()
            part[h, 2] = (ours + precv[h, 0].astype(F32)).astype(BF)
            w_copy(h, 2).start()
        width = grp * DH
        for h in range(kvh):
            dw_out[:, h * width:(h + 1) * width] = dot(xt[z], dqall[h], NN)
        for k in range(zper):
            for idx in range(len(plane)):
                x_copy(idx, k).wait_send()
            for idx in (1, 2):
                x_forward(idx, k).wait_send()
        for h in range(kvh):
            for s in [0] + hops:
                a_copy(h, s).wait_send()
            for s in hops:
                f_copy(h, s).wait_send()

    def add_in(level):
        g_copy(level).wait_recv()
        acc[...] = acc[...] + grecv[level].astype(F32)

    def sent_kv(level):
        kv_copy(level, 0).wait_send()
        kv_copy(level, 1).wait_send()

    if with_dw:
        @pl.when(first)
        def _():
            sent_kv(0)
            add_in(0)

            @pl.when(me >= dist[1])
            def _():
                g_copy(0).wait_send()

        @pl.when(second)
        def _():
            g_copy(0).wait_send()

            @pl.when(me >= dist[1])
            def _():
                sent_kv(0)

        @pl.when((me >= dist[2]) & (me + dist[2] < n))
        def _():
            sent_kv(3)

        for level in (1, 2, 3):
            @pl.when(me + dist[level] < n)
            def _():
                if level < 3:
                    sent_kv(level)
                add_in(level)

            @pl.when(me >= dist[level])
            def _():
                g_copy(level).wait_send()
    else:
        for level, d in enumerate(dist):
            @pl.when(me + d < n)
            def _():
                sent_kv(level)
                add_in(level)

            @pl.when(me >= d)
            def _():
                g_copy(level).wait_send()

    dk_out[...] = acc[0].astype(BF)
    dv_out[...] = acc[1].astype(BF)
    if with_dw:
        for h in range(kvh):
            lanes = slice(h * width, (h + 1) * width)
            w_copy(h, 0).wait_send()
            w_copy(h, 1).wait()
            w_copy(h, 2).wait()
            dw_out[:, lanes] = dw_out[:, lanes] + precv[h, 1].astype(F32) + precv[h, 2].astype(F32)


def writer(*refs):
    count = (len(refs) - 1) // 2
    sem = refs[-1]
    copies = [pltpu.make_async_copy(refs[i], refs[count + i], sem.at[i]) for i in range(count)]
    for copy in copies:
        copy.start()
    for copy in copies:
        copy.wait()


def shards(layer_input, queries, keys, values, attn_out, grad_out, log_sum, chosen):
    n = lax.axis_size("kv")
    tp = lax.axis_size("tp")
    tok, qw = queries.shape
    kw = keys.shape[1]
    kvh, qh = kw // DH, qw // DH
    cols = qh // kvh * tok
    depth = layer_input.shape[1] * tp
    rows = depth // n
    wn = math.isqrt(n)
    zn = n // wn
    with_dw = wn * wn == n and zn == 4 and tp == 2 and rows % 128 == 0
    vm = pl.BlockSpec(memory_space=pltpu.VMEM)
    out_shape = [
        jax.ShapeDtypeStruct((tok, qw), BF),
        jax.ShapeDtypeStruct((tok, kw), BF),
        jax.ShapeDtypeStruct((tok, kw), BF),
    ]
    args = [keys, values, queries, grad_out, attn_out, log_sum.T]
    if with_dw:
        args.insert(3, layer_input)
    scratch = [pltpu.VMEM(a.shape, a.dtype) for a in args] + [
        pltpu.SMEM(chosen.T.shape, chosen.dtype),
        pltpu.SemaphoreType.DMA((len(args) + 1,)),
        pltpu.VMEM((kvh, cols, DH), BF),
        pltpu.VMEM((kvh, cols, DH), BF),
        pltpu.VMEM((kvh, 1, cols), F32),
        pltpu.VMEM((kvh, 1, cols), F32),
        pltpu.VMEM((kvh, DH, cols), F32),
        pltpu.VMEM((2, tok, kw), F32),
        pltpu.VMEM((LEVELS, 2, tok, kw), BF),
        pltpu.VMEM((LEVELS, 2, tok, kw), BF),
        pltpu.VMEM((LEVELS, 2, tok, kw), BF),
        pltpu.SemaphoreType.DMA((LEVELS, 2)),
        pltpu.SemaphoreType.DMA((LEVELS, 2)),
        pltpu.SemaphoreType.DMA((LEVELS,)),
        pltpu.SemaphoreType.DMA((LEVELS,)),
    ]
    hbm = pl.BlockSpec(memory_space=pltpu.HBM)
    specs = [hbm] * (len(args) + 1)
    if with_dw:
        out_shape.append(jax.ShapeDtypeStruct((rows, qw), F32))
        peers = 7
        zper = zn // tp
        scratch += [
            pltpu.VMEM((zn, wn * tok, rows), BF),
            pltpu.VMEM((zn, rows, wn * tok), BF),
            pltpu.VMEM((kvh, wn * tok, qw // kvh), BF),
            pltpu.VMEM((kvh, zn - 1, rows, qw // kvh), BF),
            pltpu.VMEM((kvh, zn - 1, rows, qw // kvh), BF),
            pltpu.SemaphoreType.DMA((peers, zper)),
            pltpu.SemaphoreType.DMA((peers, zper)),
            pltpu.SemaphoreType.DMA((kvh, wn // 2)),
            pltpu.SemaphoreType.DMA((kvh, wn // 2)),
            pltpu.SemaphoreType.DMA((kvh, max(wn // 2 - 1, 1))),
            pltpu.SemaphoreType.DMA((kvh, max(wn // 2 - 1, 1))),
            pltpu.SemaphoreType.DMA((kvh, zn - 1)),
            pltpu.SemaphoreType.DMA((kvh, zn - 1)),
        ]
    outs = pl.pallas_call(
        functools.partial(kernel, (n, tp, with_dw)),
        out_shape=[pltpu.VMEM(a.shape, a.dtype) for a in out_shape],
        in_specs=specs,
        out_specs=[vm] * len(out_shape),
        scratch_shapes=scratch,
        compiler_params=pltpu.CompilerParams(
            collective_id=0, has_side_effects=True, vmem_limit_bytes=66100000),
    )(*args, chosen.T)
    outs = pl.pallas_call(
        writer,
        out_shape=out_shape,
        in_specs=[vm] * len(out_shape),
        out_specs=[hbm] * len(out_shape),
        scratch_shapes=[pltpu.SemaphoreType.DMA((len(out_shape),))],
        compiler_params=pltpu.CompilerParams(vmem_limit_bytes=1024 * 1024),
    )(*outs)
    if with_dw:
        return tuple(outs)
    whole_input = lax.all_gather(layer_input, "tp", axis=1, tiled=True)
    grad_weight = lax.psum_scatter(
        jnp.einsum("td,tc->dc", whole_input, outs[0], preferred_element_type=F32),
        "kv", scatter_dimension=0, tiled=True)
    return tuple(outs) + (grad_weight,)


def solution(mesh):
    spec = P("kv", "tp")
    return jax.shard_map(
        shards,
        mesh=mesh,
        in_specs=(spec,) * 7 + (P(),),
        out_specs=(spec,) * 4,
        check_vma=False,
    )
```

```python
import functools
import math

import jax
import jax.numpy as jnp
from jax import lax
from jax.experimental import pallas as pl
from jax.experimental.pallas import tpu as pltpu
from jax.sharding import PartitionSpec as P

DH = 64
BLOCK = 64
PER = 2
LEVELS = 4
LOG2E = 1.4426950408889634
NEG = -1e30
NT = (((1,), (1,)), ((), ()))
TN = (((0,), (0,)), ((), ()))
NN = (((1,), (0,)), ((), ()))
BF = jnp.bfloat16
F32 = jnp.float32


def dot(a, b, dims):
    return lax.dot_general(a, b, dims, preferred_element_type=F32)


def kernel(cfg, *refs):
    n, tp, with_dw = cfg
    count_in = 7 if with_dw else 6
    hbm, refs = refs[:count_in], refs[count_in:]
    ch_hbm, refs = refs[0], refs[1:]
    count_out = 4 if with_dw else 3
    outs, refs = refs[:count_out], refs[count_out:]
    held, refs = refs[:count_in], refs[count_in:]
    ch_ref, refs = refs[0], refs[1:]
    (in_s, qs, gs, lrow, drow, dqt, acc, kvbuf, gsend, grecv,
     kv_s, kv_r, g_s, g_r) = refs[:14]
    dq_out, dk_out, dv_out = outs[:3]
    k_ref, v_ref, q_ref, g_ref, o_ref, lse_ref = held[:3] + held[-3:]
    if with_dw:
        x_ref = held[3]
        dw_out = outs[3]
        (xbuf, xt, dqall, part, precv, x_s, x_r, a_s, a_r, f_s, f_r, w_s, w_r) = refs[14:]
    loads = [pltpu.make_async_copy(hbm[i], held[i], in_s.at[i]) for i in range(count_in)]
    loads.append(pltpu.make_async_copy(ch_hbm, ch_ref, in_s.at[count_in]))
    for load in loads:
        load.start()
    me = lax.axis_index("kv")
    mt = lax.axis_index("tp")
    tok = q_ref.shape[0]
    kvh = k_ref.shape[1] // DH
    qh = q_ref.shape[1] // DH
    grp = qh // kvh
    nb = tok // BLOCK
    cols = grp * tok
    scale = DH ** -0.5
    dist = [1, n // 8, n // 4, n // 2]

    def span(level):
        if isinstance(level, int):
            return dist[level]
        return jnp.where(level == 0, dist[0], jnp.where(level == 1, dist[1], jnp.where(level == 2, dist[2], dist[3])))

    if with_dw:
        wn = math.isqrt(n)
        zn = n // wn
        zper = zn // tp
        rows = dw_out.shape[0]
        z = me // wn
        w = lax.rem(me, wn)
        pair = w + 1 - 2 * lax.rem(w, 2)
        across = lax.rem(w + 2, wn)
        across_pair = lax.rem(pair + 2, wn)
        near = z + 1 - 2 * lax.rem(z, 2)
        far = lax.rem(z + 2, zn)
        partner = me + 1 - 2 * lax.rem(me, 2)
        first = lax.rem(me, 2) == 0
        second = lax.rem(me, 2) == 1
        order = [1 - lax.rem(z, 2), lax.rem(z, 2)]
        plane = [(pair, mt), (across, mt), (across_pair, mt), (w, 1 - mt), (pair, 1 - mt)]

    barrier = pltpu.get_barrier_semaphore()
    count = jnp.int32(0)
    for d in dist[1:] if with_dw else dist:
        @pl.when(me + d < n)
        def _():
            pl.semaphore_signal(barrier, inc=1, device_id={"kv": me + d}, device_id_type=pl.DeviceIdType.MESH)

        @pl.when(me >= d)
        def _():
            pl.semaphore_signal(barrier, inc=1, device_id={"kv": me - d}, device_id_type=pl.DeviceIdType.MESH)

        count = count + jnp.where(me + d < n, 1, 0) + jnp.where(me >= d, 1, 0)
    if with_dw:
        for wt, tt in plane:
            pl.semaphore_signal(barrier, inc=1, device_id={"kv": z * wn + wt, "tp": tt}, device_id_type=pl.DeviceIdType.MESH)
        for zt in (near, far):
            pl.semaphore_signal(barrier, inc=1, device_id={"kv": zt * wn + w}, device_id_type=pl.DeviceIdType.MESH)
        count = count + len(plane) + 2
    pl.semaphore_wait(barrier, count)

    def kv_copy(level, i):
        return pltpu.make_async_remote_copy(
            src_ref=(k_ref, v_ref)[i], dst_ref=kvbuf.at[level, i],
            send_sem=kv_s.at[level, i], recv_sem=kv_r.at[level, i],
            device_id={"kv": me + span(level)}, device_id_type=pl.DeviceIdType.MESH)

    def kv_pass_on(level, i, held_kv):
        to, src = (0, held_kv) if level == 0 else (3, kvbuf.at[2, i])
        return pltpu.make_async_remote_copy(
            src_ref=src, dst_ref=kvbuf.at[to, i],
            send_sem=kv_s.at[to, i], recv_sem=kv_r.at[to, i],
            device_id={"kv": partner if level == 0 else me + dist[2]}, device_id_type=pl.DeviceIdType.MESH)

    def g_copy(level):
        to = jnp.where(level == 0, partner, me - span(level)) if with_dw else me - dist[level]
        return pltpu.make_async_remote_copy(
            src_ref=gsend.at[level], dst_ref=grecv.at[level],
            send_sem=g_s.at[level], recv_sem=g_r.at[level],
            device_id={"kv": to}, device_id_type=pl.DeviceIdType.MESH)

    loads[0].wait()
    loads[1].wait()
    turns = [0, 1, 3, 2]
    if with_dw:
        late = w == 0
        turns = [jnp.where(second, 0, 2), jnp.where(second, 2, jnp.where(late, 0, 1)),
                 jnp.where(second, 1, jnp.where(late, 3, 0)), jnp.where(late, 1, 3)]
    for level in (2, 1) if with_dw else turns:
        @pl.when(me + dist[level] < n)
        def _():
            kv_copy(level, 0).start()
            kv_copy(level, 1).start()

    if with_dw:
        @pl.when(first)
        def _():
            kv_pass_on(0, 0, k_ref).start()
            kv_pass_on(0, 1, v_ref).start()

        def x_copy(idx, k):
            wt, tt = plane[idx]
            zz = order[k]
            off = pl.multiple_of((zz * wn + wt) * rows, rows)
            return pltpu.make_async_remote_copy(
                src_ref=x_ref.at[:, pl.ds(off, rows)],
                dst_ref=xbuf.at[mt * zper + zz, pl.ds(pl.multiple_of(w * tok, tok), tok)],
                send_sem=x_s.at[idx, k], recv_sem=x_r.at[idx, k],
                device_id={"kv": z * wn + wt, "tp": tt}, device_id_type=pl.DeviceIdType.MESH)

        def x_forward(idx, k):
            slot = xbuf.at[mt * zper + order[k], pl.ds(pl.multiple_of(plane[idx][0] * tok, tok), tok)]
            return pltpu.make_async_remote_copy(
                src_ref=slot, dst_ref=slot,
                send_sem=x_s.at[idx + 4, k], recv_sem=x_r.at[idx + 4, k],
                device_id={"kv": me, "tp": 1 - mt}, device_id_type=pl.DeviceIdType.MESH)

        loads[3].wait()
        for k in range(zper):
            for idx in (1, 2, 3, 4, 0):
                x_copy(idx, k).start()
        for zz in range(zper):
            off = pl.multiple_of((zz * wn + w) * rows, rows)
            xbuf[mt * zper + zz, pl.ds(pl.multiple_of(w * tok, tok), tok), :] = x_ref[:, pl.ds(off, rows)]

    for i in range(count_in + 1):
        if i not in (0, 1, 3) or (i == 3 and not with_dw):
            loads[i].wait()
    lse_t = lse_ref[...] * (-LOG2E)
    prod = g_ref[...].astype(F32) * o_ref[...].astype(F32)
    hi = prod.astype(BF)
    lo = (prod - hi.astype(F32)).astype(BF)
    pick = (lax.broadcasted_iota(jnp.int32, (16, qh * DH), 1) // DH
            == lax.broadcasted_iota(jnp.int32, (16, qh * DH), 0)).astype(F32).astype(BF)
    delta_t = dot(pick, hi, NT) + dot(pick, lo, NT)
    part_cols = grp * BLOCK
    for h in range(kvh):
        for g in range(grp):
            i = h * grp + g
            for qb in range(nb):
                rows_ = slice(qb * BLOCK, (qb + 1) * BLOCK)
                to = slice(qb * part_cols + g * BLOCK, qb * part_cols + (g + 1) * BLOCK)
                lrow[h, 0:1, to] = lse_t[i:i + 1, rows_]
                drow[h, 0:1, to] = delta_t[i:i + 1, rows_]
                qs[h, to, :] = q_ref[rows_, i * DH:(i + 1) * DH]
                gs[h, to, :] = g_ref[rows_, i * DH:(i + 1) * DH]

    def run_pass(h, ks, vs, keep):
        to = [slice(qb * part_cols, (qb + 1) * part_cols) for qb in range(nb)]
        st = [dot(k, qs[h, t, :], NT) for k, t in zip(ks, to)]
        dp = [dot(v, gs[h, t, :], NT) for v, t in zip(vs, to)]
        st = [x * (scale * LOG2E) + lrow[h, 0:1, t] for x, t in zip(st, to)]
        p = [jnp.exp2(x if keep is None else jnp.where(keep, x, NEG)) for x in st]
        ds = [(x * (y - drow[h, 0:1, t])).astype(BF) for x, y, t in zip(p, dp, to)]
        dv = [dot(x.astype(BF), gs[h, t, :], NN) for x, t in zip(p, to)]
        dq = [dot(k, x, TN) for k, x in zip(ks, ds)]
        dk = [dot(x, qs[h, t, :], NN) for x, t in zip(ds, to)]
        return dq, dk, dv

    causal = (lax.rem(lax.broadcasted_iota(jnp.int32, (BLOCK, part_cols), 1), BLOCK)
              >= lax.broadcasted_iota(jnp.int32, (BLOCK, part_cols), 0))
    for h in range(kvh):
        lanes = slice(h * DH, (h + 1) * DH)
        blocks = [slice(qb * BLOCK, (qb + 1) * BLOCK) for qb in range(nb)]
        dq, dk, dv = run_pass(h, [k_ref[r, lanes] for r in blocks], [v_ref[r, lanes] for r in blocks], causal)
        dqt[h] = jnp.concatenate(dq, axis=1)
        acc[0, :, lanes] = jnp.concatenate(dk, axis=0) * scale
        acc[1, :, lanes] = jnp.concatenate(dv, axis=0)

    def picks(level):
        found = []
        for qb in range(nb):
            pair_ = [jnp.clip(ch_ref[PER * level + i, me * nb + qb] - (me - span(level)) * nb, 0, nb - 1)
                     for i in range(PER)]
            found.append((jnp.minimum(*pair_), jnp.maximum(*pair_)))
        return found

    def far_pass(level, h, found):
        lanes = slice(h * DH, (h + 1) * DH)
        ks, vs = [], []
        for i, picked in enumerate((ks, vs)):
            blocks = [kvbuf[level, i, b * BLOCK:(b + 1) * BLOCK, lanes] for b in range(nb)]
            for low, high in found:
                first_, second_ = blocks[0], blocks[1]
                for b in range(1, nb - 1):
                    first_ = jnp.where(low == b, blocks[b], first_)
                for b in range(2, nb):
                    second_ = jnp.where(high == b, blocks[b], second_)
                picked.append(jnp.concatenate([first_, second_], axis=0))
        dq, dk, dv = run_pass(h, ks, vs, None)
        dqt[h] = dqt[h] + jnp.concatenate(dq, axis=1)
        for i, new in enumerate((dk, dv)):
            for b in range(nb):
                total = None
                for qb in range(nb):
                    low, high = found[qb]
                    add = jnp.zeros((BLOCK, DH), F32)
                    if b:
                        add = jnp.where(high == b, new[qb][BLOCK:], add)
                    if b < nb - 1:
                        add = jnp.where(low == b, new[qb][:BLOCK], add)
                    total = add if total is None else total + add
                if i == 0:
                    total = total * scale
                gsend[level, i, b * BLOCK:(b + 1) * BLOCK, lanes] = total.astype(BF)

    def wait_kv(level):
        kv_copy(level, 0).wait_recv()
        kv_copy(level, 1).wait_recv()

    def far_level(level):
        found = picks(level)
        for h in range(kvh):
            far_pass(level, h, found)

    def arrive(level):
        wait_kv(level)
        if with_dw:
            @pl.when((level == 2) & (me + dist[2] < n))
            def _():
                kv_pass_on(3, 0, None).start()
                kv_pass_on(3, 1, None).start()

            @pl.when((level == 1) & second)
            def _():
                kv_pass_on(0, 0, kvbuf.at[1, 0]).start()
                kv_pass_on(0, 1, kvbuf.at[1, 1]).start()

    def return_level(level):
        if with_dw:
            @pl.when(level != 1)
            def _():
                g_copy(level).start()
        else:
            g_copy(level).start()

    def pass_x_on(k):
        for idx in (1, 2):
            x_copy(idx, k).wait_recv()
            x_forward(idx, k).start()

    for turn, level in enumerate(turns[:-1]):
        if with_dw and turn == 2:
            @pl.when((z >= 1) & first)
            def _():
                pass_x_on(0)

        @pl.when(me >= span(level))
        def _():
            arrive(level)
            far_level(level)
            return_level(level)

    if with_dw:
        mine = pl.ds(pl.multiple_of(w * tok, tok), tok)
        hops = list(range(2, wn, 2))

        def a_copy(h, s):
            to = pair if s == 0 else lax.rem(w + s, wn)
            return pltpu.make_async_remote_copy(
                src_ref=dqall.at[h, mine], dst_ref=dqall.at[h, mine],
                send_sem=a_s.at[h, s // 2], recv_sem=a_r.at[h, s // 2],
                device_id={"kv": z * wn + to}, device_id_type=pl.DeviceIdType.MESH)

        def f_copy(h, s):
            slot = pl.ds(pl.multiple_of(lax.rem(w + wn - s, wn) * tok, tok), tok)
            return pltpu.make_async_remote_copy(
                src_ref=dqall.at[h, slot], dst_ref=dqall.at[h, slot],
                send_sem=f_s.at[h, s // 2 - 1], recv_sem=f_r.at[h, s // 2 - 1],
                device_id={"kv": z * wn + pair}, device_id_type=pl.DeviceIdType.MESH)

    if with_dw:
        @pl.when((z >= 2) & second)
        def _():
            pass_x_on(0)

    last = turns[-1]
    for h in range(kvh):
        @pl.when(me >= span(last))
        def _():
            if h == 0:
                arrive(last)
            far_pass(last, h, picks(last))
        whole = (dqt[h] * scale).astype(BF)
        step = 2 if grp % 2 == 0 else 1
        for qb in range(nb):
            for g in range(0, grp, step):
                at = qb * part_cols + g * BLOCK
                low = jnp.concatenate(
                    [whole[:, at + j * BLOCK:at + (j + 1) * BLOCK] for j in range(step)], axis=0).T
                i = h * grp + g
                dq_out[qb * BLOCK:(qb + 1) * BLOCK, i * DH:(i + step) * DH] = low
                if with_dw:
                    at_rows = pl.ds(pl.multiple_of(w * tok + qb * BLOCK, BLOCK), BLOCK)
                    dqall[h, at_rows, g * DH:(g + step) * DH] = low
        if with_dw:
            for s in hops:
                a_copy(h, s).start()
            a_copy(h, 0).start()

    @pl.when(me >= span(last))
    def _():
        return_level(last)

    def early_sum():
        @pl.when(second)
        def _():
            g_copy(0).wait_recv()
            gsend[1] = (gsend[1].astype(F32) + grecv[0].astype(F32)).astype(BF)

        g_copy(1).start()

    if with_dw:
        @pl.when((z < 1) | ((z < 2) & second))
        def _():
            pass_x_on(0)

        pass_x_on(1)

        @pl.when((me >= dist[1]) & (w < 2))
        def _():
            early_sum()

        def x_arrive(k):
            for idx in (0, 3, 4):
                x_copy(idx, k).wait_recv()
            for idx in (1, 2):
                x_forward(idx, k).wait_recv()

        def w_copy(h, i):
            return pltpu.make_async_remote_copy(
                src_ref=part.at[h, i], dst_ref=precv.at[h, i],
                send_sem=w_s.at[h, i], recv_sem=w_r.at[h, i],
                device_id={"kv": (far if i == 2 else near) * wn + w}, device_id_type=pl.DeviceIdType.MESH)

        def send_near(h):
            part[h, 1] = dot(xt[near], dqall[h], NN).astype(BF)
            w_copy(h, 1).start()

        for h in range(kvh):
            for s in hops:
                a_copy(h, s).wait_recv()
                f_copy(h, s).start()
            if h == 0:
                x_arrive(0)
                for zz in (lax.rem(near + 2, zn), near):
                    xt[zz] = xbuf[zz].T
            a_copy(h, 0).wait_recv()
            for s in hops:
                f_copy(h, s).wait_recv()
            part[h, 0] = dot(xt[lax.rem(near + 2, zn)], dqall[h], NN).astype(BF)
            w_copy(h, 0).start()
        @pl.when(w >= 2)
        def _():
            early_sum()

        x_arrive(1)
        for zz in (far, z):
            xt[zz] = xbuf[zz].T
        send_near(0)
        for h in range(kvh):
            ours = dot(xt[far], dqall[h], NN)
            w_copy(h, 0).wait_recv()
            part[h, 2] = (ours + precv[h, 0].astype(F32)).astype(BF)
            w_copy(h, 2).start()
            if h + 1 < kvh:
                send_near(h + 1)
        width = grp * DH
        for h in range(kvh):
            dw_out[:, h * width:(h + 1) * width] = dot(xt[z], dqall[h], NN)
        for k in range(zper):
            for idx in range(len(plane)):
                x_copy(idx, k).wait_send()
            for idx in (1, 2):
                x_forward(idx, k).wait_send()
        for h in range(kvh):
            for s in [0] + hops:
                a_copy(h, s).wait_send()
            for s in hops:
                f_copy(h, s).wait_send()

    def add_in(level):
        g_copy(level).wait_recv()
        acc[...] = acc[...] + grecv[level].astype(F32)

    def sent_kv(level):
        kv_copy(level, 0).wait_send()
        kv_copy(level, 1).wait_send()

    if with_dw:
        @pl.when(first)
        def _():
            sent_kv(0)
            add_in(0)

            @pl.when(me >= dist[1])
            def _():
                g_copy(0).wait_send()

        @pl.when(second)
        def _():
            g_copy(0).wait_send()

            @pl.when(me >= dist[1])
            def _():
                sent_kv(0)

        @pl.when((me >= dist[2]) & (me + dist[2] < n))
        def _():
            sent_kv(3)

        for level in (1, 2, 3):
            @pl.when(me + dist[level] < n)
            def _():
                if level < 3:
                    sent_kv(level)
                add_in(level)

            @pl.when(me >= dist[level])
            def _():
                g_copy(level).wait_send()
    else:
        for level, d in enumerate(dist):
            @pl.when(me + d < n)
            def _():
                sent_kv(level)
                add_in(level)

            @pl.when(me >= d)
            def _():
                g_copy(level).wait_send()

    dk_out[...] = acc[0].astype(BF)
    dv_out[...] = acc[1].astype(BF)
    if with_dw:
        for h in range(kvh):
            lanes = slice(h * width, (h + 1) * width)
            w_copy(h, 0).wait_send()
            w_copy(h, 1).wait()
            w_copy(h, 2).wait()
            dw_out[:, lanes] = dw_out[:, lanes] + precv[h, 1].astype(F32) + precv[h, 2].astype(F32)


def writer(*refs):
    count = (len(refs) - 1) // 2
    sem = refs[-1]
    copies = [pltpu.make_async_copy(refs[i], refs[count + i], sem.at[i]) for i in range(count)]
    for copy in copies:
        copy.start()
    for copy in copies:
        copy.wait()


def shards(layer_input, queries, keys, values, attn_out, grad_out, log_sum, chosen):
    n = lax.axis_size("kv")
    tp = lax.axis_size("tp")
    tok, qw = queries.shape
    kw = keys.shape[1]
    kvh, qh = kw // DH, qw // DH
    cols = qh // kvh * tok
    depth = layer_input.shape[1] * tp
    rows = depth // n
    wn = math.isqrt(n)
    zn = n // wn
    with_dw = wn * wn == n and zn == 4 and tp == 2 and rows % 128 == 0
    vm = pl.BlockSpec(memory_space=pltpu.VMEM)
    out_shape = [
        jax.ShapeDtypeStruct((tok, qw), BF),
        jax.ShapeDtypeStruct((tok, kw), BF),
        jax.ShapeDtypeStruct((tok, kw), BF),
    ]
    args = [keys, values, queries, grad_out, attn_out, log_sum.T]
    if with_dw:
        args.insert(3, layer_input)
    scratch = [pltpu.VMEM(a.shape, a.dtype) for a in args] + [
        pltpu.SMEM(chosen.T.shape, chosen.dtype),
        pltpu.SemaphoreType.DMA((len(args) + 1,)),
        pltpu.VMEM((kvh, cols, DH), BF),
        pltpu.VMEM((kvh, cols, DH), BF),
        pltpu.VMEM((kvh, 1, cols), F32),
        pltpu.VMEM((kvh, 1, cols), F32),
        pltpu.VMEM((kvh, DH, cols), F32),
        pltpu.VMEM((2, tok, kw), F32),
        pltpu.VMEM((LEVELS, 2, tok, kw), BF),
        pltpu.VMEM((LEVELS, 2, tok, kw), BF),
        pltpu.VMEM((LEVELS, 2, tok, kw), BF),
        pltpu.SemaphoreType.DMA((LEVELS, 2)),
        pltpu.SemaphoreType.DMA((LEVELS, 2)),
        pltpu.SemaphoreType.DMA((LEVELS,)),
        pltpu.SemaphoreType.DMA((LEVELS,)),
    ]
    hbm = pl.BlockSpec(memory_space=pltpu.HBM)
    specs = [hbm] * (len(args) + 1)
    if with_dw:
        out_shape.append(jax.ShapeDtypeStruct((rows, qw), F32))
        peers = 7
        zper = zn // tp
        scratch += [
            pltpu.VMEM((zn, wn * tok, rows), BF),
            pltpu.VMEM((zn, rows, wn * tok), BF),
            pltpu.VMEM((kvh, wn * tok, qw // kvh), BF),
            pltpu.VMEM((kvh, zn - 1, rows, qw // kvh), BF),
            pltpu.VMEM((kvh, zn - 1, rows, qw // kvh), BF),
            pltpu.SemaphoreType.DMA((peers, zper)),
            pltpu.SemaphoreType.DMA((peers, zper)),
            pltpu.SemaphoreType.DMA((kvh, wn // 2)),
            pltpu.SemaphoreType.DMA((kvh, wn // 2)),
            pltpu.SemaphoreType.DMA((kvh, max(wn // 2 - 1, 1))),
            pltpu.SemaphoreType.DMA((kvh, max(wn // 2 - 1, 1))),
            pltpu.SemaphoreType.DMA((kvh, zn - 1)),
            pltpu.SemaphoreType.DMA((kvh, zn - 1)),
        ]
    outs = pl.pallas_call(
        functools.partial(kernel, (n, tp, with_dw)),
        out_shape=[pltpu.VMEM(a.shape, a.dtype) for a in out_shape],
        in_specs=specs,
        out_specs=[vm] * len(out_shape),
        scratch_shapes=scratch,
        compiler_params=pltpu.CompilerParams(
            collective_id=0, has_side_effects=True, vmem_limit_bytes=66100000),
    )(*args, chosen.T)
    outs = pl.pallas_call(
        writer,
        out_shape=out_shape,
        in_specs=[vm] * len(out_shape),
        out_specs=[hbm] * len(out_shape),
        scratch_shapes=[pltpu.SemaphoreType.DMA((len(out_shape),))],
        compiler_params=pltpu.CompilerParams(vmem_limit_bytes=1024 * 1024),
    )(*outs)
    if with_dw:
        return tuple(outs)
    whole_input = lax.all_gather(layer_input, "tp", axis=1, tiled=True)
    grad_weight = lax.psum_scatter(
        jnp.einsum("td,tc->dc", whole_input, outs[0], preferred_element_type=F32),
        "kv", scatter_dimension=0, tiled=True)
    return tuple(outs) + (grad_weight,)


def solution(mesh):
    spec = P("kv", "tp")
    return jax.shard_map(
        shards,
        mesh=mesh,
        in_specs=(spec,) * 7 + (P(),),
        out_specs=(spec,) * 4,
        check_vma=False,
    )
```

```python
import functools
import math

import jax
import jax.numpy as jnp
from jax import lax
from jax.experimental import pallas as pl
from jax.experimental.pallas import tpu as pltpu
from jax.sharding import PartitionSpec as P

DH = 64
BLOCK = 64
PER = 2
LEVELS = 4
LOG2E = 1.4426950408889634
NEG = -1e30
NT = (((1,), (1,)), ((), ()))
TN = (((0,), (0,)), ((), ()))
NN = (((1,), (0,)), ((), ()))
BF = jnp.bfloat16
F32 = jnp.float32


def dot(a, b, dims):
    return lax.dot_general(a, b, dims, preferred_element_type=F32)


def kernel(cfg, *refs):
    n, tp, with_dw = cfg
    count_in = 7 if with_dw else 6
    hbm, refs = refs[:count_in], refs[count_in:]
    ch_hbm, refs = refs[0], refs[1:]
    count_out = 4 if with_dw else 3
    outs, refs = refs[:count_out], refs[count_out:]
    kv_ref, qgo, lse_ref, refs = refs[0], refs[1], refs[2], refs[3:]
    if with_dw:
        x_ref, refs = refs[0], refs[1:]
    ch_ref, refs = refs[0], refs[1:]
    (in_s, qs, gs, lrow, drow, dqt, acc, kvbuf, gsend, grecv,
     kv_s, kv_r, g_s, g_r) = refs[:14]
    dq_out, dk_out, dv_out = outs[:3]
    k_ref, v_ref = kv_ref.at[0], kv_ref.at[1]
    q_ref, g_ref, o_ref = qgo.at[0], qgo.at[1], qgo.at[2]
    if with_dw:
        dw_out = outs[3]
        (xbuf, xt, dqall, part, precv, x_s, x_r, a_s, a_r, w_s, w_r) = refs[14:]
    places = [k_ref, v_ref, q_ref, g_ref, o_ref, lse_ref] + ([x_ref] if with_dw else [])
    for i, to in enumerate(places):
        pltpu.make_async_copy(hbm[i], to, in_s.at[(0, 0, 1, 1, 1, 2, 4)[i]]).start()
    pltpu.make_async_copy(ch_hbm, ch_ref, in_s.at[3]).start()

    def drain(ref, sem):
        pltpu.make_async_copy(ref, ref, sem).wait()

    me = lax.axis_index("kv")
    mt = lax.axis_index("tp")
    tok = q_ref.shape[0]
    kvh = k_ref.shape[1] // DH
    qh = q_ref.shape[1] // DH
    grp = qh // kvh
    nb = tok // BLOCK
    cols = grp * tok
    scale = DH ** -0.5
    dist = [1, n // 8, n // 4, n // 2]

    def span(level):
        if isinstance(level, int):
            return dist[level]
        return jnp.where(level == 0, dist[0], jnp.where(level == 1, dist[1], jnp.where(level == 2, dist[2], dist[3])))

    if with_dw:
        wn = math.isqrt(n)
        zn = n // wn
        zper = zn // tp
        rows = dw_out.shape[0]
        z = me // wn
        w = lax.rem(me, wn)
        pair = w + 1 - 2 * lax.rem(w, 2)
        across = lax.rem(w + 2, wn)
        across_pair = lax.rem(pair + 2, wn)
        near = z + 1 - 2 * lax.rem(z, 2)
        far = lax.rem(z + 2, zn)
        outer = (z == 0) | (z == zn - 1)
        inner = (z > 0) & (z < zn - 1)
        to_outer = jnp.where(outer, zn - 1 - z, zn - 1 - near)
        to_inner = jnp.where(outer, zn - 1 - near, zn - 1 - z)
        partner = me + 1 - 2 * lax.rem(me, 2)
        first = lax.rem(me, 2) == 0
        second = lax.rem(me, 2) == 1
        order = [1 - lax.rem(z, 2), lax.rem(z, 2)]
        plane = [(pair, mt), (across, mt), (across_pair, mt), (w, 1 - mt), (pair, 1 - mt)]

    barrier = pltpu.get_barrier_semaphore()
    count = jnp.int32(0)
    for d in dist[1:] if with_dw else dist:
        @pl.when(me + d < n)
        def _():
            pl.semaphore_signal(barrier, inc=1, device_id={"kv": me + d}, device_id_type=pl.DeviceIdType.MESH)

        @pl.when(me >= d)
        def _():
            pl.semaphore_signal(barrier, inc=1, device_id={"kv": me - d}, device_id_type=pl.DeviceIdType.MESH)

        count = count + jnp.where(me + d < n, 1, 0) + jnp.where(me >= d, 1, 0)
    if with_dw:
        for wt, tt in plane:
            pl.semaphore_signal(barrier, inc=1, device_id={"kv": z * wn + wt, "tp": tt}, device_id_type=pl.DeviceIdType.MESH)
        for zt in (near, far):
            pl.semaphore_signal(barrier, inc=1, device_id={"kv": zt * wn + w}, device_id_type=pl.DeviceIdType.MESH)
        count = count + len(plane) + 2
    pl.semaphore_wait(barrier, count)

    def kv_copy(level):
        return pltpu.make_async_remote_copy(
            src_ref=kv_ref, dst_ref=kvbuf.at[level],
            send_sem=kv_s.at[level], recv_sem=kv_r.at[level],
            device_id={"kv": me + span(level)}, device_id_type=pl.DeviceIdType.MESH)

    def kv_pass_on(level, src):
        return pltpu.make_async_remote_copy(
            src_ref=src, dst_ref=kvbuf.at[level],
            send_sem=kv_s.at[level], recv_sem=kv_r.at[level],
            device_id={"kv": partner if level == 0 else me + dist[2]}, device_id_type=pl.DeviceIdType.MESH)

    def g_copy(level):
        to = jnp.where(level == 0, partner, me - span(level)) if with_dw else me - dist[level]
        return pltpu.make_async_remote_copy(
            src_ref=gsend.at[level], dst_ref=grecv.at[level],
            send_sem=g_s.at[level], recv_sem=g_r.at[level],
            device_id={"kv": to}, device_id_type=pl.DeviceIdType.MESH)

    drain(kv_ref, in_s.at[0])
    turns = [0, 1, 3, 2]
    if with_dw:
        late = w == 0
        turns = [jnp.where(second, 0, 2), jnp.where(second, 2, jnp.where(late, 0, 1)),
                 jnp.where(second, 1, jnp.where(late, 3, 0)), jnp.where(late, 1, 3)]
    for level in (2, 1) if with_dw else turns:
        @pl.when(me + dist[level] < n)
        def _():
            kv_copy(level).start()

    if with_dw:
        @pl.when(first)
        def _():
            kv_pass_on(0, kv_ref).start()

        def x_copy(idx, k):
            wt, tt = plane[idx]
            zz = order[k]
            off = pl.multiple_of((zz * wn + wt) * rows, rows)
            return pltpu.make_async_remote_copy(
                src_ref=x_ref.at[:, pl.ds(off, rows)],
                dst_ref=xbuf.at[mt * zper + zz, pl.ds(pl.multiple_of(w * tok, tok), tok)],
                send_sem=x_s.at[0 if idx else 1], recv_sem=x_r.at[k, 0 if idx in (1, 2) else 1],
                device_id={"kv": z * wn + wt, "tp": tt}, device_id_type=pl.DeviceIdType.MESH)

        def x_forward(idx, k):
            slot = xbuf.at[mt * zper + order[k], pl.ds(pl.multiple_of(plane[idx][0] * tok, tok), tok)]
            return pltpu.make_async_remote_copy(
                src_ref=slot, dst_ref=slot,
                send_sem=x_s.at[1], recv_sem=x_r.at[k, 2],
                device_id={"kv": me, "tp": 1 - mt}, device_id_type=pl.DeviceIdType.MESH)

        drain(x_ref, in_s.at[4])
        for k in range(zper):
            for idx in (3, 4, 0) if k else (1, 2, 3, 4, 0):
                x_copy(idx, k).start()
        for zz in range(zper):
            off = pl.multiple_of((zz * wn + w) * rows, rows)
            xbuf[mt * zper + zz, pl.ds(pl.multiple_of(w * tok, tok), tok), :] = x_ref[:, pl.ds(off, rows)]

    drain(qgo, in_s.at[1])
    drain(lse_ref, in_s.at[2])
    pltpu.make_async_copy(ch_hbm, ch_ref, in_s.at[3]).wait()
    lse_t = lse_ref[...] * (-LOG2E)
    prod = g_ref[...].astype(F32) * o_ref[...].astype(F32)
    hi = prod.astype(BF)
    lo = (prod - hi.astype(F32)).astype(BF)
    pick = (lax.broadcasted_iota(jnp.int32, (16, qh * DH), 1) // DH
            == lax.broadcasted_iota(jnp.int32, (16, qh * DH), 0)).astype(F32).astype(BF)
    delta_t = dot(pick, hi, NT) + dot(pick, lo, NT)
    part_cols = grp * BLOCK
    for h in range(kvh):
        for g in range(grp):
            i = h * grp + g
            for qb in range(nb):
                rows_ = slice(qb * BLOCK, (qb + 1) * BLOCK)
                to = slice(qb * part_cols + g * BLOCK, qb * part_cols + (g + 1) * BLOCK)
                lrow[h, 0:1, to] = lse_t[i:i + 1, rows_]
                drow[h, 0:1, to] = delta_t[i:i + 1, rows_]
                qs[h, to, :] = q_ref[rows_, i * DH:(i + 1) * DH]
                gs[h, to, :] = g_ref[rows_, i * DH:(i + 1) * DH]

    def run_pass(h, ks, vs, keep):
        to = [slice(qb * part_cols, (qb + 1) * part_cols) for qb in range(nb)]
        st = [dot(k, qs[h, t, :], NT) for k, t in zip(ks, to)]
        dp = [dot(v, gs[h, t, :], NT) for v, t in zip(vs, to)]
        st = [x * (scale * LOG2E) + lrow[h, 0:1, t] for x, t in zip(st, to)]
        p = [jnp.exp2(x if keep is None else jnp.where(keep, x, NEG)) for x in st]
        ds = [(x * (y - drow[h, 0:1, t])).astype(BF) for x, y, t in zip(p, dp, to)]
        dv = [dot(x.astype(BF), gs[h, t, :], NN) for x, t in zip(p, to)]
        dq = [dot(k, x, TN) for k, x in zip(ks, ds)]
        dk = [dot(x, qs[h, t, :], NN) for x, t in zip(ds, to)]
        return dq, dk, dv

    causal = (lax.rem(lax.broadcasted_iota(jnp.int32, (BLOCK, part_cols), 1), BLOCK)
              >= lax.broadcasted_iota(jnp.int32, (BLOCK, part_cols), 0))
    for h in range(kvh):
        lanes = slice(h * DH, (h + 1) * DH)
        blocks = [slice(qb * BLOCK, (qb + 1) * BLOCK) for qb in range(nb)]
        dq, dk, dv = run_pass(h, [k_ref[r, lanes] for r in blocks], [v_ref[r, lanes] for r in blocks], causal)
        dqt[h] = jnp.concatenate(dq, axis=1)
        acc[0, :, lanes] = jnp.concatenate(dk, axis=0) * scale
        acc[1, :, lanes] = jnp.concatenate(dv, axis=0)

    def picks(level):
        found = []
        for qb in range(nb):
            pair_ = [jnp.clip(ch_ref[PER * level + i, me * nb + qb] - (me - span(level)) * nb, 0, nb - 1)
                     for i in range(PER)]
            found.append((jnp.minimum(*pair_), jnp.maximum(*pair_)))
        return found

    def far_pass(level, h, found):
        lanes = slice(h * DH, (h + 1) * DH)
        ks, vs = [], []
        for i, picked in enumerate((ks, vs)):
            blocks = [kvbuf[level, i, b * BLOCK:(b + 1) * BLOCK, lanes] for b in range(nb)]
            for low, high in found:
                first_, second_ = blocks[0], blocks[1]
                for b in range(1, nb - 1):
                    first_ = jnp.where(low == b, blocks[b], first_)
                for b in range(2, nb):
                    second_ = jnp.where(high == b, blocks[b], second_)
                picked.append(jnp.concatenate([first_, second_], axis=0))
        dq, dk, dv = run_pass(h, ks, vs, None)
        dqt[h] = dqt[h] + jnp.concatenate(dq, axis=1)
        for i, new in enumerate((dk, dv)):
            for b in range(nb):
                total = None
                for qb in range(nb):
                    low, high = found[qb]
                    add = jnp.zeros((BLOCK, DH), F32)
                    if b:
                        add = jnp.where(high == b, new[qb][BLOCK:], add)
                    if b < nb - 1:
                        add = jnp.where(low == b, new[qb][:BLOCK], add)
                    total = add if total is None else total + add
                if i == 0:
                    total = total * scale
                gsend[level, i, b * BLOCK:(b + 1) * BLOCK, lanes] = total.astype(BF)

    def wait_kv(level):
        kv_copy(level).wait_recv()

    def far_level(level):
        found = picks(level)
        for h in range(kvh):
            far_pass(level, h, found)

    def arrive(level):
        wait_kv(level)
        if with_dw:
            @pl.when((level == 2) & (me + dist[2] < n))
            def _():
                kv_pass_on(3, kvbuf.at[2]).start()

            @pl.when((level == 1) & second)
            def _():
                kv_pass_on(0, kvbuf.at[1]).start()

    def return_level(level):
        if with_dw:
            @pl.when(level != 1)
            def _():
                g_copy(level).start()
        else:
            g_copy(level).start()

    def pass_x_on(k):
        drain(xbuf.at[0, 0:2 * tok], x_r.at[k, 0])
        for idx in (1, 2):
            x_forward(idx, k).start()

    for turn, level in enumerate(turns[:-1]):
        if with_dw and turn == 1:
            x_copy(1, 1).start()
            x_copy(2, 1).start()

        if with_dw and turn == 2:
            @pl.when((z >= 1) & first)
            def _():
                pass_x_on(0)

        @pl.when(me >= span(level))
        def _():
            arrive(level)
            far_level(level)
            return_level(level)

    if with_dw:
        mine = pl.ds(pl.multiple_of(w * tok, tok), tok)
        hops = list(range(2, wn, 2))

        def a_copy(h, s):
            to = pair if s == 0 else lax.rem(w + s, wn)
            return pltpu.make_async_remote_copy(
                src_ref=dqall.at[h, mine], dst_ref=dqall.at[h, mine],
                send_sem=a_s, recv_sem=a_r.at[h, s // 2],
                device_id={"kv": z * wn + to}, device_id_type=pl.DeviceIdType.MESH)

        def f_copy(h, s):
            slot = pl.ds(pl.multiple_of(lax.rem(w + wn - s, wn) * tok, tok), tok)
            return pltpu.make_async_remote_copy(
                src_ref=dqall.at[h, slot], dst_ref=dqall.at[h, slot],
                send_sem=a_s, recv_sem=a_r.at[h, 0],
                device_id={"kv": z * wn + pair}, device_id_type=pl.DeviceIdType.MESH)

    if with_dw:
        @pl.when((z >= 2) & second)
        def _():
            pass_x_on(0)

    last = turns[-1]
    for h in range(kvh):
        @pl.when(me >= span(last))
        def _():
            if h == 0:
                arrive(last)
            far_pass(last, h, picks(last))
        whole = (dqt[h] * scale).astype(BF)
        step = 2 if grp % 2 == 0 else 1
        for qb in range(nb):
            for g in range(0, grp, step):
                at = qb * part_cols + g * BLOCK
                low = jnp.concatenate(
                    [whole[:, at + j * BLOCK:at + (j + 1) * BLOCK] for j in range(step)], axis=0).T
                i = h * grp + g
                dq_out[qb * BLOCK:(qb + 1) * BLOCK, i * DH:(i + step) * DH] = low
                if with_dw:
                    at_rows = pl.ds(pl.multiple_of(w * tok + qb * BLOCK, BLOCK), BLOCK)
                    dqall[h, at_rows, g * DH:(g + step) * DH] = low
        if with_dw:
            for s in hops:
                a_copy(h, s).start()
            a_copy(h, 0).start()

    @pl.when(me >= span(last))
    def _():
        return_level(last)

    def early_sum():
        @pl.when(second)
        def _():
            g_copy(0).wait_recv()
            gsend[1] = (gsend[1].astype(F32) + grecv[0].astype(F32)).astype(BF)

        g_copy(1).start()

    if with_dw:
        @pl.when((z < 1) | ((z < 2) & second))
        def _():
            pass_x_on(0)

        pass_x_on(1)

        @pl.when((me >= dist[1]) & (w < 2))
        def _():
            early_sum()

        def x_arrive(k):
            drain(xbuf.at[0, 0:3 * tok], x_r.at[k, 1])
            drain(xbuf.at[0, 0:2 * tok], x_r.at[k, 2])

        def w_copy(h, i, slot, to):
            return pltpu.make_async_remote_copy(
                src_ref=part.at[h, i], dst_ref=precv.at[h, slot],
                send_sem=w_s, recv_sem=w_r.at[h, slot],
                device_id={"kv": to * wn + w}, device_id_type=pl.DeviceIdType.MESH)

        def w_arrive(h, slot):
            w_copy(h, 1, slot, near).wait_recv()

        def send_part(h, i, slot, block, to, add=None):
            new = dot(xt[block], dqall[h], NN)
            if add is not None:
                w_arrive(h, add)
                new = new + precv[h, add].astype(F32)
            part[h, i] = new.astype(BF)
            w_copy(h, i, slot, to).start()

        def across_on(h):
            for s in hops:
                a_copy(h, s).wait_recv()
                f_copy(h, s).start()

        for h in range(kvh):
            if h == 0:
                across_on(h)

                @pl.when(second)
                def _():
                    for later in range(1, kvh):
                        across_on(later)
            else:
                @pl.when(first)
                def _():
                    across_on(h)
            if h < zper:
                x_arrive(h)
                for zz in ((lax.rem(near + 2, zn), near), (far, z))[h]:
                    xt[zz] = xbuf[zz].T
            if h == 1:
                @pl.when(outer)
                def _():
                    send_part(0, 2, 3, to_inner, near)

            drain(dqall.at[h, 0:2 * tok], a_r.at[h, 0])
            @pl.when(outer)
            def _():
                send_part(h, 0, 0, to_outer, near)
                if h:
                    send_part(h, 2, 3, to_inner, near)

            @pl.when(inner)
            def _():
                send_part(h, 1, 1, near, near)

        @pl.when(w >= 2)
        def _():
            early_sum()

        @pl.when(outer)
        def _():
            for h in range(kvh):
                send_part(h, 1, 1, near, near)

        for h in range(kvh):
            @pl.when(inner)
            def _():
                send_part(h, 0, 2, to_outer, to_outer, 0)
                send_part(h, 2, 2, to_inner, to_inner, 3)

        width = grp * DH
        for h in range(kvh):
            dw_out[:, h * width:(h + 1) * width] = dot(xt[z], dqall[h], NN)
        drain(xbuf.at[0:2], x_s.at[0])
        drain(xbuf.at[0:3, 0:2 * tok], x_s.at[1])
        drain(dqall.at[:, 0:3 * tok], a_s)

    def add_in(level):
        g_copy(level).wait_recv()
        acc[...] = acc[...] + grecv[level].astype(F32)

    def sent_kv(level):
        kv_copy(level).wait_send()

    if with_dw:
        @pl.when(first)
        def _():
            sent_kv(0)
            add_in(0)

            @pl.when(me >= dist[1])
            def _():
                g_copy(0).wait_send()

        @pl.when(second)
        def _():
            g_copy(0).wait_send()

            @pl.when(me >= dist[1])
            def _():
                sent_kv(0)

        @pl.when((me >= dist[2]) & (me + dist[2] < n))
        def _():
            sent_kv(3)

        for level in (1, 2, 3):
            @pl.when(me + dist[level] < n)
            def _():
                if level < 3:
                    sent_kv(level)
                add_in(level)

            @pl.when(me >= dist[level])
            def _():
                g_copy(level).wait_send()
    else:
        for level, d in enumerate(dist):
            @pl.when(me + d < n)
            def _():
                sent_kv(level)
                add_in(level)

            @pl.when(me >= d)
            def _():
                g_copy(level).wait_send()

    dk_out[...] = acc[0].astype(BF)
    dv_out[...] = acc[1].astype(BF)
    if with_dw:
        for h in range(kvh):
            lanes = slice(h * width, (h + 1) * width)
            w_arrive(h, 1)
            w_arrive(h, 2)
            dw_out[:, lanes] = dw_out[:, lanes] + precv[h, 1].astype(F32) + precv[h, 2].astype(F32)
        drain(part, w_s)


def writer(*refs):
    count = (len(refs) - 1) // 2
    sem = refs[-1]
    copies = [pltpu.make_async_copy(refs[i], refs[count + i], sem.at[i]) for i in range(count)]
    for copy in copies:
        copy.start()
    for copy in copies:
        copy.wait()


def shards(layer_input, queries, keys, values, attn_out, grad_out, log_sum, chosen):
    n = lax.axis_size("kv")
    tp = lax.axis_size("tp")
    tok, qw = queries.shape
    kw = keys.shape[1]
    kvh, qh = kw // DH, qw // DH
    cols = qh // kvh * tok
    depth = layer_input.shape[1] * tp
    rows = depth // n
    wn = math.isqrt(n)
    zn = n // wn
    with_dw = wn * wn == n and zn == 4 and tp == 2 and rows % 128 == 0
    vm = pl.BlockSpec(memory_space=pltpu.VMEM)
    out_shape = [
        jax.ShapeDtypeStruct((tok, qw), BF),
        jax.ShapeDtypeStruct((tok, kw), BF),
        jax.ShapeDtypeStruct((tok, kw), BF),
    ]
    args = [keys, values, queries, grad_out, attn_out, log_sum.T]
    if with_dw:
        args.append(layer_input)
    held = [((2, tok, kw), BF), ((3, tok, qw), BF)] + [(a.shape, a.dtype) for a in args[5:]]
    scratch = [pltpu.VMEM(*a) for a in held] + [
        pltpu.SMEM(chosen.T.shape, chosen.dtype),
        pltpu.SemaphoreType.DMA((5,)),
        pltpu.VMEM((kvh, cols, DH), BF),
        pltpu.VMEM((kvh, cols, DH), BF),
        pltpu.VMEM((kvh, 1, cols), F32),
        pltpu.VMEM((kvh, 1, cols), F32),
        pltpu.VMEM((kvh, DH, cols), F32),
        pltpu.VMEM((2, tok, kw), F32),
        pltpu.VMEM((LEVELS, 2, tok, kw), BF),
        pltpu.VMEM((LEVELS, 2, tok, kw), BF),
        pltpu.VMEM((LEVELS, 2, tok, kw), BF),
        pltpu.SemaphoreType.DMA((LEVELS,)),
        pltpu.SemaphoreType.DMA((LEVELS,)),
        pltpu.SemaphoreType.DMA((LEVELS,)),
        pltpu.SemaphoreType.DMA((LEVELS,)),
    ]
    hbm = pl.BlockSpec(memory_space=pltpu.HBM)
    specs = [hbm] * (len(args) + 1)
    if with_dw:
        out_shape.append(jax.ShapeDtypeStruct((rows, qw), F32))
        zper = zn // tp
        scratch += [
            pltpu.VMEM((zn, wn * tok, rows), BF),
            pltpu.VMEM((zn, rows, wn * tok), BF),
            pltpu.VMEM((kvh, wn * tok, qw // kvh), BF),
            pltpu.VMEM((kvh, zn - 1, rows, qw // kvh), BF),
            pltpu.VMEM((kvh, zn, rows, qw // kvh), BF),
            pltpu.SemaphoreType.DMA((2,)),
            pltpu.SemaphoreType.DMA((zper, 3)),
            pltpu.SemaphoreType.DMA,
            pltpu.SemaphoreType.DMA((kvh, 2)),
            pltpu.SemaphoreType.DMA,
            pltpu.SemaphoreType.DMA((kvh, zn)),
        ]
    outs = pl.pallas_call(
        functools.partial(kernel, (n, tp, with_dw)),
        out_shape=[pltpu.VMEM(a.shape, a.dtype) for a in out_shape],
        in_specs=specs,
        out_specs=[vm] * len(out_shape),
        scratch_shapes=scratch,
        compiler_params=pltpu.CompilerParams(
            collective_id=0, has_side_effects=True, vmem_limit_bytes=66100000),
    )(*args, chosen.T)
    outs = pl.pallas_call(
        writer,
        out_shape=out_shape,
        in_specs=[vm] * len(out_shape),
        out_specs=[hbm] * len(out_shape),
        scratch_shapes=[pltpu.SemaphoreType.DMA((len(out_shape),))],
        compiler_params=pltpu.CompilerParams(vmem_limit_bytes=1024 * 1024),
    )(*outs)
    if with_dw:
        return tuple(outs)
    whole_input = lax.all_gather(layer_input, "tp", axis=1, tiled=True)
    grad_weight = lax.psum_scatter(
        jnp.einsum("td,tc->dc", whole_input, outs[0], preferred_element_type=F32),
        "kv", scatter_dimension=0, tiled=True)
    return tuple(outs) + (grad_weight,)


def solution(mesh):
    spec = P("kv", "tp")
    return jax.shard_map(
        shards,
        mesh=mesh,
        in_specs=(spec,) * 7 + (P(),),
        out_specs=(spec,) * 4,
        check_vma=False,
    )
```

```python
import functools
import math

import jax
import jax.numpy as jnp
from jax import lax
from jax.experimental import pallas as pl
from jax.experimental.pallas import tpu as pltpu
from jax.sharding import PartitionSpec as P

DH = 64
BLOCK = 64
PER = 2
LEVELS = 4
LOG2E = 1.4426950408889634
NEG = -1e30
NT = (((1,), (1,)), ((), ()))
TN = (((0,), (0,)), ((), ()))
NN = (((1,), (0,)), ((), ()))
BF = jnp.bfloat16
F32 = jnp.float32


def dot(a, b, dims):
    return lax.dot_general(a, b, dims, preferred_element_type=F32)


def kernel(cfg, *refs):
    n, tp, with_dw = cfg
    count_in = 7 if with_dw else 6
    hbm, refs = refs[:count_in], refs[count_in:]
    ch_hbm, refs = refs[0], refs[1:]
    count_out = 4 if with_dw else 3
    outs, refs = refs[:count_out], refs[count_out:]
    kv_ref, qgo, lse_ref, refs = refs[0], refs[1], refs[2], refs[3:]
    if with_dw:
        x_ref, refs = refs[0], refs[1:]
    ch_ref, refs = refs[0], refs[1:]
    (in_s, qs, gs, lrow, drow, dqt, acc, kvbuf, gsend, grecv,
     kv_s, kv_r, g_s, g_r) = refs[:14]
    dq_out, dk_out, dv_out = outs[:3]
    k_ref, v_ref = kv_ref.at[0], kv_ref.at[1]
    q_ref, g_ref, o_ref = qgo.at[0], qgo.at[1], qgo.at[2]
    if with_dw:
        dw_out = outs[3]
        (xbuf, xt, dqall, part, precv, x_s, x_r, a_s, a_r, w_s, w_r) = refs[14:]
    places = [k_ref, v_ref, q_ref, g_ref, o_ref, lse_ref] + ([x_ref] if with_dw else [])
    for i, to in enumerate(places):
        pltpu.make_async_copy(hbm[i], to, in_s.at[(0, 0, 1, 1, 1, 2, 4)[i]]).start()
    pltpu.make_async_copy(ch_hbm, ch_ref, in_s.at[3]).start()

    def drain(ref, sem):
        pltpu.make_async_copy(ref, ref, sem).wait()

    me = lax.axis_index("kv")
    mt = lax.axis_index("tp")
    tok = q_ref.shape[0]
    kvh = k_ref.shape[1] // DH
    qh = q_ref.shape[1] // DH
    grp = qh // kvh
    nb = tok // BLOCK
    cols = grp * tok
    scale = DH ** -0.5
    dist = [1, n // 8, n // 4, n // 2]

    def span(level):
        if isinstance(level, int):
            return dist[level]
        return jnp.where(level == 0, dist[0], jnp.where(level == 1, dist[1], jnp.where(level == 2, dist[2], dist[3])))

    if with_dw:
        wn = math.isqrt(n)
        zn = n // wn
        zper = zn // tp
        rows = dw_out.shape[0]
        z = me // wn
        w = lax.rem(me, wn)
        pair = w + 1 - 2 * lax.rem(w, 2)
        across = lax.rem(w + 2, wn)
        across_pair = lax.rem(pair + 2, wn)
        near = z + 1 - 2 * lax.rem(z, 2)
        far = lax.rem(z + 2, zn)
        outer = (z == 0) | (z == zn - 1)
        inner = (z > 0) & (z < zn - 1)
        to_outer = jnp.where(outer, zn - 1 - z, zn - 1 - near)
        to_inner = jnp.where(outer, zn - 1 - near, zn - 1 - z)
        partner = me + 1 - 2 * lax.rem(me, 2)
        first = lax.rem(me, 2) == 0
        second = lax.rem(me, 2) == 1
        order = [1 - lax.rem(z, 2), lax.rem(z, 2)]
        plane = [(pair, mt), (across, mt), (across_pair, mt), (w, 1 - mt), (pair, 1 - mt)]

    barrier = pltpu.get_barrier_semaphore()
    count = jnp.int32(0)
    for d in dist[1:] if with_dw else dist:
        @pl.when(me + d < n)
        def _():
            pl.semaphore_signal(barrier, inc=1, device_id={"kv": me + d}, device_id_type=pl.DeviceIdType.MESH)

        @pl.when(me >= d)
        def _():
            pl.semaphore_signal(barrier, inc=1, device_id={"kv": me - d}, device_id_type=pl.DeviceIdType.MESH)

        count = count + jnp.where(me + d < n, 1, 0) + jnp.where(me >= d, 1, 0)
    if with_dw:
        for wt, tt in plane:
            pl.semaphore_signal(barrier, inc=1, device_id={"kv": z * wn + wt, "tp": tt}, device_id_type=pl.DeviceIdType.MESH)
        for zt in (near, far):
            pl.semaphore_signal(barrier, inc=1, device_id={"kv": zt * wn + w}, device_id_type=pl.DeviceIdType.MESH)
        count = count + len(plane) + 2
    pl.semaphore_wait(barrier, count)

    def kv_copy(level):
        return pltpu.make_async_remote_copy(
            src_ref=kv_ref, dst_ref=kvbuf.at[level],
            send_sem=kv_s.at[level], recv_sem=kv_r.at[level],
            device_id={"kv": me + span(level)}, device_id_type=pl.DeviceIdType.MESH)

    def kv_pass_on(level, src):
        return pltpu.make_async_remote_copy(
            src_ref=src, dst_ref=kvbuf.at[level],
            send_sem=kv_s.at[level], recv_sem=kv_r.at[level],
            device_id={"kv": partner if level == 0 else me + dist[2]}, device_id_type=pl.DeviceIdType.MESH)

    def g_copy(level):
        to = jnp.where(level == 0, partner, me - span(level)) if with_dw else me - dist[level]
        return pltpu.make_async_remote_copy(
            src_ref=gsend.at[level], dst_ref=grecv.at[level],
            send_sem=g_s.at[level], recv_sem=g_r.at[level],
            device_id={"kv": to}, device_id_type=pl.DeviceIdType.MESH)

    drain(kv_ref, in_s.at[0])
    turns = [0, 1, 3, 2]
    if with_dw:
        late = w == 0
        turns = [jnp.where(second, 0, 2), jnp.where(second, 2, jnp.where(late, 0, 1)),
                 jnp.where(second, 1, jnp.where(late, 3, 0)), jnp.where(late, 1, 3)]
    for level in (2, 1) if with_dw else turns:
        @pl.when(me + dist[level] < n)
        def _():
            kv_copy(level).start()

    if with_dw:
        @pl.when(first)
        def _():
            kv_pass_on(0, kv_ref).start()

        def x_copy(idx, k):
            wt, tt = plane[idx]
            zz = order[k]
            off = pl.multiple_of((zz * wn + wt) * rows, rows)
            return pltpu.make_async_remote_copy(
                src_ref=x_ref.at[:, pl.ds(off, rows)],
                dst_ref=xbuf.at[mt * zper + zz, pl.ds(pl.multiple_of(w * tok, tok), tok)],
                send_sem=x_s.at[0 if idx else 1], recv_sem=x_r.at[k, 0 if idx in (1, 2) else 1],
                device_id={"kv": z * wn + wt, "tp": tt}, device_id_type=pl.DeviceIdType.MESH)

        def x_forward(idx, k):
            slot = xbuf.at[mt * zper + order[k], pl.ds(pl.multiple_of(plane[idx][0] * tok, tok), tok)]
            return pltpu.make_async_remote_copy(
                src_ref=slot, dst_ref=slot,
                send_sem=x_s.at[1], recv_sem=x_r.at[k, 2],
                device_id={"kv": me, "tp": 1 - mt}, device_id_type=pl.DeviceIdType.MESH)

        drain(x_ref, in_s.at[4])
        for k in range(zper):
            for idx in (3, 4, 0) if k else (1, 2, 3, 4, 0):
                x_copy(idx, k).start()
        for zz in range(zper):
            off = pl.multiple_of((zz * wn + w) * rows, rows)
            xbuf[mt * zper + zz, pl.ds(pl.multiple_of(w * tok, tok), tok), :] = x_ref[:, pl.ds(off, rows)]

    drain(qgo, in_s.at[1])
    drain(lse_ref, in_s.at[2])
    pltpu.make_async_copy(ch_hbm, ch_ref, in_s.at[3]).wait()
    lse_t = lse_ref[...] * (-LOG2E)
    prod = g_ref[...].astype(F32) * o_ref[...].astype(F32)
    hi = prod.astype(BF)
    lo = (prod - hi.astype(F32)).astype(BF)
    pick = (lax.broadcasted_iota(jnp.int32, (16, qh * DH), 1) // DH
            == lax.broadcasted_iota(jnp.int32, (16, qh * DH), 0)).astype(F32).astype(BF)
    delta_t = dot(pick, hi, NT) + dot(pick, lo, NT)
    part_cols = grp * BLOCK
    for h in range(kvh):
        for g in range(grp):
            i = h * grp + g
            for qb in range(nb):
                rows_ = slice(qb * BLOCK, (qb + 1) * BLOCK)
                to = slice(qb * part_cols + g * BLOCK, qb * part_cols + (g + 1) * BLOCK)
                lrow[h, 0:1, to] = lse_t[i:i + 1, rows_]
                drow[h, 0:1, to] = delta_t[i:i + 1, rows_]
                qs[h, to, :] = q_ref[rows_, i * DH:(i + 1) * DH]
                gs[h, to, :] = g_ref[rows_, i * DH:(i + 1) * DH]

    def run_pass(heads, ks, vs, keep):
        to = [slice(qb * part_cols, (qb + 1) * part_cols) for qb in range(nb)]
        each = [(h, t, k, v) for h, hk, hv in zip(heads, ks, vs) for t, k, v in zip(to, hk, hv)]
        st = [dot(k, qs[h, t, :], NT) for h, t, k, v in each]
        dp = [dot(v, gs[h, t, :], NT) for h, t, k, v in each]
        st = [x * (scale * LOG2E) + lrow[h, 0:1, t] for x, (h, t, k, v) in zip(st, each)]
        p = [jnp.exp2(x if keep is None else jnp.where(keep, x, NEG)) for x in st]
        ds = [(x * (y - drow[h, 0:1, t])).astype(BF) for x, y, (h, t, k, v) in zip(p, dp, each)]
        dv = [dot(x.astype(BF), gs[h, t, :], NN) for x, (h, t, k, v) in zip(p, each)]
        dq = [dot(k, x, TN) for x, (h, t, k, v) in zip(ds, each)]
        dk = [dot(x, qs[h, t, :], NN) for x, (h, t, k, v) in zip(ds, each)]
        return [(dq[i * nb:(i + 1) * nb], dk[i * nb:(i + 1) * nb], dv[i * nb:(i + 1) * nb]) for i in range(len(heads))]

    causal = (lax.rem(lax.broadcasted_iota(jnp.int32, (BLOCK, part_cols), 1), BLOCK)
              >= lax.broadcasted_iota(jnp.int32, (BLOCK, part_cols), 0))
    blocks = [slice(qb * BLOCK, (qb + 1) * BLOCK) for qb in range(nb)]
    lanes_of = [slice(h * DH, (h + 1) * DH) for h in range(kvh)]
    own = run_pass(list(range(kvh)), [[k_ref[r, l] for r in blocks] for l in lanes_of],
                   [[v_ref[r, l] for r in blocks] for l in lanes_of], causal)
    for h, (dq, dk, dv) in enumerate(own):
        dqt[h] = jnp.concatenate(dq, axis=1)
        acc[0, :, lanes_of[h]] = jnp.concatenate(dk, axis=0) * scale
        acc[1, :, lanes_of[h]] = jnp.concatenate(dv, axis=0)

    def picks(level):
        found = []
        for qb in range(nb):
            pair_ = [jnp.clip(ch_ref[PER * level + i, me * nb + qb] - (me - span(level)) * nb, 0, nb - 1)
                     for i in range(PER)]
            found.append((jnp.minimum(*pair_), jnp.maximum(*pair_)))
        return found

    def far_pass(level, heads, found):
        ks, vs = [], []
        for i, picked in enumerate((ks, vs)):
            for h in heads:
                blocks = [kvbuf[level, i, b * BLOCK:(b + 1) * BLOCK, lanes_of[h]] for b in range(nb)]
                chosen_blocks = []
                for low, high in found:
                    first_, second_ = blocks[0], blocks[1]
                    for b in range(1, nb - 1):
                        first_ = jnp.where(low == b, blocks[b], first_)
                    for b in range(2, nb):
                        second_ = jnp.where(high == b, blocks[b], second_)
                    chosen_blocks.append(jnp.concatenate([first_, second_], axis=0))
                picked.append(chosen_blocks)
        for h, (dq, dk, dv) in zip(heads, run_pass(heads, ks, vs, None)):
            dqt[h] = dqt[h] + jnp.concatenate(dq, axis=1)
            for i, new in enumerate((dk, dv)):
                for b in range(nb):
                    total = None
                    for qb in range(nb):
                        low, high = found[qb]
                        add = jnp.zeros((BLOCK, DH), F32)
                        if b:
                            add = jnp.where(high == b, new[qb][BLOCK:], add)
                        if b < nb - 1:
                            add = jnp.where(low == b, new[qb][:BLOCK], add)
                        total = add if total is None else total + add
                    if i == 0:
                        total = total * scale
                    gsend[level, i, b * BLOCK:(b + 1) * BLOCK, lanes_of[h]] = total.astype(BF)

    def wait_kv(level):
        kv_copy(level).wait_recv()

    def far_level(level):
        found = picks(level)
        far_pass(level, list(range(kvh)), found)

    def arrive(level):
        wait_kv(level)
        if with_dw:
            @pl.when((level == 2) & (me + dist[2] < n))
            def _():
                kv_pass_on(3, kvbuf.at[2]).start()

            @pl.when((level == 1) & second)
            def _():
                kv_pass_on(0, kvbuf.at[1]).start()

    def return_level(level):
        if with_dw:
            @pl.when(level != 1)
            def _():
                g_copy(level).start()
        else:
            g_copy(level).start()

    def pass_x_on(k):
        drain(xbuf.at[0, 0:2 * tok], x_r.at[k, 0])
        for idx in (1, 2):
            x_forward(idx, k).start()

    for turn, level in enumerate(turns[:-1]):
        if with_dw and turn == 1:
            x_copy(1, 1).start()
            x_copy(2, 1).start()

        if with_dw and turn == 2:
            @pl.when((z >= 1) & first)
            def _():
                pass_x_on(0)

        @pl.when(me >= span(level))
        def _():
            arrive(level)
            far_level(level)
            return_level(level)

    if with_dw:
        mine = pl.ds(pl.multiple_of(w * tok, tok), tok)
        hops = list(range(2, wn, 2))

        def a_copy(h, s):
            to = pair if s == 0 else lax.rem(w + s, wn)
            return pltpu.make_async_remote_copy(
                src_ref=dqall.at[h, mine], dst_ref=dqall.at[h, mine],
                send_sem=a_s, recv_sem=a_r.at[h, s // 2],
                device_id={"kv": z * wn + to}, device_id_type=pl.DeviceIdType.MESH)

        def f_copy(h, s):
            slot = pl.ds(pl.multiple_of(lax.rem(w + wn - s, wn) * tok, tok), tok)
            return pltpu.make_async_remote_copy(
                src_ref=dqall.at[h, slot], dst_ref=dqall.at[h, slot],
                send_sem=a_s, recv_sem=a_r.at[h, 0],
                device_id={"kv": z * wn + pair}, device_id_type=pl.DeviceIdType.MESH)

    if with_dw:
        @pl.when((z >= 2) & second)
        def _():
            pass_x_on(0)

    last = turns[-1]
    for h in range(kvh):
        @pl.when(me >= span(last))
        def _():
            if h == 0:
                arrive(last)
            far_pass(last, [h], picks(last))
        whole = (dqt[h] * scale).astype(BF)
        step = 2 if grp % 2 == 0 else 1
        for qb in range(nb):
            for g in range(0, grp, step):
                at = qb * part_cols + g * BLOCK
                low = jnp.concatenate(
                    [whole[:, at + j * BLOCK:at + (j + 1) * BLOCK] for j in range(step)], axis=0).T
                i = h * grp + g
                dq_out[qb * BLOCK:(qb + 1) * BLOCK, i * DH:(i + step) * DH] = low
                if with_dw:
                    at_rows = pl.ds(pl.multiple_of(w * tok + qb * BLOCK, BLOCK), BLOCK)
                    dqall[h, at_rows, g * DH:(g + step) * DH] = low
        if with_dw:
            for s in hops:
                a_copy(h, s).start()
            a_copy(h, 0).start()

    @pl.when(me >= span(last))
    def _():
        return_level(last)

    def early_sum():
        @pl.when(second)
        def _():
            g_copy(0).wait_recv()
            gsend[1] = (gsend[1].astype(F32) + grecv[0].astype(F32)).astype(BF)

        g_copy(1).start()

    if with_dw:
        @pl.when((z < 1) | ((z < 2) & second))
        def _():
            pass_x_on(0)

        pass_x_on(1)

        @pl.when((me >= dist[1]) & (w < 2))
        def _():
            early_sum()

        def x_arrive(k):
            drain(xbuf.at[0, 0:3 * tok], x_r.at[k, 1])
            drain(xbuf.at[0, 0:2 * tok], x_r.at[k, 2])

        def w_copy(h, i, slot, to):
            return pltpu.make_async_remote_copy(
                src_ref=part.at[h, i], dst_ref=precv.at[h, slot],
                send_sem=w_s, recv_sem=w_r.at[h, slot],
                device_id={"kv": to * wn + w}, device_id_type=pl.DeviceIdType.MESH)

        def w_arrive(h, slot):
            w_copy(h, 1, slot, near).wait_recv()

        def send_part(h, i, slot, block, to, add=None):
            new = dot(xt[block], dqall[h], NN)
            if add is not None:
                w_arrive(h, add)
                new = new + precv[h, add].astype(F32)
            part[h, i] = new.astype(BF)
            w_copy(h, i, slot, to).start()

        def across_on(h):
            for s in hops:
                a_copy(h, s).wait_recv()
                f_copy(h, s).start()

        for h in range(kvh):
            if h == 0:
                across_on(h)

                @pl.when(second)
                def _():
                    for later in range(1, kvh):
                        across_on(later)
            else:
                @pl.when(first)
                def _():
                    across_on(h)
            if h < zper:
                x_arrive(h)
                for zz in ((lax.rem(near + 2, zn), near), (far, z))[h]:
                    xt[zz] = xbuf[zz].T
            drain(dqall.at[h, 0:2 * tok], a_r.at[h, 0])
            @pl.when(outer)
            def _():
                send_part(h, 0, 0, to_outer, near)
                if h:
                    for each in range(kvh):
                        send_part(each, 2, 3, to_inner, near)

            @pl.when(inner)
            def _():
                send_part(h, 1, 1, near, near)

        @pl.when(w >= 2)
        def _():
            early_sum()

        @pl.when(outer)
        def _():
            for h in range(kvh):
                send_part(h, 1, 1, near, near)

        @pl.when(inner)
        def _():
            for h in range(kvh):
                send_part(h, 0, 2, to_outer, to_outer, 0)
            for h in range(kvh):
                send_part(h, 2, 2, to_inner, to_inner, 3)

        width = grp * DH
        for h in range(kvh):
            dw_out[:, h * width:(h + 1) * width] = dot(xt[z], dqall[h], NN)
        drain(xbuf.at[0:2], x_s.at[0])
        drain(xbuf.at[0:3, 0:2 * tok], x_s.at[1])
        drain(dqall.at[:, 0:3 * tok], a_s)

    def add_in(level):
        g_copy(level).wait_recv()
        acc[...] = acc[...] + grecv[level].astype(F32)

    def sent_kv(level):
        kv_copy(level).wait_send()

    if with_dw:
        @pl.when(first)
        def _():
            sent_kv(0)
            add_in(0)

            @pl.when(me >= dist[1])
            def _():
                g_copy(0).wait_send()

        @pl.when(second)
        def _():
            g_copy(0).wait_send()

            @pl.when(me >= dist[1])
            def _():
                sent_kv(0)

        @pl.when((me >= dist[2]) & (me + dist[2] < n))
        def _():
            sent_kv(3)

        for level in (1, 2, 3):
            @pl.when(me + dist[level] < n)
            def _():
                if level < 3:
                    sent_kv(level)
                add_in(level)

            @pl.when(me >= dist[level])
            def _():
                g_copy(level).wait_send()
    else:
        for level, d in enumerate(dist):
            @pl.when(me + d < n)
            def _():
                sent_kv(level)
                add_in(level)

            @pl.when(me >= d)
            def _():
                g_copy(level).wait_send()

    dk_out[...] = acc[0].astype(BF)
    dv_out[...] = acc[1].astype(BF)
    if with_dw:
        for h in range(kvh):
            lanes = slice(h * width, (h + 1) * width)
            w_arrive(h, 1)
            w_arrive(h, 2)
            dw_out[:, lanes] = dw_out[:, lanes] + precv[h, 1].astype(F32) + precv[h, 2].astype(F32)
        drain(part, w_s)


def writer(*refs):
    count = (len(refs) - 1) // 2
    sem = refs[-1]
    copies = [pltpu.make_async_copy(refs[i], refs[count + i], sem.at[i]) for i in range(count)]
    for copy in copies:
        copy.start()
    for copy in copies:
        copy.wait()


def shards(layer_input, queries, keys, values, attn_out, grad_out, log_sum, chosen):
    n = lax.axis_size("kv")
    tp = lax.axis_size("tp")
    tok, qw = queries.shape
    kw = keys.shape[1]
    kvh, qh = kw // DH, qw // DH
    cols = qh // kvh * tok
    depth = layer_input.shape[1] * tp
    rows = depth // n
    wn = math.isqrt(n)
    zn = n // wn
    with_dw = wn * wn == n and zn == 4 and tp == 2 and rows % 128 == 0
    vm = pl.BlockSpec(memory_space=pltpu.VMEM)
    out_shape = [
        jax.ShapeDtypeStruct((tok, qw), BF),
        jax.ShapeDtypeStruct((tok, kw), BF),
        jax.ShapeDtypeStruct((tok, kw), BF),
    ]
    args = [keys, values, queries, grad_out, attn_out, log_sum.T]
    if with_dw:
        args.append(layer_input)
    held = [((2, tok, kw), BF), ((3, tok, qw), BF)] + [(a.shape, a.dtype) for a in args[5:]]
    scratch = [pltpu.VMEM(*a) for a in held] + [
        pltpu.SMEM(chosen.T.shape, chosen.dtype),
        pltpu.SemaphoreType.DMA((5,)),
        pltpu.VMEM((kvh, cols, DH), BF),
        pltpu.VMEM((kvh, cols, DH), BF),
        pltpu.VMEM((kvh, 1, cols), F32),
        pltpu.VMEM((kvh, 1, cols), F32),
        pltpu.VMEM((kvh, DH, cols), F32),
        pltpu.VMEM((2, tok, kw), F32),
        pltpu.VMEM((LEVELS, 2, tok, kw), BF),
        pltpu.VMEM((LEVELS, 2, tok, kw), BF),
        pltpu.VMEM((LEVELS, 2, tok, kw), BF),
        pltpu.SemaphoreType.DMA((LEVELS,)),
        pltpu.SemaphoreType.DMA((LEVELS,)),
        pltpu.SemaphoreType.DMA((LEVELS,)),
        pltpu.SemaphoreType.DMA((LEVELS,)),
    ]
    hbm = pl.BlockSpec(memory_space=pltpu.HBM)
    specs = [hbm] * (len(args) + 1)
    if with_dw:
        out_shape.append(jax.ShapeDtypeStruct((rows, qw), F32))
        zper = zn // tp
        scratch += [
            pltpu.VMEM((zn, wn * tok, rows), BF),
            pltpu.VMEM((zn, rows, wn * tok), BF),
            pltpu.VMEM((kvh, wn * tok, qw // kvh), BF),
            pltpu.VMEM((kvh, zn - 1, rows, qw // kvh), BF),
            pltpu.VMEM((kvh, zn, rows, qw // kvh), BF),
            pltpu.SemaphoreType.DMA((2,)),
            pltpu.SemaphoreType.DMA((zper, 3)),
            pltpu.SemaphoreType.DMA,
            pltpu.SemaphoreType.DMA((kvh, 2)),
            pltpu.SemaphoreType.DMA,
            pltpu.SemaphoreType.DMA((kvh, zn)),
        ]
    outs = pl.pallas_call(
        functools.partial(kernel, (n, tp, with_dw)),
        out_shape=[pltpu.VMEM(a.shape, a.dtype) for a in out_shape],
        in_specs=specs,
        out_specs=[vm] * len(out_shape),
        scratch_shapes=scratch,
        compiler_params=pltpu.CompilerParams(
            collective_id=0, has_side_effects=True, vmem_limit_bytes=66100000),
    )(*args, chosen.T)
    outs = pl.pallas_call(
        writer,
        out_shape=out_shape,
        in_specs=[vm] * len(out_shape),
        out_specs=[hbm] * len(out_shape),
        scratch_shapes=[pltpu.SemaphoreType.DMA((len(out_shape),))],
        compiler_params=pltpu.CompilerParams(vmem_limit_bytes=1024 * 1024),
    )(*outs)
    if with_dw:
        return tuple(outs)
    whole_input = lax.all_gather(layer_input, "tp", axis=1, tiled=True)
    grad_weight = lax.psum_scatter(
        jnp.einsum("td,tc->dc", whole_input, outs[0], preferred_element_type=F32),
        "kv", scatter_dimension=0, tiled=True)
    return tuple(outs) + (grad_weight,)


def solution(mesh):
    spec = P("kv", "tp")
    return jax.shard_map(
        shards,
        mesh=mesh,
        in_specs=(spec,) * 7 + (P(),),
        out_specs=(spec,) * 4,
        check_vma=False,
    )
```

```python
import functools
import math

import jax
import jax.numpy as jnp
from jax import lax
from jax.experimental import pallas as pl
from jax.experimental.pallas import tpu as pltpu
from jax.sharding import PartitionSpec as P

DH = 64
BLOCK = 64
PER = 2
LEVELS = 4
LOG2E = 1.4426950408889634
NEG = -1e30
NT = (((1,), (1,)), ((), ()))
TN = (((0,), (0,)), ((), ()))
NN = (((1,), (0,)), ((), ()))
BF = jnp.bfloat16
F32 = jnp.float32


def dot(a, b, dims):
    return lax.dot_general(a, b, dims, preferred_element_type=F32)


def kernel(cfg, *refs):
    n, tp, with_dw = cfg
    count_in = 7 if with_dw else 6
    hbm, refs = refs[:count_in], refs[count_in:]
    ch_hbm, refs = refs[0], refs[1:]
    count_out = 4 if with_dw else 3
    outs, refs = refs[:count_out], refs[count_out:]
    kv_ref, qgo, lse_ref, refs = refs[0], refs[1], refs[2], refs[3:]
    if with_dw:
        x_ref, refs = refs[0], refs[1:]
    ch_ref, refs = refs[0], refs[1:]
    (in_s, qs, gs, lrow, drow, dqt, acc, kvbuf, gsend, grecv,
     kv_s, kv_r, g_s, g_r) = refs[:14]
    dq_out, dk_out, dv_out = outs[:3]
    k_ref, v_ref = kv_ref.at[0], kv_ref.at[1]
    q_ref, g_ref, o_ref = qgo.at[0], qgo.at[1], qgo.at[2]
    if with_dw:
        dw_out = outs[3]
        (xbuf, xt, dqall, part, precv, x_s, x_r, a_s, a_r, w_s, w_r) = refs[14:]
    places = [k_ref, v_ref, q_ref, g_ref, o_ref, lse_ref] + ([x_ref] if with_dw else [])
    for i, to in enumerate(places):
        pltpu.make_async_copy(hbm[i], to, in_s.at[(0, 0, 1, 1, 1, 2, 4)[i]]).start()
    pltpu.make_async_copy(ch_hbm, ch_ref, in_s.at[3]).start()

    def drain(ref, sem):
        pltpu.make_async_copy(ref, ref, sem).wait()

    me = lax.axis_index("kv")
    mt = lax.axis_index("tp")
    tok = q_ref.shape[0]
    kvh = k_ref.shape[1] // DH
    qh = q_ref.shape[1] // DH
    grp = qh // kvh
    nb = tok // BLOCK
    cols = grp * tok
    scale = DH ** -0.5
    dist = [1, n // 8, n // 4, n // 2]

    def span(level):
        if isinstance(level, int):
            return dist[level]
        return jnp.where(level == 0, dist[0], jnp.where(level == 1, dist[1], jnp.where(level == 2, dist[2], dist[3])))

    if with_dw:
        wn = math.isqrt(n)
        zn = n // wn
        zper = zn // tp
        rows = dw_out.shape[0]
        z = me // wn
        w = lax.rem(me, wn)
        pair = w + 1 - 2 * lax.rem(w, 2)
        across = lax.rem(w + 2, wn)
        across_pair = lax.rem(pair + 2, wn)
        near = z + 1 - 2 * lax.rem(z, 2)
        far = lax.rem(z + 2, zn)
        outer = (z == 0) | (z == zn - 1)
        inner = (z > 0) & (z < zn - 1)
        to_outer = jnp.where(outer, zn - 1 - z, zn - 1 - near)
        to_inner = jnp.where(outer, zn - 1 - near, zn - 1 - z)
        partner = me + 1 - 2 * lax.rem(me, 2)
        first = lax.rem(me, 2) == 0
        second = lax.rem(me, 2) == 1
        order = [1 - lax.rem(z, 2), lax.rem(z, 2)]
        plane = [(pair, mt), (across, mt), (across_pair, mt), (w, 1 - mt), (pair, 1 - mt)]

    barrier = pltpu.get_barrier_semaphore()
    count = jnp.int32(0)
    for d in dist[1:] if with_dw else dist:
        @pl.when(me + d < n)
        def _():
            pl.semaphore_signal(barrier, inc=1, device_id={"kv": me + d}, device_id_type=pl.DeviceIdType.MESH)

        @pl.when(me >= d)
        def _():
            pl.semaphore_signal(barrier, inc=1, device_id={"kv": me - d}, device_id_type=pl.DeviceIdType.MESH)

        count = count + jnp.where(me + d < n, 1, 0) + jnp.where(me >= d, 1, 0)
    if with_dw:
        for wt, tt in plane:
            pl.semaphore_signal(barrier, inc=1, device_id={"kv": z * wn + wt, "tp": tt}, device_id_type=pl.DeviceIdType.MESH)
        for zt in (near, far):
            pl.semaphore_signal(barrier, inc=1, device_id={"kv": zt * wn + w}, device_id_type=pl.DeviceIdType.MESH)
        count = count + len(plane) + 2
    pl.semaphore_wait(barrier, count)

    def kv_copy(level):
        return pltpu.make_async_remote_copy(
            src_ref=kv_ref, dst_ref=kvbuf.at[level],
            send_sem=kv_s.at[level], recv_sem=kv_r.at[level],
            device_id={"kv": me + span(level)}, device_id_type=pl.DeviceIdType.MESH)

    def kv_pass_on(level, src):
        return pltpu.make_async_remote_copy(
            src_ref=src, dst_ref=kvbuf.at[level],
            send_sem=kv_s.at[level], recv_sem=kv_r.at[level],
            device_id={"kv": partner if level == 0 else me + dist[2]}, device_id_type=pl.DeviceIdType.MESH)

    def g_copy(level):
        to = jnp.where(level == 0, partner, me - span(level)) if with_dw else me - dist[level]
        return pltpu.make_async_remote_copy(
            src_ref=gsend.at[level], dst_ref=grecv.at[level],
            send_sem=g_s.at[level], recv_sem=g_r.at[level],
            device_id={"kv": to}, device_id_type=pl.DeviceIdType.MESH)

    drain(kv_ref, in_s.at[0])
    turns = [0, 1, 3, 2]
    if with_dw:
        late = w == 0
        turns = [jnp.where(second, 0, 2), jnp.where(second, 2, jnp.where(late, 0, 1)),
                 jnp.where(second, 1, jnp.where(late, 3, 0)), jnp.where(late, 1, 3)]
    for level in (2, 1) if with_dw else turns:
        @pl.when((me + dist[level] < n) & (w < 3) if with_dw and level == 1 else me + dist[level] < n)
        def _():
            kv_copy(level).start()

    if with_dw:
        @pl.when(first)
        def _():
            kv_pass_on(0, kv_ref).start()

        def x_copy(idx, k):
            wt, tt = plane[idx]
            zz = order[k]
            off = pl.multiple_of((zz * wn + wt) * rows, rows)
            return pltpu.make_async_remote_copy(
                src_ref=x_ref.at[:, pl.ds(off, rows)],
                dst_ref=xbuf.at[mt * zper + zz, pl.ds(pl.multiple_of(w * tok, tok), tok)],
                send_sem=x_s.at[0 if idx else 1], recv_sem=x_r.at[k, 0 if idx in (1, 2) else 1],
                device_id={"kv": z * wn + wt, "tp": tt}, device_id_type=pl.DeviceIdType.MESH)

        def x_forward(idx, k):
            slot = xbuf.at[mt * zper + order[k], pl.ds(pl.multiple_of(plane[idx][0] * tok, tok), tok)]
            return pltpu.make_async_remote_copy(
                src_ref=slot, dst_ref=slot,
                send_sem=x_s.at[1], recv_sem=x_r.at[k, 2],
                device_id={"kv": me, "tp": 1 - mt}, device_id_type=pl.DeviceIdType.MESH)

        drain(x_ref, in_s.at[4])
        for k in range(zper):
            for idx in (1, 2, 3, 4, 0):
                x_copy(idx, k).start()
        for zz in range(zper):
            off = pl.multiple_of((zz * wn + w) * rows, rows)
            xbuf[mt * zper + zz, pl.ds(pl.multiple_of(w * tok, tok), tok), :] = x_ref[:, pl.ds(off, rows)]

    drain(qgo, in_s.at[1])
    drain(lse_ref, in_s.at[2])
    pltpu.make_async_copy(ch_hbm, ch_ref, in_s.at[3]).wait()
    lse_t = lse_ref[...] * (-LOG2E)
    prod = g_ref[...].astype(F32) * o_ref[...].astype(F32)
    hi = prod.astype(BF)
    lo = (prod - hi.astype(F32)).astype(BF)
    pick = (lax.broadcasted_iota(jnp.int32, (16, qh * DH), 1) // DH
            == lax.broadcasted_iota(jnp.int32, (16, qh * DH), 0)).astype(F32).astype(BF)
    delta_t = dot(pick, hi, NT) + dot(pick, lo, NT)
    part_cols = grp * BLOCK
    for h in range(kvh):
        for g in range(grp):
            i = h * grp + g
            for qb in range(nb):
                rows_ = slice(qb * BLOCK, (qb + 1) * BLOCK)
                to = slice(qb * part_cols + g * BLOCK, qb * part_cols + (g + 1) * BLOCK)
                lrow[h, 0:1, to] = lse_t[i:i + 1, rows_]
                drow[h, 0:1, to] = delta_t[i:i + 1, rows_]
                qs[h, to, :] = q_ref[rows_, i * DH:(i + 1) * DH]
                gs[h, to, :] = g_ref[rows_, i * DH:(i + 1) * DH]

    def run_pass(heads, ks, vs, keep):
        to = [slice(qb * part_cols, (qb + 1) * part_cols) for qb in range(nb)]
        each = [(h, t, k, v) for h, hk, hv in zip(heads, ks, vs) for t, k, v in zip(to, hk, hv)]
        st = [dot(k, qs[h, t, :], NT) for h, t, k, v in each]
        dp = [dot(v, gs[h, t, :], NT) for h, t, k, v in each]
        st = [x * (scale * LOG2E) + lrow[h, 0:1, t] for x, (h, t, k, v) in zip(st, each)]
        p = [jnp.exp2(x if keep is None else jnp.where(keep, x, NEG)) for x in st]
        ds = [(x * (y - drow[h, 0:1, t])).astype(BF) for x, y, (h, t, k, v) in zip(p, dp, each)]
        dv = [dot(x.astype(BF), gs[h, t, :], NN) for x, (h, t, k, v) in zip(p, each)]
        dq = [dot(k, x, TN) for x, (h, t, k, v) in zip(ds, each)]
        dk = [dot(x, qs[h, t, :], NN) for x, (h, t, k, v) in zip(ds, each)]
        return [(dq[i * nb:(i + 1) * nb], dk[i * nb:(i + 1) * nb], dv[i * nb:(i + 1) * nb]) for i in range(len(heads))]

    causal = (lax.rem(lax.broadcasted_iota(jnp.int32, (BLOCK, part_cols), 1), BLOCK)
              >= lax.broadcasted_iota(jnp.int32, (BLOCK, part_cols), 0))
    blocks = [slice(qb * BLOCK, (qb + 1) * BLOCK) for qb in range(nb)]
    lanes_of = [slice(h * DH, (h + 1) * DH) for h in range(kvh)]
    own = run_pass(list(range(kvh)), [[k_ref[r, l] for r in blocks] for l in lanes_of],
                   [[v_ref[r, l] for r in blocks] for l in lanes_of], causal)
    for h, (dq, dk, dv) in enumerate(own):
        dqt[h] = jnp.concatenate(dq, axis=1)
        acc[0, :, lanes_of[h]] = jnp.concatenate(dk, axis=0) * scale
        acc[1, :, lanes_of[h]] = jnp.concatenate(dv, axis=0)

    if with_dw:
        @pl.when((me + dist[1] < n) & (w == 3))
        def _():
            kv_copy(1).start()

    def picks(level):
        found = []
        for qb in range(nb):
            pair_ = [jnp.clip(ch_ref[PER * level + i, me * nb + qb] - (me - span(level)) * nb, 0, nb - 1)
                     for i in range(PER)]
            found.append((jnp.minimum(*pair_), jnp.maximum(*pair_)))
        return found

    def far_pass(level, heads, found):
        ks, vs = [], []
        for i, picked in enumerate((ks, vs)):
            for h in heads:
                blocks = [kvbuf[level, i, b * BLOCK:(b + 1) * BLOCK, lanes_of[h]] for b in range(nb)]
                chosen_blocks = []
                for low, high in found:
                    first_, second_ = blocks[0], blocks[1]
                    for b in range(1, nb - 1):
                        first_ = jnp.where(low == b, blocks[b], first_)
                    for b in range(2, nb):
                        second_ = jnp.where(high == b, blocks[b], second_)
                    chosen_blocks.append(jnp.concatenate([first_, second_], axis=0))
                picked.append(chosen_blocks)
        for h, (dq, dk, dv) in zip(heads, run_pass(heads, ks, vs, None)):
            dqt[h] = dqt[h] + jnp.concatenate(dq, axis=1)
            for i, new in enumerate((dk, dv)):
                for b in range(nb):
                    total = None
                    for qb in range(nb):
                        low, high = found[qb]
                        add = jnp.zeros((BLOCK, DH), F32)
                        if b:
                            add = jnp.where(high == b, new[qb][BLOCK:], add)
                        if b < nb - 1:
                            add = jnp.where(low == b, new[qb][:BLOCK], add)
                        total = add if total is None else total + add
                    if i == 0:
                        total = total * scale
                    gsend[level, i, b * BLOCK:(b + 1) * BLOCK, lanes_of[h]] = total.astype(BF)

    def wait_kv(level):
        kv_copy(level).wait_recv()

    def far_level(level):
        found = picks(level)
        far_pass(level, list(range(kvh)), found)

    def arrive(level):
        wait_kv(level)
        if with_dw:
            @pl.when((level == 2) & (me + dist[2] < n))
            def _():
                kv_pass_on(3, kvbuf.at[2]).start()

            @pl.when((level == 1) & second)
            def _():
                kv_pass_on(0, kvbuf.at[1]).start()

    def return_level(level):
        if with_dw:
            @pl.when(level != 1)
            def _():
                g_copy(level).start()
        else:
            g_copy(level).start()

    def pass_x_on(k):
        drain(xbuf.at[0, 0:2 * tok], x_r.at[k, 0])
        for idx in (1, 2):
            x_forward(idx, k).start()

    for turn, level in enumerate(turns[:-1]):
        if with_dw and turn == 2:
            @pl.when((z >= 1) & first)
            def _():
                pass_x_on(0)

        @pl.when(me >= span(level))
        def _():
            arrive(level)
            far_level(level)
            return_level(level)

    if with_dw:
        mine = pl.ds(pl.multiple_of(w * tok, tok), tok)
        hops = list(range(2, wn, 2))

        def a_copy(h, s):
            to = pair if s == 0 else lax.rem(w + s, wn)
            return pltpu.make_async_remote_copy(
                src_ref=dqall.at[h, mine], dst_ref=dqall.at[h, mine],
                send_sem=a_s, recv_sem=a_r.at[h, s // 2],
                device_id={"kv": z * wn + to}, device_id_type=pl.DeviceIdType.MESH)

        def f_copy(h, s):
            slot = pl.ds(pl.multiple_of(lax.rem(w + wn - s, wn) * tok, tok), tok)
            return pltpu.make_async_remote_copy(
                src_ref=dqall.at[h, slot], dst_ref=dqall.at[h, slot],
                send_sem=a_s, recv_sem=a_r.at[h, 0],
                device_id={"kv": z * wn + pair}, device_id_type=pl.DeviceIdType.MESH)

    if with_dw:
        @pl.when((z >= 2) & second)
        def _():
            pass_x_on(0)

    last = turns[-1]
    for h in range(kvh):
        @pl.when(me >= span(last))
        def _():
            if h == 0:
                arrive(last)
            far_pass(last, [h], picks(last))
        whole = (dqt[h] * scale).astype(BF)
        step = 2 if grp % 2 == 0 else 1
        for qb in range(nb):
            for g in range(0, grp, step):
                at = qb * part_cols + g * BLOCK
                low = jnp.concatenate(
                    [whole[:, at + j * BLOCK:at + (j + 1) * BLOCK] for j in range(step)], axis=0).T
                i = h * grp + g
                dq_out[qb * BLOCK:(qb + 1) * BLOCK, i * DH:(i + step) * DH] = low
                if with_dw:
                    at_rows = pl.ds(pl.multiple_of(w * tok + qb * BLOCK, BLOCK), BLOCK)
                    dqall[h, at_rows, g * DH:(g + step) * DH] = low
        if with_dw:
            for s in hops:
                a_copy(h, s).start()
            a_copy(h, 0).start()

    @pl.when(me >= span(last))
    def _():
        return_level(last)

    def early_sum():
        @pl.when(second)
        def _():
            g_copy(0).wait_recv()
            gsend[1] = (gsend[1].astype(F32) + grecv[0].astype(F32)).astype(BF)

        g_copy(1).start()

    if with_dw:
        @pl.when((z < 1) | ((z < 2) & second))
        def _():
            pass_x_on(0)

        pass_x_on(1)

        @pl.when((me >= dist[1]) & (w < 2))
        def _():
            early_sum()

        def x_arrive(k):
            drain(xbuf.at[0, 0:3 * tok], x_r.at[k, 1])
            drain(xbuf.at[0, 0:2 * tok], x_r.at[k, 2])

        wide = grp * DH // 2
        chunks = list(range(2 * kvh))

        def w_copy(h, i, slot, to):
            return pltpu.make_async_remote_copy(
                src_ref=part.at[h, i], dst_ref=precv.at[h, slot],
                send_sem=w_s, recv_sem=w_r.at[h, slot],
                device_id={"kv": to * wn + w}, device_id_type=pl.DeviceIdType.MESH)

        def w_arrive(h, slot):
            w_copy(h, 1, slot, near).wait_recv()

        def send_part(h, i, slot, block, to, add=None):
            new = dot(xt[block], dqall[h // 2, :, (h % 2) * wide:(h % 2 + 1) * wide], NN)
            if add is not None:
                w_arrive(h, add)
                new = new + precv[h, add].astype(F32)
            part[h, i] = new.astype(BF)
            w_copy(h, i, slot, to).start()

        def across_on(h):
            for s in hops:
                a_copy(h, s).wait_recv()
                f_copy(h, s).start()

        for h in range(kvh):
            if h == 0:
                across_on(h)

                @pl.when(second)
                def _():
                    for later in range(1, kvh):
                        across_on(later)
            else:
                @pl.when(first)
                def _():
                    across_on(h)
            if h < zper:
                x_arrive(h)
                for zz in ((lax.rem(near + 2, zn), near), (far, z))[h]:
                    xt[zz] = xbuf[zz].T
            drain(dqall.at[h, 0:2 * tok], a_r.at[h, 0])
            @pl.when(outer)
            def _():
                for each in (2 * h, 2 * h + 1):
                    send_part(each, 0, 0, to_outer, near)
                if h:
                    for each in chunks:
                        send_part(each, 2, 3, to_inner, near)

            @pl.when(inner)
            def _():
                for each in (2 * h, 2 * h + 1):
                    send_part(each, 1, 1, near, near)

        @pl.when(w >= 2)
        def _():
            early_sum()

        @pl.when(outer)
        def _():
            for each in chunks:
                send_part(each, 1, 1, near, near)

        @pl.when(inner)
        def _():
            for h in chunks:
                send_part(h, 0, 2, to_outer, to_outer, 0)
            for h in chunks:
                send_part(h, 2, 2, to_inner, to_inner, 3)

        width = grp * DH
        for h in range(kvh):
            dw_out[:, h * width:(h + 1) * width] = dot(xt[z], dqall[h], NN)
        drain(xbuf.at[0:2], x_s.at[0])
        drain(xbuf.at[0:3, 0:2 * tok], x_s.at[1])
        drain(dqall.at[:, 0:3 * tok], a_s)

    def add_in(level):
        g_copy(level).wait_recv()
        acc[...] = acc[...] + grecv[level].astype(F32)

    def sent_kv(level):
        kv_copy(level).wait_send()

    if with_dw:
        @pl.when(first)
        def _():
            sent_kv(0)
            add_in(0)

            @pl.when(me >= dist[1])
            def _():
                g_copy(0).wait_send()

        @pl.when(second)
        def _():
            g_copy(0).wait_send()

            @pl.when(me >= dist[1])
            def _():
                sent_kv(0)

        @pl.when((me >= dist[2]) & (me + dist[2] < n))
        def _():
            sent_kv(3)

        for level in (1, 2, 3):
            @pl.when(me + dist[level] < n)
            def _():
                if level < 3:
                    sent_kv(level)
                add_in(level)

            @pl.when(me >= dist[level])
            def _():
                g_copy(level).wait_send()
    else:
        for level, d in enumerate(dist):
            @pl.when(me + d < n)
            def _():
                sent_kv(level)
                add_in(level)

            @pl.when(me >= d)
            def _():
                g_copy(level).wait_send()

    dk_out[...] = acc[0].astype(BF)
    dv_out[...] = acc[1].astype(BF)
    if with_dw:
        for h in chunks:
            lanes = slice(h * wide, (h + 1) * wide)
            w_arrive(h, 1)
            w_arrive(h, 2)
            dw_out[:, lanes] = dw_out[:, lanes] + precv[h, 1].astype(F32) + precv[h, 2].astype(F32)
        drain(part, w_s)


def writer(*refs):
    count = (len(refs) - 1) // 2
    sem = refs[-1]
    copies = [pltpu.make_async_copy(refs[i], refs[count + i], sem.at[i]) for i in range(count)]
    for copy in copies:
        copy.start()
    for copy in copies:
        copy.wait()


def shards(layer_input, queries, keys, values, attn_out, grad_out, log_sum, chosen):
    n = lax.axis_size("kv")
    tp = lax.axis_size("tp")
    tok, qw = queries.shape
    kw = keys.shape[1]
    kvh, qh = kw // DH, qw // DH
    cols = qh // kvh * tok
    depth = layer_input.shape[1] * tp
    rows = depth // n
    wn = math.isqrt(n)
    zn = n // wn
    with_dw = wn * wn == n and zn == 4 and tp == 2 and rows % 128 == 0
    vm = pl.BlockSpec(memory_space=pltpu.VMEM)
    out_shape = [
        jax.ShapeDtypeStruct((tok, qw), BF),
        jax.ShapeDtypeStruct((tok, kw), BF),
        jax.ShapeDtypeStruct((tok, kw), BF),
    ]
    args = [keys, values, queries, grad_out, attn_out, log_sum.T]
    if with_dw:
        args.append(layer_input)
    held = [((2, tok, kw), BF), ((3, tok, qw), BF)] + [(a.shape, a.dtype) for a in args[5:]]
    scratch = [pltpu.VMEM(*a) for a in held] + [
        pltpu.SMEM(chosen.T.shape, chosen.dtype),
        pltpu.SemaphoreType.DMA((5,)),
        pltpu.VMEM((kvh, cols, DH), BF),
        pltpu.VMEM((kvh, cols, DH), BF),
        pltpu.VMEM((kvh, 1, cols), F32),
        pltpu.VMEM((kvh, 1, cols), F32),
        pltpu.VMEM((kvh, DH, cols), F32),
        pltpu.VMEM((2, tok, kw), F32),
        pltpu.VMEM((LEVELS, 2, tok, kw), BF),
        pltpu.VMEM((LEVELS, 2, tok, kw), BF),
        pltpu.VMEM((LEVELS, 2, tok, kw), BF),
        pltpu.SemaphoreType.DMA((LEVELS,)),
        pltpu.SemaphoreType.DMA((LEVELS,)),
        pltpu.SemaphoreType.DMA((LEVELS,)),
        pltpu.SemaphoreType.DMA((LEVELS,)),
    ]
    hbm = pl.BlockSpec(memory_space=pltpu.HBM)
    specs = [hbm] * (len(args) + 1)
    if with_dw:
        out_shape.append(jax.ShapeDtypeStruct((rows, qw), F32))
        zper = zn // tp
        scratch += [
            pltpu.VMEM((zn, wn * tok, rows), BF),
            pltpu.VMEM((zn, rows, wn * tok), BF),
            pltpu.VMEM((kvh, wn * tok, qw // kvh), BF),
            pltpu.VMEM((2 * kvh, zn - 1, rows, qw // kvh // 2), BF),
            pltpu.VMEM((2 * kvh, zn, rows, qw // kvh // 2), BF),
            pltpu.SemaphoreType.DMA((2,)),
            pltpu.SemaphoreType.DMA((zper, 3)),
            pltpu.SemaphoreType.DMA,
            pltpu.SemaphoreType.DMA((kvh, 2)),
            pltpu.SemaphoreType.DMA,
            pltpu.SemaphoreType.DMA((2 * kvh, zn)),
        ]
    outs = pl.pallas_call(
        functools.partial(kernel, (n, tp, with_dw)),
        out_shape=[pltpu.VMEM(a.shape, a.dtype) for a in out_shape],
        in_specs=specs,
        out_specs=[vm] * len(out_shape),
        scratch_shapes=scratch,
        compiler_params=pltpu.CompilerParams(
            collective_id=0, has_side_effects=True, vmem_limit_bytes=66100000),
    )(*args, chosen.T)
    outs = pl.pallas_call(
        writer,
        out_shape=out_shape,
        in_specs=[vm] * len(out_shape),
        out_specs=[hbm] * len(out_shape),
        scratch_shapes=[pltpu.SemaphoreType.DMA((len(out_shape),))],
        compiler_params=pltpu.CompilerParams(vmem_limit_bytes=1024 * 1024),
    )(*outs)
    if with_dw:
        return tuple(outs)
    whole_input = lax.all_gather(layer_input, "tp", axis=1, tiled=True)
    grad_weight = lax.psum_scatter(
        jnp.einsum("td,tc->dc", whole_input, outs[0], preferred_element_type=F32),
        "kv", scatter_dimension=0, tiled=True)
    return tuple(outs) + (grad_weight,)


def solution(mesh):
    spec = P("kv", "tp")
    return jax.shard_map(
        shards,
        mesh=mesh,
        in_specs=(spec,) * 7 + (P(),),
        out_specs=(spec,) * 4,
        check_vma=False,
    )
```

```python
import functools
import math

import jax
import jax.numpy as jnp
from jax import lax
from jax.experimental import pallas as pl
from jax.experimental.pallas import tpu as pltpu
from jax.sharding import PartitionSpec as P

DH = 64
BLOCK = 64
PER = 2
LEVELS = 4
LOG2E = 1.4426950408889634
NEG = -1e30
NT = (((1,), (1,)), ((), ()))
TN = (((0,), (0,)), ((), ()))
NN = (((1,), (0,)), ((), ()))
BF = jnp.bfloat16
F32 = jnp.float32


def dot(a, b, dims):
    return lax.dot_general(a, b, dims, preferred_element_type=F32)


def kernel(cfg, *refs):
    n, tp, with_dw = cfg
    count_in = 7 if with_dw else 6
    hbm, refs = refs[:count_in], refs[count_in:]
    ch_hbm, refs = refs[0], refs[1:]
    count_out = 4 if with_dw else 3
    outs, refs = refs[:count_out], refs[count_out:]
    kv_ref, qgo, lse_ref, refs = refs[0], refs[1], refs[2], refs[3:]
    if with_dw:
        x_ref, refs = refs[0], refs[1:]
    ch_ref, refs = refs[0], refs[1:]
    (in_s, qs, gs, lrow, drow, dqt, acc, kvbuf, gsend, grecv,
     kv_s, kv_r, g_s, g_r) = refs[:14]
    dq_out, dk_out, dv_out = outs[:3]
    k_ref, v_ref = kv_ref.at[0], kv_ref.at[1]
    q_ref, g_ref, o_ref = qgo.at[0], qgo.at[1], qgo.at[2]
    if with_dw:
        dw_out = outs[3]
        (xbuf, xt, dqall, part, precv, x_s, x_r, a_s, a_r, w_s, w_r) = refs[14:]
    places = [k_ref, v_ref, q_ref, g_ref, o_ref, lse_ref] + ([x_ref] if with_dw else [])
    for i, to in enumerate(places):
        pltpu.make_async_copy(hbm[i], to, in_s.at[(0, 0, 1, 1, 1, 2, 4)[i]]).start()
    pltpu.make_async_copy(ch_hbm, ch_ref, in_s.at[3]).start()

    def drain(ref, sem):
        pltpu.make_async_copy(ref, ref, sem).wait()

    me = lax.axis_index("kv")
    mt = lax.axis_index("tp")
    tok = q_ref.shape[0]
    kvh = k_ref.shape[1] // DH
    qh = q_ref.shape[1] // DH
    grp = qh // kvh
    nb = tok // BLOCK
    cols = grp * tok
    scale = DH ** -0.5
    dist = [1, n // 8, n // 4, n // 2]

    def span(level):
        if isinstance(level, int):
            return dist[level]
        return jnp.where(level == 0, dist[0], jnp.where(level == 1, dist[1], jnp.where(level == 2, dist[2], dist[3])))

    if with_dw:
        wn = math.isqrt(n)
        zn = n // wn
        zper = zn // tp
        rows = dw_out.shape[0]
        z = me // wn
        w = lax.rem(me, wn)
        pair = w + 1 - 2 * lax.rem(w, 2)
        across = lax.rem(w + 2, wn)
        across_pair = lax.rem(pair + 2, wn)
        near = z + 1 - 2 * lax.rem(z, 2)
        far = lax.rem(z + 2, zn)
        outer = (z == 0) | (z == zn - 1)
        inner = (z > 0) & (z < zn - 1)
        to_outer = jnp.where(outer, zn - 1 - z, zn - 1 - near)
        to_inner = jnp.where(outer, zn - 1 - near, zn - 1 - z)
        partner = me + 1 - 2 * lax.rem(me, 2)
        first = lax.rem(me, 2) == 0
        second = lax.rem(me, 2) == 1
        order = [1 - lax.rem(z, 2), lax.rem(z, 2)]
        plane = [(pair, mt), (across, mt), (across_pair, mt), (w, 1 - mt), (pair, 1 - mt)]

    barrier = pltpu.get_barrier_semaphore()
    count = jnp.int32(0)
    for d in dist[1:] if with_dw else dist:
        @pl.when(me + d < n)
        def _():
            pl.semaphore_signal(barrier, inc=1, device_id={"kv": me + d}, device_id_type=pl.DeviceIdType.MESH)

        @pl.when(me >= d)
        def _():
            pl.semaphore_signal(barrier, inc=1, device_id={"kv": me - d}, device_id_type=pl.DeviceIdType.MESH)

        count = count + jnp.where(me + d < n, 1, 0) + jnp.where(me >= d, 1, 0)
    if with_dw:
        for wt, tt in plane:
            pl.semaphore_signal(barrier, inc=1, device_id={"kv": z * wn + wt, "tp": tt}, device_id_type=pl.DeviceIdType.MESH)
        for zt in (near, far):
            pl.semaphore_signal(barrier, inc=1, device_id={"kv": zt * wn + w}, device_id_type=pl.DeviceIdType.MESH)
        count = count + len(plane) + 2
    pl.semaphore_wait(barrier, count)

    def kv_copy(level):
        return pltpu.make_async_remote_copy(
            src_ref=kv_ref, dst_ref=kvbuf.at[level],
            send_sem=kv_s.at[level], recv_sem=kv_r.at[level],
            device_id={"kv": me + span(level)}, device_id_type=pl.DeviceIdType.MESH)

    def kv_pass_on(level, src):
        return pltpu.make_async_remote_copy(
            src_ref=src, dst_ref=kvbuf.at[level],
            send_sem=kv_s.at[level], recv_sem=kv_r.at[level],
            device_id={"kv": partner if level == 0 else me + dist[2]}, device_id_type=pl.DeviceIdType.MESH)

    def g_copy(level):
        to = jnp.where(level == 0, partner, me - span(level)) if with_dw else me - dist[level]
        return pltpu.make_async_remote_copy(
            src_ref=gsend.at[level], dst_ref=grecv.at[level],
            send_sem=g_s.at[level], recv_sem=g_r.at[level],
            device_id={"kv": to}, device_id_type=pl.DeviceIdType.MESH)

    drain(kv_ref, in_s.at[0])
    turns = [0, 1, 3, 2]
    if with_dw:
        late = w == 0
        turns = [jnp.where(second, 0, 2), jnp.where(second, 2, jnp.where(late, 0, 1)),
                 jnp.where(second, 1, jnp.where(late, 3, 0)), jnp.where(late, 1, 3)]
    for level in (2, 1) if with_dw else turns:
        @pl.when((me + dist[level] < n) & (w < 3) if with_dw and level == 1 else me + dist[level] < n)
        def _():
            kv_copy(level).start()

    if with_dw:
        @pl.when(first)
        def _():
            kv_pass_on(0, kv_ref).start()

        def x_copy(idx, k):
            wt, tt = plane[idx]
            zz = order[k]
            off = pl.multiple_of((zz * wn + wt) * rows, rows)
            return pltpu.make_async_remote_copy(
                src_ref=x_ref.at[:, pl.ds(off, rows)],
                dst_ref=xbuf.at[mt * zper + zz, pl.ds(pl.multiple_of(w * tok, tok), tok)],
                send_sem=x_s.at[0 if idx else 1], recv_sem=x_r.at[k, 0 if idx in (1, 2) else 1],
                device_id={"kv": z * wn + wt, "tp": tt}, device_id_type=pl.DeviceIdType.MESH)

        def x_forward(idx, k):
            slot = xbuf.at[mt * zper + order[k], pl.ds(pl.multiple_of(plane[idx][0] * tok, tok), tok)]
            return pltpu.make_async_remote_copy(
                src_ref=slot, dst_ref=slot,
                send_sem=x_s.at[1], recv_sem=x_r.at[k, 2],
                device_id={"kv": me, "tp": 1 - mt}, device_id_type=pl.DeviceIdType.MESH)

        drain(x_ref, in_s.at[4])
        for k in range(zper):
            for idx in (1, 2, 3, 4, 0):
                x_copy(idx, k).start()
        for zz in range(zper):
            off = pl.multiple_of((zz * wn + w) * rows, rows)
            xbuf[mt * zper + zz, pl.ds(pl.multiple_of(w * tok, tok), tok), :] = x_ref[:, pl.ds(off, rows)]

    drain(qgo, in_s.at[1])
    drain(lse_ref, in_s.at[2])
    pltpu.make_async_copy(ch_hbm, ch_ref, in_s.at[3]).wait()
    lse_t = lse_ref[...] * (-LOG2E)
    prod = g_ref[...].astype(F32) * o_ref[...].astype(F32)
    hi = prod.astype(BF)
    lo = (prod - hi.astype(F32)).astype(BF)
    pick = (lax.broadcasted_iota(jnp.int32, (16, qh * DH), 1) // DH
            == lax.broadcasted_iota(jnp.int32, (16, qh * DH), 0)).astype(F32).astype(BF)
    delta_t = dot(pick, hi, NT) + dot(pick, lo, NT)
    part_cols = grp * BLOCK
    for h in range(kvh):
        for g in range(grp):
            i = h * grp + g
            for qb in range(nb):
                rows_ = slice(qb * BLOCK, (qb + 1) * BLOCK)
                to = slice(qb * part_cols + g * BLOCK, qb * part_cols + (g + 1) * BLOCK)
                lrow[h, 0:1, to] = lse_t[i:i + 1, rows_]
                drow[h, 0:1, to] = delta_t[i:i + 1, rows_]
                qs[h, to, :] = q_ref[rows_, i * DH:(i + 1) * DH]
                gs[h, to, :] = g_ref[rows_, i * DH:(i + 1) * DH]

    def run_pass(heads, ks, vs, keep):
        to = [slice(qb * part_cols, (qb + 1) * part_cols) for qb in range(nb)]
        each = [(h, t, k, v) for h, hk, hv in zip(heads, ks, vs) for t, k, v in zip(to, hk, hv)]
        st = [dot(k, qs[h, t, :], NT) for h, t, k, v in each]
        dp = [dot(v, gs[h, t, :], NT) for h, t, k, v in each]
        st = [x * (scale * LOG2E) + lrow[h, 0:1, t] for x, (h, t, k, v) in zip(st, each)]
        p = [jnp.exp2(x if keep is None else jnp.where(keep, x, NEG)) for x in st]
        ds = [(x * (y - drow[h, 0:1, t])).astype(BF) for x, y, (h, t, k, v) in zip(p, dp, each)]
        dv = [dot(x.astype(BF), gs[h, t, :], NN) for x, (h, t, k, v) in zip(p, each)]
        dq = [dot(k, x, TN) for x, (h, t, k, v) in zip(ds, each)]
        dk = [dot(x, qs[h, t, :], NN) for x, (h, t, k, v) in zip(ds, each)]
        return [(dq[i * nb:(i + 1) * nb], dk[i * nb:(i + 1) * nb], dv[i * nb:(i + 1) * nb]) for i in range(len(heads))]

    causal = (lax.rem(lax.broadcasted_iota(jnp.int32, (BLOCK, part_cols), 1), BLOCK)
              >= lax.broadcasted_iota(jnp.int32, (BLOCK, part_cols), 0))
    blocks = [slice(qb * BLOCK, (qb + 1) * BLOCK) for qb in range(nb)]
    lanes_of = [slice(h * DH, (h + 1) * DH) for h in range(kvh)]
    own = run_pass(list(range(kvh)), [[k_ref[r, l] for r in blocks] for l in lanes_of],
                   [[v_ref[r, l] for r in blocks] for l in lanes_of], causal)
    for h, (dq, dk, dv) in enumerate(own):
        dqt[h] = jnp.concatenate(dq, axis=1)
        acc[0, :, lanes_of[h]] = jnp.concatenate(dk, axis=0) * scale
        acc[1, :, lanes_of[h]] = jnp.concatenate(dv, axis=0)

    if with_dw:
        @pl.when((me + dist[1] < n) & (w == 3))
        def _():
            kv_copy(1).start()

    def picks(level):
        found = []
        for qb in range(nb):
            pair_ = [jnp.clip(ch_ref[PER * level + i, me * nb + qb] - (me - span(level)) * nb, 0, nb - 1)
                     for i in range(PER)]
            found.append((jnp.minimum(*pair_), jnp.maximum(*pair_)))
        return found

    def far_pass(level, heads, found):
        ks, vs = [], []
        for i, picked in enumerate((ks, vs)):
            for h in heads:
                blocks = [kvbuf[level, i, b * BLOCK:(b + 1) * BLOCK, lanes_of[h]] for b in range(nb)]
                chosen_blocks = []
                for low, high in found:
                    first_, second_ = blocks[0], blocks[1]
                    for b in range(1, nb - 1):
                        first_ = jnp.where(low == b, blocks[b], first_)
                    for b in range(2, nb):
                        second_ = jnp.where(high == b, blocks[b], second_)
                    chosen_blocks.append(jnp.concatenate([first_, second_], axis=0))
                picked.append(chosen_blocks)
        for h, (dq, dk, dv) in zip(heads, run_pass(heads, ks, vs, None)):
            dqt[h] = dqt[h] + jnp.concatenate(dq, axis=1)
            for i, new in enumerate((dk, dv)):
                for b in range(nb):
                    total = None
                    for qb in range(nb):
                        low, high = found[qb]
                        add = jnp.zeros((BLOCK, DH), F32)
                        if b:
                            add = jnp.where(high == b, new[qb][BLOCK:], add)
                        if b < nb - 1:
                            add = jnp.where(low == b, new[qb][:BLOCK], add)
                        total = add if total is None else total + add
                    if i == 0:
                        total = total * scale
                    gsend[level, i, b * BLOCK:(b + 1) * BLOCK, lanes_of[h]] = total.astype(BF)

    def wait_kv(level):
        kv_copy(level).wait_recv()

    def far_level(level):
        found = picks(level)
        far_pass(level, list(range(kvh)), found)

    def arrive(level):
        wait_kv(level)
        if with_dw:
            @pl.when((level == 2) & (me + dist[2] < n))
            def _():
                kv_pass_on(3, kvbuf.at[2]).start()

            @pl.when((level == 1) & second)
            def _():
                kv_pass_on(0, kvbuf.at[1]).start()

    def return_level(level):
        if with_dw:
            @pl.when(level != 1)
            def _():
                g_copy(level).start()
        else:
            g_copy(level).start()

    def pass_x_on(k):
        drain(xbuf.at[0, 0:2 * tok], x_r.at[k, 0])
        for idx in (1, 2):
            x_forward(idx, k).start()

    for turn, level in enumerate(turns[:-1]):
        if with_dw and turn == 2:
            @pl.when((z >= 1) & first)
            def _():
                pass_x_on(0)

        @pl.when(me >= span(level))
        def _():
            arrive(level)
            far_level(level)
            return_level(level)

    if with_dw:
        mine = pl.ds(pl.multiple_of(w * tok, tok), tok)
        hops = list(range(2, wn, 2))

        def a_copy(h, s):
            to = pair if s == 0 else lax.rem(w + s, wn)
            return pltpu.make_async_remote_copy(
                src_ref=dqall.at[h, mine], dst_ref=dqall.at[h, mine],
                send_sem=a_s, recv_sem=a_r.at[h, s // 2],
                device_id={"kv": z * wn + to}, device_id_type=pl.DeviceIdType.MESH)

        def f_copy(h, s):
            slot = pl.ds(pl.multiple_of(lax.rem(w + wn - s, wn) * tok, tok), tok)
            return pltpu.make_async_remote_copy(
                src_ref=dqall.at[h, slot], dst_ref=dqall.at[h, slot],
                send_sem=a_s, recv_sem=a_r.at[h, 0],
                device_id={"kv": z * wn + pair}, device_id_type=pl.DeviceIdType.MESH)

    if with_dw:
        @pl.when((z >= 2) & second)
        def _():
            pass_x_on(0)

    last = turns[-1]
    for h in range(kvh):
        @pl.when(me >= span(last))
        def _():
            if h == 0:
                arrive(last)
            far_pass(last, [h], picks(last))
        whole = (dqt[h] * scale).astype(BF)
        step = 2 if grp % 2 == 0 else 1
        for g in range(0, grp, step):
            for qb in range(nb):
                at = qb * part_cols + g * BLOCK
                low = jnp.concatenate(
                    [whole[:, at + j * BLOCK:at + (j + 1) * BLOCK] for j in range(step)], axis=0).T
                i = h * grp + g
                dq_out[qb * BLOCK:(qb + 1) * BLOCK, i * DH:(i + step) * DH] = low
                if with_dw:
                    at_rows = pl.ds(pl.multiple_of(w * tok + qb * BLOCK, BLOCK), BLOCK)
                    dqall[2 * h + g // 2, at_rows, g % 2 * DH:(g % 2 + step) * DH] = low
            if with_dw and (g + step) % 2 == 0:
                each = 2 * h + g // 2
                for s in hops:
                    a_copy(each, s).start()
                a_copy(each, 0).start()

    @pl.when(me >= span(last))
    def _():
        return_level(last)

    def early_sum():
        @pl.when(second)
        def _():
            g_copy(0).wait_recv()
            gsend[1] = (gsend[1].astype(F32) + grecv[0].astype(F32)).astype(BF)

        g_copy(1).start()

    if with_dw:
        @pl.when((z < 1) | ((z < 2) & second))
        def _():
            pass_x_on(0)

        pass_x_on(1)

        @pl.when((me >= dist[1]) & (w < 2))
        def _():
            early_sum()

        def x_arrive(k):
            drain(xbuf.at[0, 0:3 * tok], x_r.at[k, 1])
            drain(xbuf.at[0, 0:2 * tok], x_r.at[k, 2])

        wide = grp * DH // 2
        chunks = list(range(2 * kvh))

        def w_copy(h, i, slot, to):
            return pltpu.make_async_remote_copy(
                src_ref=part.at[h, i], dst_ref=precv.at[h, slot],
                send_sem=w_s, recv_sem=w_r.at[h, slot],
                device_id={"kv": to * wn + w}, device_id_type=pl.DeviceIdType.MESH)

        def w_arrive(h, slot):
            w_copy(h, 1, slot, near).wait_recv()

        def send_part(h, i, slot, block, to, add=None):
            new = dot(xt[block], dqall[h], NN)
            if add is not None:
                w_arrive(h, add)
                new = new + precv[h, add].astype(F32)
            part[h, i] = new.astype(BF)
            w_copy(h, i, slot, to).start()

        def across_on(h):
            for s in hops:
                a_copy(h, s).wait_recv()
                f_copy(h, s).start()

        for h in range(kvh):
            if h == 0:
                across_on(0)
                across_on(1)

                @pl.when(second)
                def _():
                    for each in chunks[2:]:
                        across_on(each)
            else:
                @pl.when(first)
                def _():
                    across_on(2 * h)
                    across_on(2 * h + 1)

            if h < zper:
                x_arrive(h)
                for zz in ((lax.rem(near + 2, zn), near), (far, z))[h]:
                    xt[zz] = xbuf[zz].T
            for each in (2 * h, 2 * h + 1):
                drain(dqall.at[each, 0:2 * tok], a_r.at[each, 0])

                @pl.when(outer)
                def _():
                    send_part(each, 0, 0, to_outer, near)

            @pl.when(outer)
            def _():
                if h:
                    for each in chunks:
                        send_part(each, 2, 3, to_inner, near)

            @pl.when(inner)
            def _():
                for each in (2 * h, 2 * h + 1):
                    send_part(each, 1, 1, near, near)

        @pl.when(w >= 2)
        def _():
            early_sum()

        @pl.when(outer)
        def _():
            for each in chunks:
                send_part(each, 1, 1, near, near)

        @pl.when(inner)
        def _():
            for h in chunks:
                send_part(h, 0, 2, to_outer, to_outer, 0)
            for h in chunks:
                send_part(h, 2, 2, to_inner, to_inner, 3)

        for h in chunks:
            dw_out[:, h * wide:(h + 1) * wide] = dot(xt[z], dqall[h], NN)
        drain(xbuf.at[0:2], x_s.at[0])
        drain(xbuf.at[0:3, 0:2 * tok], x_s.at[1])
        drain(dqall.at[:, 0:3 * tok], a_s)

    def add_in(level):
        g_copy(level).wait_recv()
        acc[...] = acc[...] + grecv[level].astype(F32)

    def sent_kv(level):
        kv_copy(level).wait_send()

    if with_dw:
        @pl.when(first)
        def _():
            sent_kv(0)
            add_in(0)

            @pl.when(me >= dist[1])
            def _():
                g_copy(0).wait_send()

        @pl.when(second)
        def _():
            g_copy(0).wait_send()

            @pl.when(me >= dist[1])
            def _():
                sent_kv(0)

        @pl.when((me >= dist[2]) & (me + dist[2] < n))
        def _():
            sent_kv(3)

        for level in (1, 2, 3):
            @pl.when(me + dist[level] < n)
            def _():
                if level < 3:
                    sent_kv(level)
                add_in(level)

            @pl.when(me >= dist[level])
            def _():
                g_copy(level).wait_send()
    else:
        for level, d in enumerate(dist):
            @pl.when(me + d < n)
            def _():
                sent_kv(level)
                add_in(level)

            @pl.when(me >= d)
            def _():
                g_copy(level).wait_send()

    dk_out[...] = acc[0].astype(BF)
    dv_out[...] = acc[1].astype(BF)
    if with_dw:
        for h in chunks:
            lanes = slice(h * wide, (h + 1) * wide)
            w_arrive(h, 1)
            w_arrive(h, 2)
            dw_out[:, lanes] = dw_out[:, lanes] + precv[h, 1].astype(F32) + precv[h, 2].astype(F32)
        drain(part, w_s)


def writer(*refs):
    count = (len(refs) - 1) // 2
    sem = refs[-1]
    copies = [pltpu.make_async_copy(refs[i], refs[count + i], sem.at[i]) for i in range(count)]
    for copy in copies:
        copy.start()
    for copy in copies:
        copy.wait()


def shards(layer_input, queries, keys, values, attn_out, grad_out, log_sum, chosen):
    n = lax.axis_size("kv")
    tp = lax.axis_size("tp")
    tok, qw = queries.shape
    kw = keys.shape[1]
    kvh, qh = kw // DH, qw // DH
    cols = qh // kvh * tok
    depth = layer_input.shape[1] * tp
    rows = depth // n
    wn = math.isqrt(n)
    zn = n // wn
    with_dw = wn * wn == n and zn == 4 and tp == 2 and rows % 128 == 0
    vm = pl.BlockSpec(memory_space=pltpu.VMEM)
    out_shape = [
        jax.ShapeDtypeStruct((tok, qw), BF),
        jax.ShapeDtypeStruct((tok, kw), BF),
        jax.ShapeDtypeStruct((tok, kw), BF),
    ]
    args = [keys, values, queries, grad_out, attn_out, log_sum.T]
    if with_dw:
        args.append(layer_input)
    held = [((2, tok, kw), BF), ((3, tok, qw), BF)] + [(a.shape, a.dtype) for a in args[5:]]
    scratch = [pltpu.VMEM(*a) for a in held] + [
        pltpu.SMEM(chosen.T.shape, chosen.dtype),
        pltpu.SemaphoreType.DMA((5,)),
        pltpu.VMEM((kvh, cols, DH), BF),
        pltpu.VMEM((kvh, cols, DH), BF),
        pltpu.VMEM((kvh, 1, cols), F32),
        pltpu.VMEM((kvh, 1, cols), F32),
        pltpu.VMEM((kvh, DH, cols), F32),
        pltpu.VMEM((2, tok, kw), F32),
        pltpu.VMEM((LEVELS, 2, tok, kw), BF),
        pltpu.VMEM((LEVELS, 2, tok, kw), BF),
        pltpu.VMEM((LEVELS, 2, tok, kw), BF),
        pltpu.SemaphoreType.DMA((LEVELS,)),
        pltpu.SemaphoreType.DMA((LEVELS,)),
        pltpu.SemaphoreType.DMA((LEVELS,)),
        pltpu.SemaphoreType.DMA((LEVELS,)),
    ]
    hbm = pl.BlockSpec(memory_space=pltpu.HBM)
    specs = [hbm] * (len(args) + 1)
    if with_dw:
        out_shape.append(jax.ShapeDtypeStruct((rows, qw), F32))
        zper = zn // tp
        scratch += [
            pltpu.VMEM((zn, wn * tok, rows), BF),
            pltpu.VMEM((zn, rows, wn * tok), BF),
            pltpu.VMEM((2 * kvh, wn * tok, qw // kvh // 2), BF),
            pltpu.VMEM((2 * kvh, zn - 1, rows, qw // kvh // 2), BF),
            pltpu.VMEM((2 * kvh, zn, rows, qw // kvh // 2), BF),
            pltpu.SemaphoreType.DMA((2,)),
            pltpu.SemaphoreType.DMA((zper, 3)),
            pltpu.SemaphoreType.DMA,
            pltpu.SemaphoreType.DMA((2 * kvh, 2)),
            pltpu.SemaphoreType.DMA,
            pltpu.SemaphoreType.DMA((2 * kvh, zn)),
        ]
    outs = pl.pallas_call(
        functools.partial(kernel, (n, tp, with_dw)),
        out_shape=[pltpu.VMEM(a.shape, a.dtype) for a in out_shape],
        in_specs=specs,
        out_specs=[vm] * len(out_shape),
        scratch_shapes=scratch,
        compiler_params=pltpu.CompilerParams(
            collective_id=0, has_side_effects=True, vmem_limit_bytes=66100000),
    )(*args, chosen.T)
    outs = pl.pallas_call(
        writer,
        out_shape=out_shape,
        in_specs=[vm] * len(out_shape),
        out_specs=[hbm] * len(out_shape),
        scratch_shapes=[pltpu.SemaphoreType.DMA((len(out_shape),))],
        compiler_params=pltpu.CompilerParams(vmem_limit_bytes=1024 * 1024),
    )(*outs)
    if with_dw:
        return tuple(outs)
    whole_input = lax.all_gather(layer_input, "tp", axis=1, tiled=True)
    grad_weight = lax.psum_scatter(
        jnp.einsum("td,tc->dc", whole_input, outs[0], preferred_element_type=F32),
        "kv", scatter_dimension=0, tiled=True)
    return tuple(outs) + (grad_weight,)


def solution(mesh):
    spec = P("kv", "tp")
    return jax.shard_map(
        shards,
        mesh=mesh,
        in_specs=(spec,) * 7 + (P(),),
        out_specs=(spec,) * 4,
        check_vma=False,
    )
```

```python
import functools
import math

import jax
import jax.numpy as jnp
from jax import lax
from jax.experimental import pallas as pl
from jax.experimental.pallas import tpu as pltpu
from jax.sharding import PartitionSpec as P

DH = 64
BLOCK = 64
PER = 2
LEVELS = 4
LOG2E = 1.4426950408889634
NEG = -1e30
NT = (((1,), (1,)), ((), ()))
TN = (((0,), (0,)), ((), ()))
NN = (((1,), (0,)), ((), ()))
BF = jnp.bfloat16
F32 = jnp.float32


def dot(a, b, dims):
    return lax.dot_general(a, b, dims, preferred_element_type=F32)


def kernel(cfg, *refs):
    n, tp, with_dw = cfg
    count_in = 7 if with_dw else 6
    hbm, refs = refs[:count_in], refs[count_in:]
    ch_hbm, refs = refs[0], refs[1:]
    count_out = 4 if with_dw else 3
    outs, refs = refs[:count_out], refs[count_out:]
    kv_ref, qgo, lse_ref, refs = refs[0], refs[1], refs[2], refs[3:]
    if with_dw:
        x_ref, refs = refs[0], refs[1:]
    ch_ref, refs = refs[0], refs[1:]
    (in_s, qs, gs, lrow, drow, dqt, acc, kvbuf, gsend, grecv,
     kv_s, kv_r, g_s, g_r) = refs[:14]
    dq_out, dk_out, dv_out = outs[:3]
    k_ref, v_ref = kv_ref.at[0], kv_ref.at[1]
    q_ref, g_ref, o_ref = qgo.at[0], qgo.at[1], qgo.at[2]
    if with_dw:
        dw_out = outs[3]
        (xbuf, xt, dqall, part, precv, x_s, x_r, a_s, a_r, w_s, w_r, w_n) = refs[14:]
    places = [k_ref, v_ref, q_ref, g_ref, o_ref, lse_ref] + ([x_ref] if with_dw else [])
    for i, to in enumerate(places):
        pltpu.make_async_copy(hbm[i], to, in_s.at[(0, 0, 1, 1, 1, 2, 4)[i]]).start()
    pltpu.make_async_copy(ch_hbm, ch_ref, in_s.at[3]).start()

    def drain(ref, sem):
        pltpu.make_async_copy(ref, ref, sem).wait()

    me = lax.axis_index("kv")
    mt = lax.axis_index("tp")
    tok = q_ref.shape[0]
    kvh = k_ref.shape[1] // DH
    qh = q_ref.shape[1] // DH
    grp = qh // kvh
    nb = tok // BLOCK
    cols = grp * tok
    scale = DH ** -0.5
    dist = [1, n // 8, n // 4, n // 2]

    def span(level):
        if isinstance(level, int):
            return dist[level]
        return jnp.where(level == 0, dist[0], jnp.where(level == 1, dist[1], jnp.where(level == 2, dist[2], dist[3])))

    if with_dw:
        wn = math.isqrt(n)
        zn = n // wn
        zper = zn // tp
        rows = dw_out.shape[0]
        z = me // wn
        w = lax.rem(me, wn)
        pair = w + 1 - 2 * lax.rem(w, 2)
        across = lax.rem(w + 2, wn)
        across_pair = lax.rem(pair + 2, wn)
        near = z + 1 - 2 * lax.rem(z, 2)
        far = lax.rem(z + 2, zn)
        outer = (z == 0) | (z == zn - 1)
        inner = (z > 0) & (z < zn - 1)
        to_outer = jnp.where(outer, zn - 1 - z, zn - 1 - near)
        to_inner = jnp.where(outer, zn - 1 - near, zn - 1 - z)
        partner = me + 1 - 2 * lax.rem(me, 2)
        first = lax.rem(me, 2) == 0
        second = lax.rem(me, 2) == 1
        order = [1 - lax.rem(z, 2), lax.rem(z, 2)]
        plane = [(pair, mt), (across, mt), (across_pair, mt), (w, 1 - mt), (pair, 1 - mt)]

    barrier = pltpu.get_barrier_semaphore()
    count = jnp.int32(0)
    for d in dist[1:] if with_dw else dist:
        @pl.when(me + d < n)
        def _():
            pl.semaphore_signal(barrier, inc=1, device_id={"kv": me + d}, device_id_type=pl.DeviceIdType.MESH)

        @pl.when(me >= d)
        def _():
            pl.semaphore_signal(barrier, inc=1, device_id={"kv": me - d}, device_id_type=pl.DeviceIdType.MESH)

        count = count + jnp.where(me + d < n, 1, 0) + jnp.where(me >= d, 1, 0)
    if with_dw:
        for wt, tt in plane:
            pl.semaphore_signal(barrier, inc=1, device_id={"kv": z * wn + wt, "tp": tt}, device_id_type=pl.DeviceIdType.MESH)
        for zt in (near, far):
            pl.semaphore_signal(barrier, inc=1, device_id={"kv": zt * wn + w}, device_id_type=pl.DeviceIdType.MESH)
        count = count + len(plane) + 2
    pl.semaphore_wait(barrier, count)

    def kv_copy(level):
        return pltpu.make_async_remote_copy(
            src_ref=kv_ref, dst_ref=kvbuf.at[level],
            send_sem=kv_s.at[level], recv_sem=kv_r.at[level],
            device_id={"kv": me + span(level)}, device_id_type=pl.DeviceIdType.MESH)

    def kv_pass_on(level, src):
        return pltpu.make_async_remote_copy(
            src_ref=src, dst_ref=kvbuf.at[level],
            send_sem=kv_s.at[level], recv_sem=kv_r.at[level],
            device_id={"kv": partner if level == 0 else me + dist[2]}, device_id_type=pl.DeviceIdType.MESH)

    def g_copy(level):
        to = jnp.where(level == 0, partner, me - span(level)) if with_dw else me - dist[level]
        return pltpu.make_async_remote_copy(
            src_ref=gsend.at[level], dst_ref=grecv.at[level],
            send_sem=g_s.at[level], recv_sem=g_r.at[level],
            device_id={"kv": to}, device_id_type=pl.DeviceIdType.MESH)

    drain(kv_ref, in_s.at[0])
    turns = [0, 1, 3, 2]
    if with_dw:
        late = w == 0
        turns = [jnp.where(second, 0, 2), jnp.where(second, 2, jnp.where(late, 0, 1)),
                 jnp.where(second, 1, jnp.where(late, 3, 0)), jnp.where(late, 1, 3)]
    for level in (2, 1) if with_dw else turns:
        @pl.when((me + dist[level] < n) & (w < 3) if with_dw and level == 1 else me + dist[level] < n)
        def _():
            kv_copy(level).start()

    if with_dw:
        @pl.when(first)
        def _():
            kv_pass_on(0, kv_ref).start()

        def x_copy(idx, k):
            wt, tt = plane[idx]
            zz = order[k]
            off = pl.multiple_of((zz * wn + wt) * rows, rows)
            return pltpu.make_async_remote_copy(
                src_ref=x_ref.at[:, pl.ds(off, rows)],
                dst_ref=xbuf.at[mt * zper + zz, pl.ds(pl.multiple_of(w * tok, tok), tok)],
                send_sem=x_s.at[0 if idx else 1], recv_sem=x_r.at[k, 0 if idx in (1, 2) else 1],
                device_id={"kv": z * wn + wt, "tp": tt}, device_id_type=pl.DeviceIdType.MESH)

        def x_forward(idx, k):
            slot = xbuf.at[mt * zper + order[k], pl.ds(pl.multiple_of(plane[idx][0] * tok, tok), tok)]
            return pltpu.make_async_remote_copy(
                src_ref=slot, dst_ref=slot,
                send_sem=x_s.at[1], recv_sem=x_r.at[k, 2],
                device_id={"kv": me, "tp": 1 - mt}, device_id_type=pl.DeviceIdType.MESH)

        drain(x_ref, in_s.at[4])
        for k in range(zper):
            for idx in (1, 2, 3, 4, 0):
                x_copy(idx, k).start()
        for zz in range(zper):
            off = pl.multiple_of((zz * wn + w) * rows, rows)
            xbuf[mt * zper + zz, pl.ds(pl.multiple_of(w * tok, tok), tok), :] = x_ref[:, pl.ds(off, rows)]

    drain(qgo, in_s.at[1])
    drain(lse_ref, in_s.at[2])
    pltpu.make_async_copy(ch_hbm, ch_ref, in_s.at[3]).wait()
    lse_t = lse_ref[...] * (-LOG2E)
    prod = g_ref[...].astype(F32) * o_ref[...].astype(F32)
    hi = prod.astype(BF)
    lo = (prod - hi.astype(F32)).astype(BF)
    pick = (lax.broadcasted_iota(jnp.int32, (16, qh * DH), 1) // DH
            == lax.broadcasted_iota(jnp.int32, (16, qh * DH), 0)).astype(F32).astype(BF)
    delta_t = dot(pick, hi, NT) + dot(pick, lo, NT)
    part_cols = grp * BLOCK
    for h in range(kvh):
        for g in range(grp):
            i = h * grp + g
            for qb in range(nb):
                rows_ = slice(qb * BLOCK, (qb + 1) * BLOCK)
                to = slice(qb * part_cols + g * BLOCK, qb * part_cols + (g + 1) * BLOCK)
                lrow[h, 0:1, to] = lse_t[i:i + 1, rows_]
                drow[h, 0:1, to] = delta_t[i:i + 1, rows_]
                qs[h, to, :] = q_ref[rows_, i * DH:(i + 1) * DH]
                gs[h, to, :] = g_ref[rows_, i * DH:(i + 1) * DH]

    def run_pass(heads, ks, vs, keep):
        to = [slice(qb * part_cols, (qb + 1) * part_cols) for qb in range(nb)]
        each = [(h, t, k, v) for h, hk, hv in zip(heads, ks, vs) for t, k, v in zip(to, hk, hv)]
        st = [dot(k, qs[h, t, :], NT) for h, t, k, v in each]
        dp = [dot(v, gs[h, t, :], NT) for h, t, k, v in each]
        st = [x * (scale * LOG2E) + lrow[h, 0:1, t] for x, (h, t, k, v) in zip(st, each)]
        p = [jnp.exp2(x if keep is None else jnp.where(keep, x, NEG)) for x in st]
        ds = [(x * (y - drow[h, 0:1, t])).astype(BF) for x, y, (h, t, k, v) in zip(p, dp, each)]
        dv = [dot(x.astype(BF), gs[h, t, :], NN) for x, (h, t, k, v) in zip(p, each)]
        dq = [dot(k, x, TN) for x, (h, t, k, v) in zip(ds, each)]
        dk = [dot(x, qs[h, t, :], NN) for x, (h, t, k, v) in zip(ds, each)]
        return [(dq[i * nb:(i + 1) * nb], dk[i * nb:(i + 1) * nb], dv[i * nb:(i + 1) * nb]) for i in range(len(heads))]

    causal = (lax.rem(lax.broadcasted_iota(jnp.int32, (BLOCK, part_cols), 1), BLOCK)
              >= lax.broadcasted_iota(jnp.int32, (BLOCK, part_cols), 0))
    blocks = [slice(qb * BLOCK, (qb + 1) * BLOCK) for qb in range(nb)]
    lanes_of = [slice(h * DH, (h + 1) * DH) for h in range(kvh)]
    own = run_pass(list(range(kvh)), [[k_ref[r, l] for r in blocks] for l in lanes_of],
                   [[v_ref[r, l] for r in blocks] for l in lanes_of], causal)
    for h, (dq, dk, dv) in enumerate(own):
        dqt[h] = jnp.concatenate(dq, axis=1)
        acc[0, :, lanes_of[h]] = jnp.concatenate(dk, axis=0) * scale
        acc[1, :, lanes_of[h]] = jnp.concatenate(dv, axis=0)

    if with_dw:
        @pl.when((me + dist[1] < n) & (w == 3))
        def _():
            kv_copy(1).start()

    def picks(level):
        found = []
        for qb in range(nb):
            pair_ = [jnp.clip(ch_ref[PER * level + i, me * nb + qb] - (me - span(level)) * nb, 0, nb - 1)
                     for i in range(PER)]
            found.append((jnp.minimum(*pair_), jnp.maximum(*pair_)))
        return found

    def far_pass(level, heads, found):
        ks, vs = [], []
        for i, picked in enumerate((ks, vs)):
            for h in heads:
                blocks = [kvbuf[level, i, b * BLOCK:(b + 1) * BLOCK, lanes_of[h]] for b in range(nb)]
                chosen_blocks = []
                for low, high in found:
                    first_, second_ = blocks[0], blocks[1]
                    for b in range(1, nb - 1):
                        first_ = jnp.where(low == b, blocks[b], first_)
                    for b in range(2, nb):
                        second_ = jnp.where(high == b, blocks[b], second_)
                    chosen_blocks.append(jnp.concatenate([first_, second_], axis=0))
                picked.append(chosen_blocks)
        for h, (dq, dk, dv) in zip(heads, run_pass(heads, ks, vs, None)):
            dqt[h] = dqt[h] + jnp.concatenate(dq, axis=1)
            for i, new in enumerate((dk, dv)):
                for b in range(nb):
                    total = None
                    for qb in range(nb):
                        low, high = found[qb]
                        add = jnp.zeros((BLOCK, DH), F32)
                        if b:
                            add = jnp.where(high == b, new[qb][BLOCK:], add)
                        if b < nb - 1:
                            add = jnp.where(low == b, new[qb][:BLOCK], add)
                        total = add if total is None else total + add
                    if i == 0:
                        total = total * scale
                    gsend[level, i, b * BLOCK:(b + 1) * BLOCK, lanes_of[h]] = total.astype(BF)

    def wait_kv(level):
        kv_copy(level).wait_recv()

    def far_level(level):
        found = picks(level)
        far_pass(level, list(range(kvh)), found)

    def arrive(level):
        wait_kv(level)
        if with_dw:
            @pl.when((level == 2) & (me + dist[2] < n))
            def _():
                kv_pass_on(3, kvbuf.at[2]).start()

            @pl.when((level == 1) & second)
            def _():
                kv_pass_on(0, kvbuf.at[1]).start()

    def return_level(level):
        if with_dw:
            @pl.when(level != 1)
            def _():
                g_copy(level).start()
        else:
            g_copy(level).start()

    def pass_x_on(k):
        drain(xbuf.at[0, 0:2 * tok], x_r.at[k, 0])
        for idx in (1, 2):
            x_forward(idx, k).start()

    for turn, level in enumerate(turns[:-1]):
        if with_dw and turn == 2:
            @pl.when((z >= 1) & first)
            def _():
                pass_x_on(0)

        @pl.when(me >= span(level))
        def _():
            arrive(level)
            far_level(level)
            return_level(level)

    if with_dw:
        mine = pl.ds(pl.multiple_of(w * tok, tok), tok)
        hops = list(range(2, wn, 2))

        def a_copy(h, s):
            to = pair if s == 0 else lax.rem(w + s, wn)
            return pltpu.make_async_remote_copy(
                src_ref=dqall.at[h, mine], dst_ref=dqall.at[h, mine],
                send_sem=a_s, recv_sem=a_r.at[h, s // 2],
                device_id={"kv": z * wn + to}, device_id_type=pl.DeviceIdType.MESH)

        def f_copy(h, s):
            slot = pl.ds(pl.multiple_of(lax.rem(w + wn - s, wn) * tok, tok), tok)
            return pltpu.make_async_remote_copy(
                src_ref=dqall.at[h, slot], dst_ref=dqall.at[h, slot],
                send_sem=a_s, recv_sem=a_r.at[h, 0],
                device_id={"kv": z * wn + pair}, device_id_type=pl.DeviceIdType.MESH)

    if with_dw:
        @pl.when((z >= 2) & second)
        def _():
            pass_x_on(0)

    last = turns[-1]
    for h in range(kvh):
        @pl.when(me >= span(last))
        def _():
            if h == 0:
                arrive(last)
            far_pass(last, [h], picks(last))
        whole = (dqt[h] * scale).astype(BF)
        step = 2 if grp % 2 == 0 else 1
        for g in range(0, grp, step):
            for qb in range(nb):
                at = qb * part_cols + g * BLOCK
                low = jnp.concatenate(
                    [whole[:, at + j * BLOCK:at + (j + 1) * BLOCK] for j in range(step)], axis=0).T
                i = h * grp + g
                dq_out[qb * BLOCK:(qb + 1) * BLOCK, i * DH:(i + step) * DH] = low
                if with_dw:
                    at_rows = pl.ds(pl.multiple_of(w * tok + qb * BLOCK, BLOCK), BLOCK)
                    dqall[2 * h + g // 2, at_rows, g % 2 * DH:(g % 2 + step) * DH] = low
            if with_dw and (g + step) % 2 == 0:
                each = 2 * h + g // 2
                for s in hops:
                    a_copy(each, s).start()
                a_copy(each, 0).start()

    @pl.when(me >= span(last))
    def _():
        return_level(last)

    def early_sum():
        @pl.when(second)
        def _():
            g_copy(0).wait_recv()
            gsend[1] = (gsend[1].astype(F32) + grecv[0].astype(F32)).astype(BF)

        g_copy(1).start()

    if with_dw:
        @pl.when((z < 1) | ((z < 2) & second))
        def _():
            pass_x_on(0)

        pass_x_on(1)

        @pl.when((me >= dist[1]) & (w < 2))
        def _():
            early_sum()

        def x_arrive(k):
            drain(xbuf.at[0, 0:3 * tok], x_r.at[k, 1])
            drain(xbuf.at[0, 0:2 * tok], x_r.at[k, 2])

        wide = grp * DH // 2
        chunks = list(range(2 * kvh))

        def w_copy(h, i, slot, to):
            return pltpu.make_async_remote_copy(
                src_ref=part.at[h, i], dst_ref=precv.at[h, slot],
                send_sem=w_s, recv_sem=w_n if slot == 1 else w_r.at[h, max(slot - 1, 0)],
                device_id={"kv": to * wn + w}, device_id_type=pl.DeviceIdType.MESH)

        def w_arrive(h, slot):
            w_copy(h, 1, slot, near).wait_recv()

        def send_part(h, i, slot, block, to, add=None):
            new = dot(xt[block], dqall[h], NN)
            if add is not None:
                w_arrive(h, add)
                new = new + precv[h, add].astype(F32)
            part[h, i] = new.astype(BF)
            w_copy(h, i, slot, to).start()

        def across_on(h):
            for s in hops:
                a_copy(h, s).wait_recv()
                f_copy(h, s).start()

        for h in range(kvh):
            if h == 0:
                across_on(0)
                across_on(1)

                @pl.when(second)
                def _():
                    for each in chunks[2:]:
                        across_on(each)
            else:
                @pl.when(first)
                def _():
                    across_on(2 * h)
                    across_on(2 * h + 1)

            if h < zper:
                x_arrive(h)
                for zz in ((lax.rem(near + 2, zn), near), (far, z))[h]:
                    xt[zz] = xbuf[zz].T
            for each in (2 * h, 2 * h + 1):
                drain(dqall.at[each, 0:2 * tok], a_r.at[each, 0])

                @pl.when(outer)
                def _():
                    send_part(each, 0, 0, to_outer, near)

            @pl.when(outer)
            def _():
                if h:
                    for each in chunks:
                        send_part(each, 2, 3, to_inner, near)

            @pl.when(inner)
            def _():
                for each in (2 * h, 2 * h + 1):
                    send_part(each, 1, 1, near, near)

        @pl.when(w >= 2)
        def _():
            early_sum()

        @pl.when(outer)
        def _():
            for each in chunks:
                send_part(each, 1, 1, near, near)

        @pl.when(inner)
        def _():
            for h in chunks:
                send_part(h, 0, 2, to_outer, to_outer, 0)
            for h in chunks:
                send_part(h, 2, 2, to_inner, to_inner, 3)

        for h in chunks:
            dw_out[:, h * wide:(h + 1) * wide] = dot(xt[z], dqall[h], NN)
        drain(xbuf.at[0:2], x_s.at[0])
        drain(xbuf.at[0:3, 0:2 * tok], x_s.at[1])
        drain(dqall.at[:, 0:3 * tok], a_s)

    def add_in(level):
        g_copy(level).wait_recv()
        acc[...] = acc[...] + grecv[level].astype(F32)

    def sent_kv(level):
        kv_copy(level).wait_send()

    if with_dw:
        @pl.when(first)
        def _():
            sent_kv(0)
            add_in(0)

            @pl.when(me >= dist[1])
            def _():
                g_copy(0).wait_send()

        @pl.when(second)
        def _():
            g_copy(0).wait_send()

            @pl.when(me >= dist[1])
            def _():
                sent_kv(0)

        @pl.when((me >= dist[2]) & (me + dist[2] < n))
        def _():
            sent_kv(3)

        for level in (1, 2, 3):
            @pl.when(me + dist[level] < n)
            def _():
                if level < 3:
                    sent_kv(level)
                add_in(level)

            @pl.when(me >= dist[level])
            def _():
                g_copy(level).wait_send()
    else:
        for level, d in enumerate(dist):
            @pl.when(me + d < n)
            def _():
                sent_kv(level)
                add_in(level)

            @pl.when(me >= d)
            def _():
                g_copy(level).wait_send()

    dk_out[...] = acc[0].astype(BF)
    dv_out[...] = acc[1].astype(BF)
    if with_dw:
        for h in chunks:
            lanes = slice(h * wide, (h + 1) * wide)
            if h == 0:
                drain(precv.at[:, 1], w_n)
            w_arrive(h, 2)
            dw_out[:, lanes] = dw_out[:, lanes] + precv[h, 1].astype(F32) + precv[h, 2].astype(F32)
        drain(part, w_s)


def writer(*refs):
    count = (len(refs) - 1) // 2
    sem = refs[-1]
    copies = [pltpu.make_async_copy(refs[i], refs[count + i], sem.at[i]) for i in range(count)]
    for copy in copies:
        copy.start()
    for copy in copies:
        copy.wait()


def shards(layer_input, queries, keys, values, attn_out, grad_out, log_sum, chosen):
    n = lax.axis_size("kv")
    tp = lax.axis_size("tp")
    tok, qw = queries.shape
    kw = keys.shape[1]
    kvh, qh = kw // DH, qw // DH
    cols = qh // kvh * tok
    depth = layer_input.shape[1] * tp
    rows = depth // n
    wn = math.isqrt(n)
    zn = n // wn
    with_dw = wn * wn == n and zn == 4 and tp == 2 and rows % 128 == 0
    vm = pl.BlockSpec(memory_space=pltpu.VMEM)
    out_shape = [
        jax.ShapeDtypeStruct((tok, qw), BF),
        jax.ShapeDtypeStruct((tok, kw), BF),
        jax.ShapeDtypeStruct((tok, kw), BF),
    ]
    args = [keys, values, queries, grad_out, attn_out, log_sum.T]
    if with_dw:
        args.append(layer_input)
    held = [((2, tok, kw), BF), ((3, tok, qw), BF)] + [(a.shape, a.dtype) for a in args[5:]]
    scratch = [pltpu.VMEM(*a) for a in held] + [
        pltpu.SMEM(chosen.T.shape, chosen.dtype),
        pltpu.SemaphoreType.DMA((5,)),
        pltpu.VMEM((kvh, cols, DH), BF),
        pltpu.VMEM((kvh, cols, DH), BF),
        pltpu.VMEM((kvh, 1, cols), F32),
        pltpu.VMEM((kvh, 1, cols), F32),
        pltpu.VMEM((kvh, DH, cols), F32),
        pltpu.VMEM((2, tok, kw), F32),
        pltpu.VMEM((LEVELS, 2, tok, kw), BF),
        pltpu.VMEM((LEVELS, 2, tok, kw), BF),
        pltpu.VMEM((LEVELS, 2, tok, kw), BF),
        pltpu.SemaphoreType.DMA((LEVELS,)),
        pltpu.SemaphoreType.DMA((LEVELS,)),
        pltpu.SemaphoreType.DMA((LEVELS,)),
        pltpu.SemaphoreType.DMA((LEVELS,)),
    ]
    hbm = pl.BlockSpec(memory_space=pltpu.HBM)
    specs = [hbm] * (len(args) + 1)
    if with_dw:
        out_shape.append(jax.ShapeDtypeStruct((rows, qw), F32))
        zper = zn // tp
        scratch += [
            pltpu.VMEM((zn, wn * tok, rows), BF),
            pltpu.VMEM((zn, rows, wn * tok), BF),
            pltpu.VMEM((2 * kvh, wn * tok, qw // kvh // 2), BF),
            pltpu.VMEM((2 * kvh, zn - 1, rows, qw // kvh // 2), BF),
            pltpu.VMEM((2 * kvh, zn, rows, qw // kvh // 2), BF),
            pltpu.SemaphoreType.DMA((2,)),
            pltpu.SemaphoreType.DMA((zper, 3)),
            pltpu.SemaphoreType.DMA,
            pltpu.SemaphoreType.DMA((2 * kvh, 2)),
            pltpu.SemaphoreType.DMA,
            pltpu.SemaphoreType.DMA((2 * kvh, zn - 1)),
            pltpu.SemaphoreType.DMA,
        ]
    outs = pl.pallas_call(
        functools.partial(kernel, (n, tp, with_dw)),
        out_shape=[pltpu.VMEM(a.shape, a.dtype) for a in out_shape],
        in_specs=specs,
        out_specs=[vm] * len(out_shape),
        scratch_shapes=scratch,
        compiler_params=pltpu.CompilerParams(
            collective_id=0, has_side_effects=True, vmem_limit_bytes=66100000),
    )(*args, chosen.T)
    outs = pl.pallas_call(
        writer,
        out_shape=out_shape,
        in_specs=[vm] * len(out_shape),
        out_specs=[hbm] * len(out_shape),
        scratch_shapes=[pltpu.SemaphoreType.DMA((len(out_shape),))],
        compiler_params=pltpu.CompilerParams(vmem_limit_bytes=1024 * 1024),
    )(*outs)
    if with_dw:
        return tuple(outs)
    whole_input = lax.all_gather(layer_input, "tp", axis=1, tiled=True)
    grad_weight = lax.psum_scatter(
        jnp.einsum("td,tc->dc", whole_input, outs[0], preferred_element_type=F32),
        "kv", scatter_dimension=0, tiled=True)
    return tuple(outs) + (grad_weight,)


def solution(mesh):
    spec = P("kv", "tp")
    return jax.shard_map(
        shards,
        mesh=mesh,
        in_specs=(spec,) * 7 + (P(),),
        out_specs=(spec,) * 4,
        check_vma=False,
    )
```
